32 devices in a mesh: sp: 4 (over z), fs: 4 (over y, x), tp: 2 (over core).
Axes of the slice: x: 2, y: 2, z: 4, core: 2. Of those that a mesh axis runs over, the one named last changes fastest.
Arguments:
- tokens: bfloat16 [4, 1024, 2048], P('fs', 'sp'), may hold values from -6 to 6
- mix_gain: float32 [2048], replicated, may hold values from 0.1 to 1.9
- query_down: bfloat16 [2048, 768], P('fs', 'tp'), may hold values from -0.125 to 0.125
- memory_down: bfloat16 [2048, 512], P('fs', 'tp'), may hold values from -0.125 to 0.125
- rope_weight: bfloat16 [2048, 32], replicated, may hold values from -0.125 to 0.125
- query_up: bfloat16 [768, 1536], P('fs', 'tp'), may hold values from -0.21875 to 0.21875
- key_up: bfloat16 [512, 1024], P('fs', 'tp'), may hold values from -0.25 to 0.25
- value_up: bfloat16 [512, 1024], P('fs', 'tp'), may hold values from -0.25 to 0.25
- latent_gain: float32 [768], replicated, may hold values from 0.1 to 1.9
- memory_gain: float32 [512], replicated, may hold values from 0.1 to 1.9
- query_gain: float32 [96], replicated, may hold values from 1 to 16
- key_gain: float32 [96], replicated, may hold values from 0.1 to 1.9
- conv_value: bfloat16 [2048, 1024], P('fs', 'tp'), may hold values from -1 to 1
- conv_gate: bfloat16 [2048, 1024], P('fs', 'tp'), may hold values from -0.125 to 0.125
- conv_kernel: bfloat16 [31, 1024], P(None, 'tp'), may hold values from -50 to 50
- channel_gain: float32 [1024], P('tp'), may hold values from 0.1 to 1.9
- channel_shift: float32 [1024], P('tp'), may hold values from -3 to 3
- heads_out: bfloat16 [1024, 2048], P('tp', 'fs'), may hold values from -0.75 to 0.75
- conv_out: bfloat16 [1024, 2048], P('tp', 'fs'), may hold values from -0.1875 to 0.1875
Outputs:
- mixed: bfloat16 [4, 1024, 2048], P('fs', 'sp')
The draws below stay inside these ranges and needn't reach their ends.
All inputs are finite; a program needn't handle non-finite values.
Results may differ from the reference program's by a relative error of at most 0.015.
The reference program's roundings to bfloat16 on the way count: a program that leaves them out, or rounds other values in their place, can miss the bound.
Values may be sent and summed in bfloat16 or wider, within the bound.
A program may use at most 64 MiB of HBM per device.

```python
import math
import jax
import jax.numpy as jnp
from jax import lax

D = 2048
HEADS = 16
QK_NOPE = 64
QK_ROPE = 32
V_DIM = 64
Q_LAT = 768
KV_LAT = 512
CONV_W = 1024
CONV_K = 31
SEG = 64
TOK_DEV = 256
QK_DIM = 96
SEQ = 1024
SEQS = 4
N_TP = 2


def draw_query_gain(key, part):
    gain_key = jax.random.fold_in(key, 11)
    return jnp.exp(jax.random.uniform(gain_key, (QK_DIM,), jnp.float32, 0.0, math.log(3.0)))


def draw_conv_value(key, part):
    noise_key, common_key, level_key = jax.random.split(jax.random.fold_in(key, 23), 3)
    noise = jnp.clip(jax.random.normal(noise_key, (D, CONV_W), jnp.float32), -5.0, 5.0)
    common = jnp.clip(jax.random.normal(common_key, (D,), jnp.float32), -5.0, 5.0)
    level = jax.random.uniform(level_key, (CONV_W,), jnp.float32, 0.5, 1.5)
    strength = 0.7
    return ((noise + strength * common[:, None] * level[None, :]) / math.sqrt(D)).astype(jnp.bfloat16)


def draw_conv_kernel(key, part):
    noise_key, scale_key = jax.random.split(jax.random.fold_in(key, 7))
    channel_pos = jnp.arange(CONV_W, dtype=jnp.float32) / CONV_W
    roughness = jnp.exp(jax.random.uniform(scale_key, (CONV_W,), jnp.float32, -0.7, 0.7))
    channel_scale = 10.0 ** channel_pos * roughness
    tap_draw = jnp.clip(jax.random.normal(noise_key, (CONV_K, CONV_W), jnp.float32), -5.0, 5.0)
    return ((tap_draw + 1.0) * channel_scale[None, :] / math.sqrt(CONV_K)).astype(jnp.bfloat16)


def steps_of(own_key, shape, cuts, least, top_value):
    level, own = 1.0, jax.random.fold_in(own_key, 6)
    for axis_at, shards_of in cuts:
        heights = jnp.exp(jax.random.uniform(jax.random.fold_in(own, axis_at), (shards_of,), jnp.float32, least / len(cuts), top_value / len(cuts)))
        level = level * jnp.repeat(heights, shape[axis_at] // shards_of).reshape([-1 if axis == axis_at else 1 for axis in range(len(shape))])
    return level


def gaussian(own_key, extent, width, reach, cuts=(), kind=jnp.bfloat16):
    factor_of = steps_of(own_key, extent, cuts, -0.22, 0.18) if cuts else 1.0
    drawn = jax.random.normal(own_key, extent, jnp.float32) * width * factor_of
    return jnp.minimum(jnp.maximum(drawn, -reach), reach).astype(kind)


def setup_inputs(seed: int = 0) -> dict:
    arg_keys = jax.random.split(jax.random.key(seed), 20)
    return {
        "tokens": gaussian(arg_keys[0], (SEQS, SEQ, D), 1.0, 6.0, ((0, 4), (1, 4))),
        "mix_gain": jnp.clip(1.0 + 0.18 * jax.random.normal(arg_keys[1], (D,), jnp.float32), 0.1, 1.9),
        "query_down": gaussian(arg_keys[2], (D, Q_LAT), D ** -0.5, 0.125, ((0, 4), (1, 2))),
        "memory_down": gaussian(arg_keys[3], (D, KV_LAT), D ** -0.5, 0.125, ((0, 4), (1, 2))),
        "rope_weight": gaussian(arg_keys[4], (D, QK_ROPE), D ** -0.5, 0.125),
        "query_up": gaussian(arg_keys[5], (Q_LAT, HEADS * QK_DIM), Q_LAT ** -0.5, 0.21875, ((0, 4), (1, 2))),
        "key_up": gaussian(arg_keys[6], (KV_LAT, HEADS * QK_NOPE), KV_LAT ** -0.5, 0.25, ((0, 4), (1, 2))),
        "value_up": gaussian(arg_keys[7], (KV_LAT, HEADS * V_DIM), KV_LAT ** -0.5, 0.25, ((0, 4), (1, 2))),
        "latent_gain": jnp.clip(1.0 + 0.18 * jax.random.normal(arg_keys[8], (Q_LAT,), jnp.float32), 0.1, 1.9),
        "memory_gain": jnp.clip(1.0 + 0.18 * jax.random.normal(arg_keys[9], (KV_LAT,), jnp.float32), 0.1, 1.9),
        "query_gain": draw_query_gain(jax.random.fold_in(arg_keys[19], 71), 0),
        "key_gain": jnp.clip(1.0 + 0.18 * jax.random.normal(arg_keys[11], (QK_DIM,), jnp.float32), 0.1, 1.9),
        "conv_value": draw_conv_value(jax.random.fold_in(arg_keys[19], 71), 0),
        "conv_gate": gaussian(arg_keys[13], (D, CONV_W), D ** -0.5, 0.125, ((0, 4), (1, 2))),
        "conv_kernel": draw_conv_kernel(jax.random.fold_in(arg_keys[19], 71), 0),
        "channel_gain": jnp.clip(1.0 + 0.18 * jax.random.normal(arg_keys[15], (CONV_W,), jnp.float32), 0.1, 1.9),
        "channel_shift": gaussian(arg_keys[16], (CONV_W,), 0.5, 3.0, ((0, 2),), jnp.float32),
        "heads_out": gaussian(arg_keys[17], (HEADS * V_DIM, D), V_DIM ** -0.5, 0.75, ((0, 2), (1, 4))),
        "conv_out": gaussian(arg_keys[18], (CONV_W, D), CONV_W ** -0.5, 0.1875, ((0, 2), (1, 4))),
    }


epsilon = 1e-06
rope_base = 10000.0
masked_score = -1e+30

def norm_rows(matrix, scale_vector):
    return matrix * lax.rsqrt(lax.optimization_barrier(jnp.mean(matrix * matrix, axis=-1, keepdims=True)) + epsilon) * scale_vector.astype(jnp.float32)

def rope_tables(positions):
    inverse_freq = 1.0 / rope_base ** (jnp.arange(0, QK_ROPE, 2, dtype=jnp.float32) / QK_ROPE)
    angles = positions.astype(jnp.float32)[:, None] * inverse_freq[None, :]
    return (jnp.cos(angles)[:, None, :], jnp.sin(angles)[:, None, :])

def rotate(matrix, cosine_table, sine_table):
    half_width = matrix.shape[-1] // 2
    front_half = matrix[..., :half_width]
    back_half = matrix[..., half_width:]
    return jnp.concatenate([front_half * cosine_table - back_half * sine_table, front_half * sine_table + back_half * cosine_table], axis=-1)

def heads_query(latent, weight, scale_vector, cosine_table, sine_table):
    row_count = latent.shape[0]
    projected = jnp.dot(latent, weight, preferred_element_type=jnp.float32)
    projected = norm_rows(projected.reshape(row_count, weight.shape[1] // QK_DIM, QK_DIM), scale_vector)
    turned = rotate(projected[..., QK_NOPE:], cosine_table, sine_table)
    return jnp.concatenate([projected[..., :QK_NOPE], turned], axis=-1).astype(jnp.bfloat16)

def heads_key(latent, rope_rows, weight, scale_vector, cosine_table, sine_table):
    row_count = latent.shape[0]
    head_count = weight.shape[1] // QK_NOPE
    nope_part = jnp.dot(latent, weight, preferred_element_type=jnp.float32).reshape(row_count, head_count, QK_NOPE)
    shared = jnp.broadcast_to(rope_rows.astype(jnp.float32)[:, None, :], (row_count, head_count, QK_ROPE))
    joined = norm_rows(jnp.concatenate([nope_part, shared], axis=-1), scale_vector)
    turned = rotate(joined[..., QK_NOPE:], cosine_table, sine_table)
    return jnp.concatenate([joined[..., :QK_NOPE], turned], axis=-1).astype(jnp.bfloat16)

def depthwise(extended, kernel, row_count):

    def add_tap(tap_index, running):
        window = lax.dynamic_slice_in_dim(extended, tap_index.astype(jnp.int32), row_count, 0).astype(jnp.float32)
        weight_row = lax.dynamic_slice_in_dim(kernel, tap_index.astype(jnp.int32), 1, 0).astype(jnp.float32)
        return running + window * weight_row
    return lax.fori_loop(0, kernel.shape[0], add_tap, jnp.zeros((row_count, kernel.shape[1]), jnp.float32))

def attention_block(queries, key_rows, value_rows, query_pos):
    key_pos = jnp.arange(key_rows.shape[0], dtype=jnp.int32)
    scores = jnp.einsum('qhd,khd->qhk', queries.astype(jnp.float32), key_rows.astype(jnp.float32)) * QK_DIM ** (-0.5)
    allowed = ((key_pos // SEG)[None, :] <= (query_pos // SEG)[:, None])[:, None, :]
    scores = jnp.where(allowed, scores, masked_score)
    row_max = lax.optimization_barrier(jnp.max(scores, axis=2, keepdims=True))
    weights = jnp.where(allowed, jnp.exp(scores - row_max), 0.0)
    row_total = lax.optimization_barrier(jnp.sum(weights, axis=2))
    rounded = weights.astype(jnp.bfloat16)
    summed = jnp.einsum('qhk,khd->qhd', rounded.astype(jnp.float32), value_rows.astype(jnp.float32))
    return (summed / row_total[:, :, None]).astype(jnp.bfloat16)

def one_sequence(tokens, mix_gain, query_down, memory_down, rope_weight, query_up, key_up, value_up, latent_gain, memory_gain, query_gain, key_gain, conv_value, conv_gate, conv_kernel, channel_gain, channel_shift, heads_out, conv_out):
    normed = norm_rows(tokens.astype(jnp.float32), mix_gain).astype(jnp.bfloat16)
    latent_query = jnp.dot(normed, query_down, preferred_element_type=jnp.float32).astype(jnp.bfloat16)
    latent_memory = jnp.dot(normed, memory_down, preferred_element_type=jnp.float32).astype(jnp.bfloat16)
    rope_rows = jnp.dot(normed, rope_weight, preferred_element_type=jnp.float32).astype(jnp.bfloat16)
    value_part = jnp.dot(normed, conv_value, preferred_element_type=jnp.float32)
    gate_part = jnp.dot(normed, conv_gate, preferred_element_type=jnp.float32)
    gated = (value_part * jax.nn.sigmoid(gate_part)).astype(jnp.bfloat16)
    query_normed = norm_rows(latent_query.astype(jnp.float32), latent_gain).astype(jnp.bfloat16)
    memory_normed = norm_rows(latent_memory.astype(jnp.float32), memory_gain).astype(jnp.bfloat16)
    positions = jnp.arange(SEQ, dtype=jnp.int32)
    cosine_table, sine_table = rope_tables(positions)
    queries = heads_query(query_normed, query_up, query_gain, cosine_table, sine_table)
    key_rows = heads_key(memory_normed, rope_rows, key_up, key_gain, cosine_table, sine_table)
    value_rows = jnp.dot(memory_normed, value_up, preferred_element_type=jnp.float32).astype(jnp.bfloat16).reshape(SEQ, HEADS, V_DIM)
    query_blocks = queries.reshape(SEQ // TOK_DEV, TOK_DEV, HEADS, QK_DIM)
    block_pos = positions.reshape(SEQ // TOK_DEV, TOK_DEV)

    def per_block(pair):
        return attention_block(pair[0], key_rows, value_rows, pair[1])
    attention = lax.map(per_block, (query_blocks, block_pos)).reshape(SEQ, HEADS * V_DIM)
    extended = jnp.concatenate([jnp.zeros((CONV_K - 1, CONV_W), jnp.bfloat16), gated], axis=0)
    conv_sum = depthwise(extended, conv_kernel, SEQ)
    row_mean = lax.optimization_barrier(jnp.mean(conv_sum, axis=1, keepdims=True))
    centered = conv_sum - row_mean
    spread = lax.optimization_barrier(jnp.mean(centered * centered, axis=1, keepdims=True))
    conv_result = jax.nn.silu(centered * lax.rsqrt(spread + epsilon) * channel_gain.astype(jnp.float32) + channel_shift.astype(jnp.float32)).astype(jnp.bfloat16)
    attn_width = HEADS * V_DIM // N_TP
    conv_width = CONV_W // N_TP
    mixed = jnp.zeros((SEQ, D), jnp.float32)
    for group_index in range(N_TP):
        head_cols = slice(group_index * attn_width, (group_index + 1) * attn_width)
        conv_cols = slice(group_index * conv_width, (group_index + 1) * conv_width)
        partial_sum = jnp.dot(attention[:, head_cols], heads_out[head_cols], preferred_element_type=jnp.float32)
        partial_sum = partial_sum + jnp.dot(conv_result[:, conv_cols], conv_out[conv_cols], preferred_element_type=jnp.float32)
        mixed = mixed + lax.optimization_barrier(partial_sum.astype(jnp.bfloat16)).astype(jnp.float32)
    return mixed.astype(jnp.bfloat16)

def reference(tokens, mix_gain, query_down, memory_down, rope_weight, query_up, key_up, value_up, latent_gain, memory_gain, query_gain, key_gain, conv_value, conv_gate, conv_kernel, channel_gain, channel_shift, heads_out, conv_out):

    def per_sequence(sequence):
        return one_sequence(sequence, mix_gain, query_down, memory_down, rope_weight, query_up, key_up, value_up, latent_gain, memory_gain, query_gain, key_gain, conv_value, conv_gate, conv_kernel, channel_gain, channel_shift, heads_out, conv_out)
    return lax.map(per_sequence, tokens)
```

```python
import functools

import jax
import jax.numpy as jnp
import numpy as np
from jax import lax
from jax.experimental import pallas as pl
from jax.experimental.pallas import tpu as pltpu
from jax.sharding import PartitionSpec as P

MESH_ID = pl.DeviceIdType.MESH

QK_NOPE = 64
QK_ROPE = 32
V_DIM = 64
CONV_W = 1024
SEG = 64
QK_DIM = 96


epsilon = 1e-06
rope_base = 10000.0
masked_score = -1e30


def norm_rows(matrix, scale_vector):
    return (
        matrix
        * lax.rsqrt(jnp.mean(matrix * matrix, axis=-1, keepdims=True) + epsilon)
        * scale_vector
    )


def rope_tables(positions):
    inverse_freq = 1.0 / rope_base ** (jnp.arange(0, QK_ROPE, 2, dtype=jnp.float32) / QK_ROPE)
    angles = positions.astype(jnp.float32)[:, None] * inverse_freq[None, :]
    return (jnp.cos(angles)[:, None, :], jnp.sin(angles)[:, None, :])


def rotate(matrix, cosine_table, sine_table):
    half_width = matrix.shape[-1] // 2
    front_half = matrix[..., :half_width]
    back_half = matrix[..., half_width:]
    return jnp.concatenate(
        [
            front_half * cosine_table - back_half * sine_table,
            front_half * sine_table + back_half * cosine_table,
        ],
        axis=-1,
    )


def heads_query(latent, weight, scale_vector, cosine_table, sine_table):
    row_count = latent.shape[0]
    projected = jnp.dot(latent, weight, preferred_element_type=jnp.float32)
    projected = norm_rows(
        projected.reshape(row_count, weight.shape[1] // QK_DIM, QK_DIM), scale_vector
    )
    turned = rotate(projected[..., QK_NOPE:], cosine_table, sine_table)
    return jnp.concatenate([projected[..., :QK_NOPE], turned], axis=-1).astype(jnp.bfloat16)


def heads_key(latent, rope_rows, weight, scale_vector, cosine_table, sine_table):
    row_count = latent.shape[0]
    head_count = weight.shape[1] // QK_NOPE
    nope_part = jnp.dot(latent, weight, preferred_element_type=jnp.float32).reshape(
        row_count, head_count, QK_NOPE
    )
    shared = jnp.broadcast_to(
        rope_rows.astype(jnp.float32)[:, None, :], (row_count, head_count, QK_ROPE)
    )
    joined = norm_rows(jnp.concatenate([nope_part, shared], axis=-1), scale_vector)
    turned = rotate(joined[..., QK_NOPE:], cosine_table, sine_table)
    return jnp.concatenate([joined[..., :QK_NOPE], turned], axis=-1).astype(jnp.bfloat16)


RIM = 32


def relayed_rows(rows, paired):
    return (rows * 5 // 16) // 16 * 16 if paired else 0


def gather_kernel(
    sizes,
    x_ref, gain_ref, rope_ref, taps_ref, cgain_ref, cshift_ref,
    qd, md, cv, cg, qu, ku, vu, ho, co,
    lq_all, lm_all, rr_all, conv_ref, qu_all, ku_all, vu_all, ho_all, co_all,
    qd_all, md_all, cv_all, cg_all, normed, acc_q, acc_m, acc_v, acc_g, ext, tail, rim,
    sums, stats, stats_all,
    send_d, recv_d, send_r, recv_r, send_z, recv_z, local_sem, rim_sem,
    sp_send, sp_recv, rr_send, rr_recv, tp_send, tp_recv,
):
    n_fs, n_sp, n_tp = sizes
    paired = n_sp % 2 == 0
    f = lax.axis_index("fs")
    s = lax.axis_index("sp")
    t = lax.axis_index("tp")
    parity = lax.rem(s, 2)
    partner = s + 1 - 2 * parity

    barrier = pltpu.get_barrier_semaphore()
    for axis, at, count in (("fs", f, n_fs), ("sp", s, n_sp), ("tp", t, n_tp)):
        for k in range(1, count):
            pl.semaphore_signal(
                barrier, inc=1, device_id={axis: lax.rem(at + k, count)}, device_id_type=MESH_ID
            )
    pl.semaphore_wait(barrier, n_fs + n_sp + n_tp - 3)

    jobs = [
        (qd, qd_all, 0), (md, md_all, 0), (cv, cv_all, 0), (cg, cg_all, 0),
        (qu, qu_all, 0), (ku, ku_all, 0), (vu, vu_all, 0), (ho, ho_all, 1), (co, co_all, 1),
    ]
    last = len(jobs) - 1
    ahead = 4

    def place(whole, shard, dim, owner, start, count):
        rows, cols = shard.shape
        if dim == 0:
            return whole.at[pl.ds(pl.multiple_of(owner * rows + start, 16), count), :]
        return whole.at[
            pl.ds(pl.multiple_of(start, 16), count),
            pl.ds(pl.multiple_of(owner * cols, 128), cols),
        ]

    square = n_fs == 4
    if square:
        near_x = f + 1 - 2 * lax.rem(f, 2)
        near_y = lax.rem(f + 2, 4)
        far = lax.rem(near_x + 2, 4)
        targets = sources = [near_x, near_y]
    else:
        targets = [lax.rem(f + k, n_fs) for k in range(1, n_fs)]
        sources = [lax.rem(f + n_fs - k, n_fs) for k in range(1, n_fs)]

    direct, far_copies, over_sp, own = [], [], [], []
    for a, (shard, whole, dim) in enumerate(jobs):
        rows = shard.shape[0]
        less = 0 if a == last else relayed_rows(rows, paired)
        start = parity * less
        count = rows - less
        direct.append([
            pltpu.make_async_remote_copy(
                src_ref=shard.at[pl.ds(pl.multiple_of(start, 16), count), :],
                dst_ref=place(whole, shard, dim, f, start, count),
                send_sem=send_d.at[a, k], recv_sem=recv_d.at[a, k],
                device_id={"fs": target}, device_id_type=MESH_ID,
            )
            for k, target in enumerate(targets)
        ])
        halves = []
        if square:
            half = (count // 2 + 15) // 16 * 16
            for k, (owner, target, begin, size) in enumerate((
                (near_y, near_x, start, half), (near_x, near_y, start + half, count - half)
            )):
                piece = place(whole, shard, dim, owner, begin, size)
                halves.append(pltpu.make_async_remote_copy(
                    src_ref=piece, dst_ref=piece,
                    send_sem=send_r.at[a, k], recv_sem=recv_r.at[a, k],
                    device_id={"fs": target}, device_id_type=MESH_ID,
                ))
        far_copies.append(halves)
        across = []
        if less:
            lack = parity * (rows - less)
            for k, owner in enumerate(sources + ([far] if square else [])):
                piece = place(whole, shard, dim, owner, lack, less)
                across.append(pltpu.make_async_remote_copy(
                    src_ref=piece, dst_ref=piece,
                    send_sem=send_z.at[a, k], recv_sem=recv_z.at[a, k],
                    device_id={"sp": partner}, device_id_type=MESH_ID,
                ))
        over_sp.append(across)
        own.append(pltpu.make_async_copy(
            shard, place(whole, shard, dim, f, 0, rows), local_sem.at[a]
        ))

    def begin_array(a):
        if a <= last:
            for copy in direct[a]:
                copy.start()

    def finish_far(a):
        for copy in far_copies[a]:
            copy.wait_recv()
        for copy in over_sp[a][len(sources):]:
            copy.start()

    def tick(a):
        for copy in direct[a]:
            copy.wait_recv()
        for copy in far_copies[a]:
            copy.start()
        begin_array(a + ahead)
        for copy in over_sp[a][: len(sources)]:
            copy.start()
        if a >= 1:
            finish_far(a - 1)

    def complete(a):
        own[a].wait()
        for copy in over_sp[a]:
            copy.wait_recv()

    for a in range(ahead):
        begin_array(a)
    for copy in own:
        copy.start()

    rows = x_ref.shape[0]
    part = 32

    @pl.loop(0, rows // part)
    def _(i):
        at = pl.ds(pl.multiple_of(i * part, part), part)
        x = x_ref[at, :].astype(jnp.float32)
        scale = lax.rsqrt(jnp.mean(x * x, axis=-1, keepdims=True) + epsilon)
        normed[at, :] = (x * scale * gain_ref[...]).astype(jnp.bfloat16)

    depth = qd.shape[0]

    def project(weight, acc):
        acc[...] = jnp.zeros_like(acc)

        @pl.loop(0, n_fs)
        def _(i):
            at = pl.ds(pl.multiple_of(i * depth, depth), depth)
            acc[...] += jnp.dot(
                normed[:, at], weight[at, :], preferred_element_type=jnp.float32
            )

    mine = pl.ds(pl.multiple_of(s * rows, 16), rows)
    rr_all[mine, :] = jnp.dot(
        normed[...], rope_ref[...], preferred_element_type=jnp.float32
    ).astype(jnp.bfloat16)
    tick(0)
    tick(1)
    tick(2)
    complete(0)
    project(qd_all, acc_q)
    lq_all[t, :, :] = acc_q[...].astype(jnp.bfloat16)
    tick(3)
    complete(1)
    project(md_all, acc_m)
    lm_all[t, mine, :] = acc_m[...].astype(jnp.bfloat16)
    tick(4)
    complete(2)
    project(cv_all, acc_v)

    exchanges, passes = [], []
    for k in range(1, n_sp):
        peer = {"sp": lax.rem(s + k, n_sp)}
        exchanges.append(pltpu.make_async_remote_copy(
            src_ref=lm_all.at[t, mine, :], dst_ref=lm_all.at[t, mine, :],
            send_sem=sp_send.at[k - 1], recv_sem=sp_recv.at[k - 1],
            device_id=peer, device_id_type=MESH_ID,
        ))
        exchanges.append(pltpu.make_async_remote_copy(
            src_ref=rr_all.at[mine, :], dst_ref=rr_all.at[mine, :],
            send_sem=rr_send.at[k - 1], recv_sem=rr_recv.at[k - 1],
            device_id=peer, device_id_type=MESH_ID,
        ))
    tp_peers = [{"tp": lax.rem(t + k, n_tp)} for k in range(1, n_tp)]

    def to_tp(kind, source, landing):
        return [
            pltpu.make_async_remote_copy(
                src_ref=source, dst_ref=landing(k),
                send_sem=tp_send.at[kind, k], recv_sem=tp_recv.at[kind, k],
                device_id=peer, device_id_type=MESH_ID,
            )
            for k, peer in enumerate(tp_peers)
        ]

    query_copies = to_tp(0, lq_all.at[t], lambda k: lq_all.at[t])
    memory_copies = to_tp(1, lm_all.at[t], lambda k: lm_all.at[t])
    stat_copies = to_tp(2, stats, lambda k: stats_all.at[k])
    for copy in exchanges + query_copies:
        copy.start()
    tick(5)
    complete(3)
    project(cg_all, acc_g)

    @pl.loop(0, rows // part)
    def _(i):
        at = pl.ds(pl.multiple_of(i * part, part), part)
        gated = (acc_v[at, :] * jax.nn.sigmoid(acc_g[at, :])).astype(jnp.bfloat16)
        ext[pl.ds(pl.multiple_of(RIM + i * part, part), part), :] = gated.astype(jnp.float32)

    tail[...] = ext[pl.ds(rows, RIM), :].astype(jnp.bfloat16)
    rim_copy = pltpu.make_async_remote_copy(
        src_ref=tail, dst_ref=rim, send_sem=rim_sem.at[0], recv_sem=rim_sem.at[1],
        device_id={"sp": lax.rem(s + 1, n_sp)}, device_id_type=MESH_ID,
    )
    tick(6)

    @pl.when(s < n_sp - 1)
    def _():
        rim_copy.start()

    for copy in exchanges:
        copy.wait_recv()
    for copy in memory_copies:
        copy.start()

    @pl.when(s > 0)
    def _():
        rim_copy.wait_recv()
        ext[pl.ds(0, RIM), :] = rim[...].astype(jnp.float32)

    @pl.when(s == 0)
    def _():
        ext[pl.ds(0, RIM), :] = jnp.zeros((RIM, ext.shape[1]), jnp.float32)

    tap_count = taps_ref.shape[0]
    block = 64

    def convolve(c):
        cols = pl.ds(pl.multiple_of(c * 128, 128), 128)
        taps = taps_ref[:, cols].astype(jnp.float32)
        for r in range(0, rows, block):
            total = jnp.zeros((block, 128), jnp.float32)
            for j in range(tap_count):
                total = total + ext[
                    pl.ds(r + RIM - (tap_count - 1) + j, block), cols
                ] * taps[j : j + 1, :]
            sums[pl.ds(r, block), cols] = total

    tiles = ext.shape[1] // 128
    pl.loop(0, tiles // 2)(convolve)
    tick(7)
    pl.loop(tiles // 2, tiles)(convolve)

    @pl.loop(0, rows // part)
    def _(i):
        begin = pl.multiple_of(i * part, part)
        values = sums[pl.ds(begin, part), :]
        stats[pl.ds(begin, part), :] = jnp.broadcast_to(
            jnp.sum(values, axis=1, keepdims=True), (part, 128)
        )
        stats[pl.ds(pl.multiple_of(rows + begin, part), part), :] = jnp.broadcast_to(
            jnp.sum(values * values, axis=1, keepdims=True), (part, 128)
        )

    tick(8)
    for copy in stat_copies:
        copy.start()
    for copy in stat_copies:
        copy.wait_recv()

    channels = ext.shape[1] * n_tp

    @pl.loop(0, rows // part)
    def _(i):
        begin = pl.multiple_of(i * part, part)
        upper = pl.ds(begin, part)
        lower = pl.ds(pl.multiple_of(rows + begin, part), part)
        total, squares = stats[upper, :], stats[lower, :]
        for k in range(n_tp - 1):
            total = total + stats_all[k, upper, :]
            squares = squares + stats_all[k, lower, :]
        mean = total[:, :1] / channels
        spread = squares[:, :1] / channels - mean * mean
        shaped = (sums[upper, :] - mean) * lax.rsqrt(spread + epsilon)
        conv_ref[upper, :] = jax.nn.silu(
            shaped * cgain_ref[...] + cshift_ref[...]
        ).astype(jnp.bfloat16)

    finish_far(last)
    for a in range(4, last + 1):
        complete(a)
    for copy in query_copies + memory_copies:
        copy.wait_recv()
    for group in direct + far_copies + over_sp:
        for copy in group:
            copy.wait_send()
    for copy in exchanges + query_copies + memory_copies + stat_copies:
        copy.wait_send()

    @pl.when(s < n_sp - 1)
    def _():
        rim_copy.wait_send()


def gather_and_project(
    sizes, x, mix_gain, rope_weight, taps, channel_gain, channel_shift,
    qd, md, cv, cg, qu, ku, vu, ho, co,
):
    n_fs, n_sp, n_tp = sizes
    rows = x.shape[0]
    bf16, f32 = jnp.bfloat16, jnp.float32
    vmem = pl.BlockSpec(memory_space=pltpu.VMEM)
    hbm = pl.BlockSpec(memory_space=pl.ANY)

    def whole(w, dim=0):
        return (w.shape[0] * n_fs, w.shape[1]) if dim == 0 else (w.shape[0], w.shape[1] * n_fs)

    out_shapes = [
        ((n_tp, rows, qd.shape[1]), bf16), ((n_tp, n_sp * rows, md.shape[1]), bf16),
        ((n_sp * rows, rope_weight.shape[1]), bf16), ((rows, cv.shape[1]), bf16),
        (whole(qu), bf16), (whole(ku), bf16), (whole(vu), bf16),
        (whole(ho, 1), bf16), (whole(co, 1), bf16),
    ]
    dma = pltpu.SemaphoreType.DMA
    tp_others = max(n_tp - 1, 1)
    sp_others = max(n_sp - 1, 1)
    return pl.pallas_call(
        functools.partial(gather_kernel, sizes),
        out_shape=[jax.ShapeDtypeStruct(*o) for o in out_shapes],
        in_specs=[vmem] * 6 + [hbm] * 9,
        out_specs=[vmem] * 9,
        scratch_shapes=[
            pltpu.VMEM(whole(qd), bf16), pltpu.VMEM(whole(md), bf16),
            pltpu.VMEM(whole(cv), bf16), pltpu.VMEM(whole(cg), bf16),
            pltpu.VMEM(x.shape, bf16), pltpu.VMEM((rows, qd.shape[1]), f32),
            pltpu.VMEM((rows, md.shape[1]), f32),
            pltpu.VMEM((rows, cv.shape[1]), f32), pltpu.VMEM((rows, cv.shape[1]), f32),
            pltpu.VMEM((rows + RIM, cv.shape[1]), f32),
            pltpu.VMEM((RIM, cv.shape[1]), bf16), pltpu.VMEM((RIM, cv.shape[1]), bf16),
            pltpu.VMEM((rows, cv.shape[1]), f32), pltpu.VMEM((2 * rows, 128), f32),
            pltpu.VMEM((tp_others, 2 * rows, 128), f32),
            dma((9, n_fs - 1)), dma((9, n_fs - 1)), dma((9, 2)), dma((9, 2)),
            dma((9, n_fs - 1)), dma((9, n_fs - 1)), dma((9,)), dma((2,)),
            dma((sp_others,)), dma((sp_others,)), dma((sp_others,)), dma((sp_others,)),
            dma((3, tp_others)), dma((3, tp_others)),
        ],
        compiler_params=pltpu.CompilerParams(
            collective_id=0, has_side_effects=True, vmem_limit_bytes=56 * 1024 * 1024
        ),
    )(
        x, mix_gain[None, :], rope_weight, taps, channel_gain[None, :], channel_shift[None, :],
        qd, md, cv, cg, qu, ku, vu, ho, co,
    )


def key_block(key_count):
    block_size = key_count
    while block_size > 2048 and block_size % 2 == 0:
        block_size = block_size // 2
    return block_size


def sum_groups(partial):
    count = lax.axis_size("tp")
    if count != 2:
        return lax.psum(partial, "tp")
    other = lax.ppermute(partial, "tp", [(0, 1), (1, 0)])
    return (partial.astype(jnp.float32) + other.astype(jnp.float32)).astype(jnp.bfloat16)


def local(
    tokens,
    mix_gain,
    query_down,
    memory_down,
    rope_weight,
    query_up,
    key_up,
    value_up,
    latent_gain,
    memory_gain,
    query_gain,
    key_gain,
    conv_value,
    conv_gate,
    conv_kernel,
    channel_gain,
    channel_shift,
    heads_out,
    conv_out,
):
    own_rows = tokens[0]
    (
        query_parts, memory_parts, rope_piece, conv_result,
        up_query, up_keys, up_values, out_heads, out_conv,
    ) = gather_and_project(
        (lax.axis_size("fs"), lax.axis_size("sp"), lax.axis_size("tp")),
        own_rows, mix_gain, rope_weight, conv_kernel, channel_gain, channel_shift,
        query_down, memory_down, conv_value, conv_gate,
        query_up, key_up, value_up, heads_out, conv_out,
    )
    row_count = own_rows.shape[0]
    whole_query = jnp.concatenate(list(query_parts), axis=1)
    whole_memory = jnp.concatenate(list(memory_parts), axis=1)
    query_normed = norm_rows(whole_query.astype(jnp.float32), latent_gain).astype(jnp.bfloat16)
    memory_piece = norm_rows(whole_memory.astype(jnp.float32), memory_gain).astype(jnp.bfloat16)
    positions = lax.axis_index("sp") * row_count + jnp.arange(row_count, dtype=jnp.int32)
    cosine_table, sine_table = rope_tables(positions)
    queries = heads_query(query_normed, up_query, query_gain, cosine_table, sine_table)
    head_count = queries.shape[1]
    query_segment = positions // SEG
    score_scale = QK_DIM ** (-0.5)
    def attend(state_carry, key_rows, value_rows, key_pos):
        running_max, row_total, weighted = state_carry
        scores = (
            jnp.einsum("qhd,khd->qhk", queries, key_rows, preferred_element_type=jnp.float32)
            * score_scale
        )
        allowed = ((key_pos // SEG)[None, :] <= query_segment[:, None])[:, None, :]
        scores = jnp.where(allowed, scores, masked_score)
        new_max = jnp.maximum(running_max, jnp.max(scores, axis=2))
        weights = jnp.where(allowed, jnp.exp(scores - new_max[:, :, None]), 0.0)
        factor = jnp.exp(running_max - new_max)
        row_total = row_total * factor + jnp.sum(weights, axis=2)
        weighted = weighted * factor[:, :, None] + jnp.einsum(
            "qhk,khd->qhd",
            weights.astype(jnp.bfloat16),
            value_rows,
            preferred_element_type=jnp.float32,
        )
        return (new_max, row_total, weighted)

    initial = (
        jnp.full((row_count, head_count), masked_score, jnp.float32),
        jnp.zeros((row_count, head_count), jnp.float32),
        jnp.zeros((row_count, head_count, V_DIM), jnp.float32),
    )
    def block_keys(block_start, block_size):
        memory_block = lax.dynamic_slice_in_dim(memory_piece, block_start, block_size, 0)
        rope_block = lax.dynamic_slice_in_dim(rope_piece, block_start, block_size, 0)
        key_pos = block_start + jnp.arange(block_size, dtype=jnp.int32)
        cosine_keys, sine_keys = rope_tables(key_pos)
        key_rows = heads_key(memory_block, rope_block, up_keys, key_gain, cosine_keys, sine_keys)
        value_rows = (
            jnp.dot(memory_block, up_values, preferred_element_type=jnp.float32)
            .astype(jnp.bfloat16)
            .reshape(block_size, head_count, V_DIM)
        )
        return (key_rows, value_rows, key_pos)

    key_count = memory_piece.shape[0]
    block_size = key_block(key_count)

    def step(block_index, running):
        key_rows, value_rows, key_pos = block_keys(block_index * block_size, block_size)
        return attend(running, key_rows, value_rows, key_pos)

    final_state = lax.fori_loop(0, key_count // block_size, step, initial)
    running_max, row_total, weighted = final_state
    attention = (
        (weighted / row_total[:, :, None])
        .astype(jnp.bfloat16)
        .reshape(row_count, head_count * V_DIM)
    )
    mixer_rows = jnp.concatenate([attention, conv_result], axis=1)
    out_weight = jnp.concatenate([out_heads, out_conv], axis=0)
    partial_sum = jnp.dot(mixer_rows, out_weight, preferred_element_type=jnp.float32)
    mixed = sum_groups(partial_sum.astype(jnp.bfloat16))
    return mixed[None]


def table_rows(count):
    inverse_freq = 1.0 / np.float32(rope_base) ** (
        np.arange(0, QK_ROPE, 2, dtype=np.float32) / np.float32(QK_ROPE)
    )
    angles = inverse_freq[:, None] * np.arange(count, dtype=np.float32)[None, :]
    angles = angles.astype(np.float64)
    return np.cos(angles).astype(np.float32), np.sin(angles).astype(np.float32)


def dot_heads(left, right):
    return lax.dot_general(
        left, right, (((0,), (0,)), ((), ())), preferred_element_type=jnp.float32
    )


def fused_kernel(
    sizes,
    x_ref, gain_ref, rope_ref, taps_ref, cgain_ref, cshift_ref,
    lgain_ref, mgain_ref, qgain_ref, kgain_ref, cos_ref, sin_ref,
    md, qd, ku, vu, qu, cv, cg, ho, co,
    mine_ref, other_ref,
    md_all, qd_all, ku_all, vu_all, qu_all, cv_all, cg_all, ho_all, co_all,
    normed, lq_all, lm_all, mem_all, rr_all, qn_t, q_t, k_t, v_t, turned, ropesq, bias, scores,
    att_t, conv_s, acc_v, acc_g, acc_out, ext, tail, rim, sums, stats, stats_all,
    send_d, recv_d, send_r, recv_r, send_z, recv_z, local_sem, rim_sem,
    sp_send, sp_recv, rr_send, rr_recv, fw_send, fw_recv, tp_send, tp_recv, out_send, out_recv,
):
    n_fs, n_sp, n_tp = sizes
    f = lax.axis_index("fs")
    s = lax.axis_index("sp")
    t = lax.axis_index("tp")
    parity = lax.rem(s, 2)
    partner = s + 1 - 2 * parity
    twin = {"tp": 1 - t}

    barrier = pltpu.get_barrier_semaphore()
    for axis, at, count in (("fs", f, n_fs), ("sp", s, n_sp), ("tp", t, n_tp)):
        for k in range(1, count):
            pl.semaphore_signal(
                barrier, inc=1, device_id={axis: lax.rem(at + k, count)}, device_id_type=MESH_ID
            )
    pl.semaphore_wait(barrier, n_fs + n_sp + n_tp - 3)

    jobs = [
        (md, md_all, 0), (qd, qd_all, 0), (ku, ku_all, 0), (vu, vu_all, 0), (qu, qu_all, 0),
        (cv, cv_all, 0), (cg, cg_all, 0), (ho, ho_all, 1), (co, co_all, 1),
    ]
    last = len(jobs) - 1
    ahead = 4

    def place(whole, shard, dim, owner, start, count):
        rows, cols = shard.shape
        if dim == 0:
            return whole.at[pl.ds(pl.multiple_of(owner * rows + start, 16), count), :]
        return whole.at[
            pl.ds(pl.multiple_of(start, 16), count),
            pl.ds(pl.multiple_of(owner * cols, 128), cols),
        ]

    near_x = f + 1 - 2 * lax.rem(f, 2)
    near_y = lax.rem(f + 2, 4)
    far = lax.rem(near_x + 2, 4)
    sources = [near_x, near_y]

    direct, far_copies, over_sp, own = [], [], [], []
    for a, (shard, whole, dim) in enumerate(jobs):
        rows = shard.shape[0]
        less = 0 if a == last else relayed_rows(rows, True)
        start = parity * less
        count = rows - less
        direct.append([
            pltpu.make_async_remote_copy(
                src_ref=shard.at[pl.ds(pl.multiple_of(start, 16), count), :],
                dst_ref=place(whole, shard, dim, f, start, count),
                send_sem=send_d.at[a, k], recv_sem=recv_d.at[a, k],
                device_id={"fs": target}, device_id_type=MESH_ID,
            )
            for k, target in enumerate(sources)
        ])
        halves = []
        half = (count // 2 + 15) // 16 * 16
        for k, (owner, target, begin, size) in enumerate((
            (near_y, near_x, start, half), (near_x, near_y, start + half, count - half)
        )):
            piece = place(whole, shard, dim, owner, begin, size)
            halves.append(pltpu.make_async_remote_copy(
                src_ref=piece, dst_ref=piece,
                send_sem=send_r.at[a, k], recv_sem=recv_r.at[a, k],
                device_id={"fs": target}, device_id_type=MESH_ID,
            ))
        far_copies.append(halves)
        across = []
        if less:
            lack = parity * (rows - less)
            for k, owner in enumerate(sources + [far]):
                piece = place(whole, shard, dim, owner, lack, less)
                across.append(pltpu.make_async_remote_copy(
                    src_ref=piece, dst_ref=piece,
                    send_sem=send_z.at[a, k], recv_sem=recv_z.at[a, k],
                    device_id={"sp": partner}, device_id_type=MESH_ID,
                ))
        over_sp.append(across)
        own.append(pltpu.make_async_copy(
            shard, place(whole, shard, dim, f, 0, rows), local_sem.at[a]
        ))

    def begin_array(a):
        if a <= last:
            for copy in direct[a]:
                copy.start()

    def finish_far(a):
        for copy in far_copies[a]:
            copy.wait_recv()
        for copy in over_sp[a][len(sources):]:
            copy.start()

    def tick(a):
        for copy in direct[a]:
            copy.wait_recv()
        for copy in far_copies[a]:
            copy.start()
        begin_array(a + ahead)
        for copy in over_sp[a][: len(sources)]:
            copy.start()
        if a >= 1:
            finish_far(a - 1)

    def complete(a):
        own[a].wait()
        for copy in over_sp[a]:
            copy.wait_recv()

    for a in range(ahead):
        begin_array(a)
    for copy in own:
        copy.start()

    rows = x_ref.shape[0]
    part = 32

    @pl.loop(0, rows // part)
    def _(i):
        at = pl.ds(pl.multiple_of(i * part, part), part)
        x = x_ref[at, :].astype(jnp.float32)
        scale = lax.rsqrt(jnp.mean(x * x, axis=-1, keepdims=True) + epsilon)
        normed[at, :] = (x * scale * gain_ref[...]).astype(jnp.bfloat16)

    depth = qd.shape[0]

    def project(weight, acc):
        acc[...] = jnp.zeros_like(acc)

        @pl.loop(0, n_fs)
        def _(i):
            at = pl.ds(pl.multiple_of(i * depth, depth), depth)
            acc[...] += jnp.dot(
                normed[:, at], weight[at, :], preferred_element_type=jnp.float32
            )

    rr_all[s] = lax.dot_general(
        rope_ref[...], normed[...], (((1,), (1,)), ((), ())), preferred_element_type=jnp.float32
    ).astype(jnp.bfloat16)

    half_rope = QK_ROPE // 2

    @pl.loop(s + 1, n_sp)
    def _(j):
        mem_all[j] = jnp.zeros(mem_all.shape[1:], jnp.bfloat16)
        rr_all[j] = jnp.zeros(rr_all.shape[1:], jnp.bfloat16)

    @pl.loop(0, n_sp)
    def _(j):
        key_at = j * rows + lax.broadcasted_iota(jnp.int32, (rows, rows), 0)
        query_at = s * rows + lax.broadcasted_iota(jnp.int32, (rows, rows), 1)
        bias[j] = jnp.where(
            lax.div(key_at, SEG) <= lax.div(query_at, SEG), 0.0, masked_score
        )

    def to_twin(kind, source, landing):
        return pltpu.make_async_remote_copy(
            src_ref=source, dst_ref=landing,
            send_sem=tp_send.at[kind], recv_sem=tp_recv.at[kind],
            device_id=twin, device_id_type=MESH_ID,
        )

    query_copy = to_twin(0, lq_all.at[t], lq_all.at[t])
    memory_copy = to_twin(1, lm_all.at[t], lm_all.at[t])
    stat_copy = to_twin(2, stats, stats_all)

    lat = md.shape[1]
    held = pl.ds(pl.multiple_of(t * lat, lat), lat)
    sends, forwards = [], []
    for k in range(1, n_sp):
        peer = {"sp": lax.rem(s + k, n_sp)}
        sends.append([
            pltpu.make_async_remote_copy(
                src_ref=mem_all.at[s, held, :], dst_ref=mem_all.at[s, held, :],
                send_sem=sp_send.at[k - 1], recv_sem=sp_recv.at[k - 1],
                device_id=peer, device_id_type=MESH_ID,
            ),
            pltpu.make_async_remote_copy(
                src_ref=rr_all.at[s], dst_ref=rr_all.at[s],
                send_sem=rr_send.at[k - 1], recv_sem=rr_recv.at[k - 1],
                device_id=peer, device_id_type=MESH_ID,
            ),
        ])
        behind = mem_all.at[lax.rem(s + n_sp - k, n_sp), held, :]
        forwards.append(pltpu.make_async_remote_copy(
            src_ref=behind, dst_ref=behind,
            send_sem=fw_send.at[k - 1], recv_sem=fw_recv.at[k - 1],
            device_id=twin, device_id_type=MESH_ID,
        ))

    tick(0)
    tick(1)
    tick(2)
    complete(0)
    project(md_all, acc_v.at[:, pl.ds(0, lat)])
    lm_all[t, :, :] = acc_v[:, :lat].astype(jnp.bfloat16)
    memory_copy.start()
    tick(3)
    complete(1)
    wide = qd.shape[1]
    project(qd_all, acc_g.at[:, pl.ds(0, wide)])
    lq_all[t, :, :] = acc_g[:, :wide].astype(jnp.bfloat16)
    query_copy.start()

    def normed_columns(parts, gains, put):
        width = parts.shape[2]

        @pl.loop(0, rows // 128)
        def _(i):
            at = pl.ds(pl.multiple_of(i * 128, 128), 128)
            pieces = [parts[g, at, :].astype(jnp.float32) for g in range(n_tp)]
            total = sum(jnp.sum(p * p, axis=-1, keepdims=True) for p in pieces)
            scale = lax.rsqrt(total / (width * n_tp) + epsilon)
            for g in range(n_tp):
                gain = gains[:, g * width : (g + 1) * width]
                shaped = (pieces[g] * scale * gain).astype(jnp.bfloat16)
                put(g * width, width, at, shaped.astype(jnp.float32).T.astype(jnp.bfloat16))

    def put_memory(begin, width, at, piece):
        mem_all[s, begin : begin + width, at] = piece

    def put_query(begin, width, at, piece):
        qn_t[begin : begin + width, at] = piece

    memory_copy.wait_recv()
    normed_columns(lm_all, mgain_ref, put_memory)
    for k in range(1, n_sp):
        @pl.when(s + k < n_sp)
        def _(k=k):
            for copy in sends[k - 1]:
                copy.start()

    tick(4)
    query_copy.wait_recv()
    normed_columns(lq_all, lgain_ref, put_query)
    complete(2)
    tick(5)
    complete(3)

    for k in range(1, n_sp):
        @pl.when(s >= k)
        def _(k=k):
            for copy in sends[k - 1]:
                copy.wait_recv()
            forwards[k - 1].start()
    for k in range(1, n_sp):
        @pl.when(s >= k)
        def _(k=k):
            forwards[k - 1].wait_recv()

    @pl.loop(0, n_sp)
    def _(j):
        k_t[j] = dot_heads(ku_all[...], mem_all[j])
        v_t[j] = dot_heads(vu_all[...], mem_all[j]).astype(jnp.bfloat16)
        shared = rr_all[j].astype(jnp.float32)
        ropesq[j] = jnp.sum(shared * shared, axis=0, keepdims=True)
        shared = shared * kgain_ref[QK_NOPE:, :]
        front, back = shared[:half_rope], shared[half_rope:]
        at = pl.ds(pl.multiple_of(j * rows, rows), rows)
        cosine, sine = cos_ref[:, at], sin_ref[:, at]
        turned[j] = jnp.concatenate(
            [front * cosine - back * sine, front * sine + back * cosine], axis=0
        )

    tick(6)
    complete(4)
    q_t[...] = dot_heads(qu_all[...], qn_t[...])
    heads = qu.shape[1] // QK_DIM
    here = pl.ds(pl.multiple_of(s * rows, rows), rows)
    score_scale = QK_DIM ** (-0.5)

    def head(h):
        q = q_t[pl.ds(pl.multiple_of(h * QK_DIM, QK_DIM), QK_DIM), :]
        q = q * lax.rsqrt(jnp.mean(q * q, axis=0, keepdims=True) + epsilon) * qgain_ref[...]
        front, back = q[QK_NOPE : QK_NOPE + half_rope], q[QK_NOPE + half_rope :]
        cosine, sine = cos_ref[:, here], sin_ref[:, here]
        q = jnp.concatenate(
            [q[:QK_NOPE], front * cosine - back * sine, front * sine + back * cosine], axis=0
        ).astype(jnp.bfloat16)
        krow = pl.ds(pl.multiple_of(h * QK_NOPE, QK_NOPE), QK_NOPE)
        vrow = pl.ds(pl.multiple_of(h * V_DIM, V_DIM), V_DIM)
        top = jnp.full((1, rows), masked_score, jnp.float32)
        for j in range(n_sp):
            nope = k_t[j, krow, :]
            scale = lax.rsqrt(
                (jnp.sum(nope * nope, axis=0, keepdims=True) + ropesq[j]) / QK_DIM + epsilon
            )
            key = jnp.concatenate(
                [nope * scale * kgain_ref[:QK_NOPE, :], turned[j] * scale], axis=0
            ).astype(jnp.bfloat16)
            block = dot_heads(key, q) + bias[j]
            scores[j] = block
            top = jnp.maximum(top, jnp.max(block, axis=0, keepdims=True))
        total = jnp.zeros((1, rows), jnp.float32)
        summed = jnp.zeros((V_DIM, rows), jnp.float32)
        for j in range(n_sp):
            weight = jnp.exp((scores[j] - top) * score_scale)
            total = total + jnp.sum(weight, axis=0, keepdims=True)
            summed = summed + jnp.dot(
                v_t[j, vrow, :], weight.astype(jnp.bfloat16),
                preferred_element_type=jnp.float32,
            )
        att_t[vrow, :] = summed / total

    pl.loop(0, heads // 2)(head)
    tick(7)
    pl.loop(heads // 2, heads)(head)
    complete(5)
    project(cv_all, acc_v)
    tick(8)
    complete(6)
    project(cg_all, acc_g)

    @pl.loop(0, rows // part)
    def _(i):
        at = pl.ds(pl.multiple_of(i * part, part), part)
        gated = (acc_v[at, :] * jax.nn.sigmoid(acc_g[at, :])).astype(jnp.bfloat16)
        ext[pl.ds(pl.multiple_of(RIM + i * part, part), part), :] = gated.astype(jnp.float32)

    tail[...] = ext[pl.ds(rows, RIM), :].astype(jnp.bfloat16)
    rim_copy = pltpu.make_async_remote_copy(
        src_ref=tail, dst_ref=rim, send_sem=rim_sem.at[0], recv_sem=rim_sem.at[1],
        device_id={"sp": lax.rem(s + 1, n_sp)}, device_id_type=MESH_ID,
    )

    @pl.when(s < n_sp - 1)
    def _():
        rim_copy.start()

    @pl.when(s > 0)
    def _():
        rim_copy.wait_recv()
        ext[pl.ds(0, RIM), :] = rim[...].astype(jnp.float32)

    @pl.when(s == 0)
    def _():
        ext[pl.ds(0, RIM), :] = jnp.zeros((RIM, ext.shape[1]), jnp.float32)

    tap_count = taps_ref.shape[0]
    block = 64

    def convolve(c):
        cols = pl.ds(pl.multiple_of(c * 128, 128), 128)
        taps = taps_ref[:, cols].astype(jnp.float32)
        for r in range(0, rows, block):
            total = jnp.zeros((block, 128), jnp.float32)
            for j in range(tap_count):
                total = total + ext[
                    pl.ds(r + RIM - (tap_count - 1) + j, block), cols
                ] * taps[j : j + 1, :]
            sums[pl.ds(r, block), cols] = total

    tiles = ext.shape[1] // 128
    pl.loop(0, tiles)(convolve)
    finish_far(last)

    @pl.loop(0, rows // part)
    def _(i):
        begin = pl.multiple_of(i * part, part)
        values = sums[pl.ds(begin, part), :]
        stats[pl.ds(begin, part), :] = jnp.broadcast_to(
            jnp.sum(values, axis=1, keepdims=True), (part, 128)
        )
        stats[pl.ds(pl.multiple_of(rows + begin, part), part), :] = jnp.broadcast_to(
            jnp.sum(values * values, axis=1, keepdims=True), (part, 128)
        )

    stat_copy.start()
    complete(7)
    att = att_t[...].T.astype(jnp.bfloat16)
    span = ho.shape[1]

    @pl.loop(0, n_fs)
    def _(i):
        cols = pl.ds(pl.multiple_of(i * span, span), span)
        acc_out[:, cols] = jnp.dot(att, ho_all[:, cols], preferred_element_type=jnp.float32)

    stat_copy.wait_recv()
    channels = ext.shape[1] * n_tp

    @pl.loop(0, rows // part)
    def _(i):
        begin = pl.multiple_of(i * part, part)
        upper = pl.ds(begin, part)
        lower = pl.ds(pl.multiple_of(rows + begin, part), part)
        total = stats[upper, :] + stats_all[upper, :]
        squares = stats[lower, :] + stats_all[lower, :]
        mean = total[:, :1] / channels
        spread = squares[:, :1] / channels - mean * mean
        shaped = (sums[upper, :] - mean) * lax.rsqrt(spread + epsilon)
        conv_s[upper, :] = jax.nn.silu(
            shaped * cgain_ref[...] + cshift_ref[...]
        ).astype(jnp.bfloat16)

    complete(8)
    outs = []
    for i in range(n_fs):
        cols = slice(i * span, (i + 1) * span)
        outs.append(pltpu.make_async_remote_copy(
            src_ref=mine_ref.at[:, cols], dst_ref=other_ref.at[:, cols],
            send_sem=out_send.at[i], recv_sem=out_recv.at[i],
            device_id=twin, device_id_type=MESH_ID,
        ))
        mine_ref[:, cols] = (
            acc_out[:, cols]
            + jnp.dot(conv_s[...], co_all[:, cols], preferred_element_type=jnp.float32)
        ).astype(jnp.bfloat16)
        outs[i].start()

    for group in direct + far_copies + over_sp:
        for copy in group:
            copy.wait_send()
    for copy in [query_copy, memory_copy, stat_copy]:
        copy.wait_send()
    for k in range(1, n_sp):
        @pl.when(s + k < n_sp)
        def _(k=k):
            for copy in sends[k - 1]:
                copy.wait_send()

        @pl.when(s >= k)
        def _(k=k):
            forwards[k - 1].wait_send()

    @pl.when(s < n_sp - 1)
    def _():
        rim_copy.wait_send()

    for copy in outs:
        copy.wait()


def fused_call(
    sizes, x, mix_gain, rope_weight, taps, channel_gain, channel_shift,
    latent_gain, memory_gain, query_gain, key_gain,
    qd, md, cv, cg, qu, ku, vu, ho, co,
):
    n_fs, n_sp, n_tp = sizes
    rows, model = x.shape
    bf16, f32 = jnp.bfloat16, jnp.float32
    vmem = pl.BlockSpec(memory_space=pltpu.VMEM)
    hbm = pl.BlockSpec(memory_space=pl.ANY)
    cosine, sine = table_rows(n_sp * rows)

    def whole(w, dim=0):
        return (w.shape[0] * n_fs, w.shape[1]) if dim == 0 else (w.shape[0], w.shape[1] * n_fs)

    def scratch(*shape, dtype=f32):
        return pltpu.VMEM(shape, dtype)

    dma = pltpu.SemaphoreType.DMA
    channels, lat = cv.shape[1], md.shape[1] * n_tp
    rope = rope_weight.shape[1]
    others = n_sp - 1
    return pl.pallas_call(
        functools.partial(fused_kernel, sizes),
        out_shape=[jax.ShapeDtypeStruct((rows, ho.shape[1] * n_fs), bf16)] * 2,
        in_specs=[vmem] * 12 + [hbm] * 9,
        out_specs=[vmem] * 2,
        scratch_shapes=[
            scratch(*whole(md), dtype=bf16), scratch(*whole(qd), dtype=bf16),
            scratch(*whole(ku), dtype=bf16), scratch(*whole(vu), dtype=bf16),
            scratch(*whole(qu), dtype=bf16), scratch(*whole(cv), dtype=bf16),
            scratch(*whole(cg), dtype=bf16), scratch(*whole(ho, 1), dtype=bf16),
            scratch(*whole(co, 1), dtype=bf16),
            scratch(rows, model, dtype=bf16), scratch(n_tp, rows, qd.shape[1], dtype=bf16),
            scratch(n_tp, rows, md.shape[1], dtype=bf16),
            scratch(n_sp, lat, rows, dtype=bf16), scratch(n_sp, rope, rows, dtype=bf16),
            scratch(qu.shape[0] * n_fs, rows, dtype=bf16), scratch(qu.shape[1], rows),
            scratch(n_sp, ku.shape[1], rows), scratch(n_sp, vu.shape[1], rows, dtype=bf16),
            scratch(n_sp, rope, rows), scratch(n_sp, 1, rows),
            scratch(n_sp, rows, rows), scratch(n_sp, rows, rows),
            scratch(vu.shape[1], rows), scratch(rows, channels, dtype=bf16),
            scratch(rows, channels), scratch(rows, channels),
            scratch(rows, ho.shape[1] * n_fs),
            scratch(rows + RIM, channels), scratch(RIM, channels, dtype=bf16),
            scratch(RIM, channels, dtype=bf16), scratch(rows, channels),
            scratch(2 * rows, 128), scratch(2 * rows, 128),
            dma((9, 2)), dma((9, 2)), dma((9, 2)), dma((9, 2)),
            dma((9, 3)), dma((9, 3)), dma((9,)), dma((2,)),
            dma((others,)), dma((others,)), dma((others,)), dma((others,)),
            dma((others,)), dma((others,)), dma((3,)), dma((3,)), dma((n_fs,)), dma((n_fs,)),
        ],
        compiler_params=pltpu.CompilerParams(
            collective_id=1, has_side_effects=True, vmem_limit_bytes=60 * 1024 * 1024
        ),
    )(
        x, mix_gain[None, :], rope_weight.T, taps, channel_gain[None, :], channel_shift[None, :],
        latent_gain[None, :], memory_gain[None, :], query_gain[:, None], key_gain[:, None],
        jnp.asarray(cosine), jnp.asarray(sine),
        md, qd, ku, vu, qu, cv, cg, ho, co,
    )


def fused_local(
    tokens, mix_gain, query_down, memory_down, rope_weight, query_up, key_up, value_up,
    latent_gain, memory_gain, query_gain, key_gain, conv_value, conv_gate, conv_kernel,
    channel_gain, channel_shift, heads_out, conv_out,
):
    mine, other = fused_call(
        (lax.axis_size("fs"), lax.axis_size("sp"), lax.axis_size("tp")),
        tokens[0], mix_gain, rope_weight, conv_kernel, channel_gain, channel_shift,
        latent_gain, memory_gain, query_gain, key_gain,
        query_down, memory_down, conv_value, conv_gate,
        query_up, key_up, value_up, heads_out, conv_out,
    )
    return (mine.astype(jnp.float32) + other.astype(jnp.float32)).astype(jnp.bfloat16)[None]


def solution(mesh):
    in_specs = (
        P("fs", "sp", None),
        P(),
        P("fs", "tp"),
        P("fs", "tp"),
        P(),
        P("fs", "tp"),
        P("fs", "tp"),
        P("fs", "tp"),
        P(),
        P(),
        P(),
        P(),
        P("fs", "tp"),
        P("fs", "tp"),
        P(None, "tp"),
        P("tp"),
        P("tp"),
        P("tp", "fs"),
        P("tp", "fs"),
    )
    out_specs = P("fs", "sp", None)
    n_fs, n_sp, n_tp = (mesh.shape[axis] for axis in ("fs", "sp", "tp"))
    fits = n_fs == 4 and n_tp == 2 and n_sp in (2, 4)
    body = fused_local if fits else local
    return jax.shard_map(body, mesh=mesh, in_specs=in_specs, out_specs=out_specs, check_vma=False)
```

```python
import functools

import jax
import jax.numpy as jnp
import numpy as np
from jax import lax
from jax.experimental import pallas as pl
from jax.experimental.pallas import tpu as pltpu
from jax.sharding import PartitionSpec as P

MESH_ID = pl.DeviceIdType.MESH

QK_NOPE = 64
QK_ROPE = 32
V_DIM = 64
CONV_W = 1024
SEG = 64
QK_DIM = 96


epsilon = 1e-06
rope_base = 10000.0
masked_score = -1e30


def norm_rows(matrix, scale_vector):
    return (
        matrix
        * lax.rsqrt(jnp.mean(matrix * matrix, axis=-1, keepdims=True) + epsilon)
        * scale_vector
    )


def rope_tables(positions):
    inverse_freq = 1.0 / rope_base ** (jnp.arange(0, QK_ROPE, 2, dtype=jnp.float32) / QK_ROPE)
    angles = positions.astype(jnp.float32)[:, None] * inverse_freq[None, :]
    return (jnp.cos(angles)[:, None, :], jnp.sin(angles)[:, None, :])


def rotate(matrix, cosine_table, sine_table):
    half_width = matrix.shape[-1] // 2
    front_half = matrix[..., :half_width]
    back_half = matrix[..., half_width:]
    return jnp.concatenate(
        [
            front_half * cosine_table - back_half * sine_table,
            front_half * sine_table + back_half * cosine_table,
        ],
        axis=-1,
    )


def heads_query(latent, weight, scale_vector, cosine_table, sine_table):
    row_count = latent.shape[0]
    projected = jnp.dot(latent, weight, preferred_element_type=jnp.float32)
    projected = norm_rows(
        projected.reshape(row_count, weight.shape[1] // QK_DIM, QK_DIM), scale_vector
    )
    turned = rotate(projected[..., QK_NOPE:], cosine_table, sine_table)
    return jnp.concatenate([projected[..., :QK_NOPE], turned], axis=-1).astype(jnp.bfloat16)


def heads_key(latent, rope_rows, weight, scale_vector, cosine_table, sine_table):
    row_count = latent.shape[0]
    head_count = weight.shape[1] // QK_NOPE
    nope_part = jnp.dot(latent, weight, preferred_element_type=jnp.float32).reshape(
        row_count, head_count, QK_NOPE
    )
    shared = jnp.broadcast_to(
        rope_rows.astype(jnp.float32)[:, None, :], (row_count, head_count, QK_ROPE)
    )
    joined = norm_rows(jnp.concatenate([nope_part, shared], axis=-1), scale_vector)
    turned = rotate(joined[..., QK_NOPE:], cosine_table, sine_table)
    return jnp.concatenate([joined[..., :QK_NOPE], turned], axis=-1).astype(jnp.bfloat16)


RIM = 32


def relayed_rows(rows, paired):
    return (rows * 5 // 16) // 16 * 16 if paired else 0


def gather_kernel(
    sizes,
    x_ref, gain_ref, rope_ref, taps_ref, cgain_ref, cshift_ref,
    qd, md, cv, cg, qu, ku, vu, ho, co,
    lq_all, lm_all, rr_all, conv_ref, qu_all, ku_all, vu_all, ho_all, co_all,
    qd_all, md_all, cv_all, cg_all, normed, acc_q, acc_m, acc_v, acc_g, ext, tail, rim,
    sums, stats, stats_all,
    send_d, recv_d, send_r, recv_r, send_z, recv_z, local_sem, rim_sem,
    sp_send, sp_recv, rr_send, rr_recv, tp_send, tp_recv,
):
    n_fs, n_sp, n_tp = sizes
    paired = n_sp % 2 == 0
    f = lax.axis_index("fs")
    s = lax.axis_index("sp")
    t = lax.axis_index("tp")
    parity = lax.rem(s, 2)
    partner = s + 1 - 2 * parity

    barrier = pltpu.get_barrier_semaphore()
    for axis, at, count in (("fs", f, n_fs), ("sp", s, n_sp), ("tp", t, n_tp)):
        for k in range(1, count):
            pl.semaphore_signal(
                barrier, inc=1, device_id={axis: lax.rem(at + k, count)}, device_id_type=MESH_ID
            )
    pl.semaphore_wait(barrier, n_fs + n_sp + n_tp - 3)

    jobs = [
        (qd, qd_all, 0), (md, md_all, 0), (cv, cv_all, 0), (cg, cg_all, 0),
        (qu, qu_all, 0), (ku, ku_all, 0), (vu, vu_all, 0), (ho, ho_all, 1), (co, co_all, 1),
    ]
    last = len(jobs) - 1
    ahead = 4

    def place(whole, shard, dim, owner, start, count):
        rows, cols = shard.shape
        if dim == 0:
            return whole.at[pl.ds(pl.multiple_of(owner * rows + start, 16), count), :]
        return whole.at[
            pl.ds(pl.multiple_of(start, 16), count),
            pl.ds(pl.multiple_of(owner * cols, 128), cols),
        ]

    square = n_fs == 4
    if square:
        near_x = f + 1 - 2 * lax.rem(f, 2)
        near_y = lax.rem(f + 2, 4)
        far = lax.rem(near_x + 2, 4)
        targets = sources = [near_x, near_y]
    else:
        targets = [lax.rem(f + k, n_fs) for k in range(1, n_fs)]
        sources = [lax.rem(f + n_fs - k, n_fs) for k in range(1, n_fs)]

    direct, far_copies, over_sp, own = [], [], [], []
    for a, (shard, whole, dim) in enumerate(jobs):
        rows = shard.shape[0]
        less = 0 if a == last else relayed_rows(rows, paired)
        start = parity * less
        count = rows - less
        direct.append([
            pltpu.make_async_remote_copy(
                src_ref=shard.at[pl.ds(pl.multiple_of(start, 16), count), :],
                dst_ref=place(whole, shard, dim, f, start, count),
                send_sem=send_d.at[a, k], recv_sem=recv_d.at[a, k],
                device_id={"fs": target}, device_id_type=MESH_ID,
            )
            for k, target in enumerate(targets)
        ])
        halves = []
        if square:
            half = (count // 2 + 15) // 16 * 16
            for k, (owner, target, begin, size) in enumerate((
                (near_y, near_x, start, half), (near_x, near_y, start + half, count - half)
            )):
                piece = place(whole, shard, dim, owner, begin, size)
                halves.append(pltpu.make_async_remote_copy(
                    src_ref=piece, dst_ref=piece,
                    send_sem=send_r.at[a, k], recv_sem=recv_r.at[a, k],
                    device_id={"fs": target}, device_id_type=MESH_ID,
                ))
        far_copies.append(halves)
        across = []
        if less:
            lack = parity * (rows - less)
            for k, owner in enumerate(sources + ([far] if square else [])):
                piece = place(whole, shard, dim, owner, lack, less)
                across.append(pltpu.make_async_remote_copy(
                    src_ref=piece, dst_ref=piece,
                    send_sem=send_z.at[a, k], recv_sem=recv_z.at[a, k],
                    device_id={"sp": partner}, device_id_type=MESH_ID,
                ))
        over_sp.append(across)
        own.append(pltpu.make_async_copy(
            shard, place(whole, shard, dim, f, 0, rows), local_sem.at[a]
        ))

    def begin_array(a):
        if a <= last:
            for copy in direct[a]:
                copy.start()

    def finish_far(a):
        for copy in far_copies[a]:
            copy.wait_recv()
        for copy in over_sp[a][len(sources):]:
            copy.start()

    def tick(a):
        for copy in direct[a]:
            copy.wait_recv()
        for copy in far_copies[a]:
            copy.start()
        begin_array(a + ahead)
        for copy in over_sp[a][: len(sources)]:
            copy.start()
        if a >= 1:
            finish_far(a - 1)

    def complete(a):
        own[a].wait()
        for copy in over_sp[a]:
            copy.wait_recv()

    for a in range(ahead):
        begin_array(a)
    for copy in own:
        copy.start()

    rows = x_ref.shape[0]
    part = 32

    @pl.loop(0, rows // part)
    def _(i):
        at = pl.ds(pl.multiple_of(i * part, part), part)
        x = x_ref[at, :].astype(jnp.float32)
        scale = lax.rsqrt(jnp.mean(x * x, axis=-1, keepdims=True) + epsilon)
        normed[at, :] = (x * scale * gain_ref[...]).astype(jnp.bfloat16)

    depth = qd.shape[0]

    def project(weight, acc):
        acc[...] = jnp.zeros_like(acc)

        @pl.loop(0, n_fs)
        def _(i):
            at = pl.ds(pl.multiple_of(i * depth, depth), depth)
            acc[...] += jnp.dot(
                normed[:, at], weight[at, :], preferred_element_type=jnp.float32
            )

    mine = pl.ds(pl.multiple_of(s * rows, 16), rows)
    rr_all[mine, :] = jnp.dot(
        normed[...], rope_ref[...], preferred_element_type=jnp.float32
    ).astype(jnp.bfloat16)
    tick(0)
    tick(1)
    tick(2)
    complete(0)
    project(qd_all, acc_q)
    lq_all[t, :, :] = acc_q[...].astype(jnp.bfloat16)
    tick(3)
    complete(1)
    project(md_all, acc_m)
    lm_all[t, mine, :] = acc_m[...].astype(jnp.bfloat16)
    tick(4)
    complete(2)
    project(cv_all, acc_v)

    exchanges, passes = [], []
    for k in range(1, n_sp):
        peer = {"sp": lax.rem(s + k, n_sp)}
        exchanges.append(pltpu.make_async_remote_copy(
            src_ref=lm_all.at[t, mine, :], dst_ref=lm_all.at[t, mine, :],
            send_sem=sp_send.at[k - 1], recv_sem=sp_recv.at[k - 1],
            device_id=peer, device_id_type=MESH_ID,
        ))
        exchanges.append(pltpu.make_async_remote_copy(
            src_ref=rr_all.at[mine, :], dst_ref=rr_all.at[mine, :],
            send_sem=rr_send.at[k - 1], recv_sem=rr_recv.at[k - 1],
            device_id=peer, device_id_type=MESH_ID,
        ))
    tp_peers = [{"tp": lax.rem(t + k, n_tp)} for k in range(1, n_tp)]

    def to_tp(kind, source, landing):
        return [
            pltpu.make_async_remote_copy(
                src_ref=source, dst_ref=landing(k),
                send_sem=tp_send.at[kind, k], recv_sem=tp_recv.at[kind, k],
                device_id=peer, device_id_type=MESH_ID,
            )
            for k, peer in enumerate(tp_peers)
        ]

    query_copies = to_tp(0, lq_all.at[t], lambda k: lq_all.at[t])
    memory_copies = to_tp(1, lm_all.at[t], lambda k: lm_all.at[t])
    stat_copies = to_tp(2, stats, lambda k: stats_all.at[k])
    for copy in exchanges + query_copies:
        copy.start()
    tick(5)
    complete(3)
    project(cg_all, acc_g)

    @pl.loop(0, rows // part)
    def _(i):
        at = pl.ds(pl.multiple_of(i * part, part), part)
        gated = (acc_v[at, :] * jax.nn.sigmoid(acc_g[at, :])).astype(jnp.bfloat16)
        ext[pl.ds(pl.multiple_of(RIM + i * part, part), part), :] = gated.astype(jnp.float32)

    tail[...] = ext[pl.ds(rows, RIM), :].astype(jnp.bfloat16)
    rim_copy = pltpu.make_async_remote_copy(
        src_ref=tail, dst_ref=rim, send_sem=rim_sem.at[0], recv_sem=rim_sem.at[1],
        device_id={"sp": lax.rem(s + 1, n_sp)}, device_id_type=MESH_ID,
    )
    tick(6)

    @pl.when(s < n_sp - 1)
    def _():
        rim_copy.start()

    for copy in exchanges:
        copy.wait_recv()
    for copy in memory_copies:
        copy.start()

    @pl.when(s > 0)
    def _():
        rim_copy.wait_recv()
        ext[pl.ds(0, RIM), :] = rim[...].astype(jnp.float32)

    @pl.when(s == 0)
    def _():
        ext[pl.ds(0, RIM), :] = jnp.zeros((RIM, ext.shape[1]), jnp.float32)

    tap_count = taps_ref.shape[0]
    block = 64

    def convolve(c):
        cols = pl.ds(pl.multiple_of(c * 128, 128), 128)
        taps = taps_ref[:, cols].astype(jnp.float32)
        for r in range(0, rows, block):
            total = jnp.zeros((block, 128), jnp.float32)
            for j in range(tap_count):
                total = total + ext[
                    pl.ds(r + RIM - (tap_count - 1) + j, block), cols
                ] * taps[j : j + 1, :]
            sums[pl.ds(r, block), cols] = total

    tiles = ext.shape[1] // 128
    pl.loop(0, tiles // 2)(convolve)
    tick(7)
    pl.loop(tiles // 2, tiles)(convolve)

    @pl.loop(0, rows // part)
    def _(i):
        begin = pl.multiple_of(i * part, part)
        values = sums[pl.ds(begin, part), :]
        stats[pl.ds(begin, part), :] = jnp.broadcast_to(
            jnp.sum(values, axis=1, keepdims=True), (part, 128)
        )
        stats[pl.ds(pl.multiple_of(rows + begin, part), part), :] = jnp.broadcast_to(
            jnp.sum(values * values, axis=1, keepdims=True), (part, 128)
        )

    tick(8)
    for copy in stat_copies:
        copy.start()
    for copy in stat_copies:
        copy.wait_recv()

    channels = ext.shape[1] * n_tp

    @pl.loop(0, rows // part)
    def _(i):
        begin = pl.multiple_of(i * part, part)
        upper = pl.ds(begin, part)
        lower = pl.ds(pl.multiple_of(rows + begin, part), part)
        total, squares = stats[upper, :], stats[lower, :]
        for k in range(n_tp - 1):
            total = total + stats_all[k, upper, :]
            squares = squares + stats_all[k, lower, :]
        mean = total[:, :1] / channels
        spread = squares[:, :1] / channels - mean * mean
        shaped = (sums[upper, :] - mean) * lax.rsqrt(spread + epsilon)
        conv_ref[upper, :] = jax.nn.silu(
            shaped * cgain_ref[...] + cshift_ref[...]
        ).astype(jnp.bfloat16)

    finish_far(last)
    for a in range(4, last + 1):
        complete(a)
    for copy in query_copies + memory_copies:
        copy.wait_recv()
    for group in direct + far_copies + over_sp:
        for copy in group:
            copy.wait_send()
    for copy in exchanges + query_copies + memory_copies + stat_copies:
        copy.wait_send()

    @pl.when(s < n_sp - 1)
    def _():
        rim_copy.wait_send()


def gather_and_project(
    sizes, x, mix_gain, rope_weight, taps, channel_gain, channel_shift,
    qd, md, cv, cg, qu, ku, vu, ho, co,
):
    n_fs, n_sp, n_tp = sizes
    rows = x.shape[0]
    bf16, f32 = jnp.bfloat16, jnp.float32
    vmem = pl.BlockSpec(memory_space=pltpu.VMEM)
    hbm = pl.BlockSpec(memory_space=pl.ANY)

    def whole(w, dim=0):
        return (w.shape[0] * n_fs, w.shape[1]) if dim == 0 else (w.shape[0], w.shape[1] * n_fs)

    out_shapes = [
        ((n_tp, rows, qd.shape[1]), bf16), ((n_tp, n_sp * rows, md.shape[1]), bf16),
        ((n_sp * rows, rope_weight.shape[1]), bf16), ((rows, cv.shape[1]), bf16),
        (whole(qu), bf16), (whole(ku), bf16), (whole(vu), bf16),
        (whole(ho, 1), bf16), (whole(co, 1), bf16),
    ]
    dma = pltpu.SemaphoreType.DMA
    tp_others = max(n_tp - 1, 1)
    sp_others = max(n_sp - 1, 1)
    return pl.pallas_call(
        functools.partial(gather_kernel, sizes),
        out_shape=[jax.ShapeDtypeStruct(*o) for o in out_shapes],
        in_specs=[vmem] * 6 + [hbm] * 9,
        out_specs=[vmem] * 9,
        scratch_shapes=[
            pltpu.VMEM(whole(qd), bf16), pltpu.VMEM(whole(md), bf16),
            pltpu.VMEM(whole(cv), bf16), pltpu.VMEM(whole(cg), bf16),
            pltpu.VMEM(x.shape, bf16), pltpu.VMEM((rows, qd.shape[1]), f32),
            pltpu.VMEM((rows, md.shape[1]), f32),
            pltpu.VMEM((rows, cv.shape[1]), f32), pltpu.VMEM((rows, cv.shape[1]), f32),
            pltpu.VMEM((rows + RIM, cv.shape[1]), f32),
            pltpu.VMEM((RIM, cv.shape[1]), bf16), pltpu.VMEM((RIM, cv.shape[1]), bf16),
            pltpu.VMEM((rows, cv.shape[1]), f32), pltpu.VMEM((2 * rows, 128), f32),
            pltpu.VMEM((tp_others, 2 * rows, 128), f32),
            dma((9, n_fs - 1)), dma((9, n_fs - 1)), dma((9, 2)), dma((9, 2)),
            dma((9, n_fs - 1)), dma((9, n_fs - 1)), dma((9,)), dma((2,)),
            dma((sp_others,)), dma((sp_others,)), dma((sp_others,)), dma((sp_others,)),
            dma((3, tp_others)), dma((3, tp_others)),
        ],
        compiler_params=pltpu.CompilerParams(
            collective_id=0, has_side_effects=True, vmem_limit_bytes=56 * 1024 * 1024
        ),
    )(
        x, mix_gain[None, :], rope_weight, taps, channel_gain[None, :], channel_shift[None, :],
        qd, md, cv, cg, qu, ku, vu, ho, co,
    )


def key_block(key_count):
    block_size = key_count
    while block_size > 2048 and block_size % 2 == 0:
        block_size = block_size // 2
    return block_size


def sum_groups(partial):
    count = lax.axis_size("tp")
    if count != 2:
        return lax.psum(partial, "tp")
    other = lax.ppermute(partial, "tp", [(0, 1), (1, 0)])
    return (partial.astype(jnp.float32) + other.astype(jnp.float32)).astype(jnp.bfloat16)


def local(
    tokens,
    mix_gain,
    query_down,
    memory_down,
    rope_weight,
    query_up,
    key_up,
    value_up,
    latent_gain,
    memory_gain,
    query_gain,
    key_gain,
    conv_value,
    conv_gate,
    conv_kernel,
    channel_gain,
    channel_shift,
    heads_out,
    conv_out,
):
    own_rows = tokens[0]
    (
        query_parts, memory_parts, rope_piece, conv_result,
        up_query, up_keys, up_values, out_heads, out_conv,
    ) = gather_and_project(
        (lax.axis_size("fs"), lax.axis_size("sp"), lax.axis_size("tp")),
        own_rows, mix_gain, rope_weight, conv_kernel, channel_gain, channel_shift,
        query_down, memory_down, conv_value, conv_gate,
        query_up, key_up, value_up, heads_out, conv_out,
    )
    row_count = own_rows.shape[0]
    whole_query = jnp.concatenate(list(query_parts), axis=1)
    whole_memory = jnp.concatenate(list(memory_parts), axis=1)
    query_normed = norm_rows(whole_query.astype(jnp.float32), latent_gain).astype(jnp.bfloat16)
    memory_piece = norm_rows(whole_memory.astype(jnp.float32), memory_gain).astype(jnp.bfloat16)
    positions = lax.axis_index("sp") * row_count + jnp.arange(row_count, dtype=jnp.int32)
    cosine_table, sine_table = rope_tables(positions)
    queries = heads_query(query_normed, up_query, query_gain, cosine_table, sine_table)
    head_count = queries.shape[1]
    query_segment = positions // SEG
    score_scale = QK_DIM ** (-0.5)
    def attend(state_carry, key_rows, value_rows, key_pos):
        running_max, row_total, weighted = state_carry
        scores = (
            jnp.einsum("qhd,khd->qhk", queries, key_rows, preferred_element_type=jnp.float32)
            * score_scale
        )
        allowed = ((key_pos // SEG)[None, :] <= query_segment[:, None])[:, None, :]
        scores = jnp.where(allowed, scores, masked_score)
        new_max = jnp.maximum(running_max, jnp.max(scores, axis=2))
        weights = jnp.where(allowed, jnp.exp(scores - new_max[:, :, None]), 0.0)
        factor = jnp.exp(running_max - new_max)
        row_total = row_total * factor + jnp.sum(weights, axis=2)
        weighted = weighted * factor[:, :, None] + jnp.einsum(
            "qhk,khd->qhd",
            weights.astype(jnp.bfloat16),
            value_rows,
            preferred_element_type=jnp.float32,
        )
        return (new_max, row_total, weighted)

    initial = (
        jnp.full((row_count, head_count), masked_score, jnp.float32),
        jnp.zeros((row_count, head_count), jnp.float32),
        jnp.zeros((row_count, head_count, V_DIM), jnp.float32),
    )
    def block_keys(block_start, block_size):
        memory_block = lax.dynamic_slice_in_dim(memory_piece, block_start, block_size, 0)
        rope_block = lax.dynamic_slice_in_dim(rope_piece, block_start, block_size, 0)
        key_pos = block_start + jnp.arange(block_size, dtype=jnp.int32)
        cosine_keys, sine_keys = rope_tables(key_pos)
        key_rows = heads_key(memory_block, rope_block, up_keys, key_gain, cosine_keys, sine_keys)
        value_rows = (
            jnp.dot(memory_block, up_values, preferred_element_type=jnp.float32)
            .astype(jnp.bfloat16)
            .reshape(block_size, head_count, V_DIM)
        )
        return (key_rows, value_rows, key_pos)

    key_count = memory_piece.shape[0]
    block_size = key_block(key_count)

    def step(block_index, running):
        key_rows, value_rows, key_pos = block_keys(block_index * block_size, block_size)
        return attend(running, key_rows, value_rows, key_pos)

    final_state = lax.fori_loop(0, key_count // block_size, step, initial)
    running_max, row_total, weighted = final_state
    attention = (
        (weighted / row_total[:, :, None])
        .astype(jnp.bfloat16)
        .reshape(row_count, head_count * V_DIM)
    )
    mixer_rows = jnp.concatenate([attention, conv_result], axis=1)
    out_weight = jnp.concatenate([out_heads, out_conv], axis=0)
    partial_sum = jnp.dot(mixer_rows, out_weight, preferred_element_type=jnp.float32)
    mixed = sum_groups(partial_sum.astype(jnp.bfloat16))
    return mixed[None]


def table_rows(count):
    inverse_freq = 1.0 / np.float32(rope_base) ** (
        np.arange(0, QK_ROPE, 2, dtype=np.float32) / np.float32(QK_ROPE)
    )
    angles = inverse_freq[:, None] * np.arange(count, dtype=np.float32)[None, :]
    angles = angles.astype(np.float64)
    return np.cos(angles).astype(np.float32), np.sin(angles).astype(np.float32)


def dot_heads(left, right):
    return lax.dot_general(
        left, right, (((0,), (0,)), ((), ())), preferred_element_type=jnp.float32
    )


def swapped_rows(count, eighths):
    return (count * eighths // 8) // 16 * 16


def fused_kernel(
    sizes,
    x_hbm, gain_hbm, rope_hbm, taps_hbm, cgain_hbm, cshift_hbm,
    lgain_hbm, mgain_hbm, qgain_hbm, kgain_hbm, cos_hbm, sin_hbm,
    qd, md, ku, vu, qu, cv, cg, ho, co,
    out_hbm,
    gain_ref, rope_ref, taps_ref, cgain_ref, cshift_ref,
    lgain_ref, mgain_ref, qgain_ref, kgain_ref, cos_ref, sin_ref,
    qd_all, md_all, ku_all, vu_all, qu_all, cv_all, cg_all, ho_all, co_all,
    x_all, normed, lq_all, lq_out, lm_all, mem_all, rr_all, qn_t, q_t, k_t, v_t,
    turned, ropesq, qcol, kcol, bias, scores,
    att_t, conv_s, acc_v, acc_g, acc_out, gate_out, gate_in, ext, tail, rim, sums, stats, stats_all,
    mine_ref, other_ref, whole_ref,
    send_d, recv_d, send_r, recv_r, send_z, recv_z, local_sem, small_sem, rim_sem, x_sem,
    part_sem, sp_send, sp_recv, fw_send, fw_recv, tp_send, tp_recv, out_send, out_recv, store_sem,
):
    n_fs, n_sp, n_tp = sizes
    f = lax.axis_index("fs")
    s = lax.axis_index("sp")
    t = lax.axis_index("tp")
    parity = lax.rem(s, 2)
    couple = lax.div(s, 2)
    couples = n_sp // 2
    partner = {"sp": s + 1 - 2 * parity}
    twin = {"tp": 1 - t}
    even, odd = parity == 0, parity == 1

    barrier = pltpu.get_barrier_semaphore()
    for axis, at, count in (("fs", f, n_fs), ("sp", s, n_sp), ("tp", t, n_tp)):
        for k in range(1, count):
            pl.semaphore_signal(
                barrier, inc=1, device_id={axis: lax.rem(at + k, count)}, device_id_type=MESH_ID
            )

    rows = x_hbm.shape[0]
    x_own = pltpu.make_async_copy(x_hbm, x_all.at[parity], x_sem.at[0])
    x_own.start()
    small = [
        pltpu.make_async_copy(source, landing, small_sem.at[i])
        for i, (source, landing) in enumerate((
            (gain_hbm, gain_ref), (rope_hbm, rope_ref), (taps_hbm, taps_ref),
            (cgain_hbm, cgain_ref), (cshift_hbm, cshift_ref), (lgain_hbm, lgain_ref),
            (mgain_hbm, mgain_ref), (qgain_hbm, qgain_ref), (kgain_hbm, kgain_ref),
            (cos_hbm, cos_ref), (sin_hbm, sin_ref),
        ))
    ]
    for copy in small:
        copy.start()

    def remote(source, landing, send, recv, device):
        return pltpu.make_async_remote_copy(
            src_ref=source, dst_ref=landing, send_sem=send, recv_sem=recv,
            device_id=device, device_id_type=MESH_ID,
        )

    share = rows // n_tp
    slab = pl.ds(pl.multiple_of(t * share, 16), share)
    x_send = remote(
        x_hbm.at[slab, :], x_all.at[parity, slab, :], x_sem.at[1], x_sem.at[2], partner
    )
    theirs = x_all.at[1 - parity, slab, :]
    x_forward = remote(theirs, theirs, x_sem.at[3], x_sem.at[4], twin)

    near_x = f + 1 - 2 * lax.rem(f, 2)
    near_y = lax.rem(f + 2, 4)
    far = lax.rem(near_x + 2, 4)
    sources = [near_x, near_y]

    def job(a, shard, whole, swap, dim=0, first=0, count=None):
        depth, cols = shard.shape
        count = depth if count is None else count
        less = swapped_rows(count, swap)
        kept = count - less

        def place(owner, start, size):
            if dim == 0:
                return whole.at[pl.ds(pl.multiple_of(owner * depth + start, 16), size), :]
            return whole.at[
                pl.ds(pl.multiple_of(start, 16), size),
                pl.ds(pl.multiple_of(owner * cols, 128), cols),
            ]

        start = first + parity * less
        direct = [
            remote(
                shard.at[pl.ds(pl.multiple_of(start, 16), kept), :], place(f, start, kept),
                send_d.at[a, k], recv_d.at[a, k], {"fs": target},
            )
            for k, target in enumerate(sources)
        ]
        half = (kept // 2 + 15) // 16 * 16
        relays = []
        for k, (owner, target, begin, size) in enumerate((
            (near_y, near_x, start, half), (near_x, near_y, start + half, kept - half)
        )):
            piece = place(owner, begin, size)
            relays.append(remote(piece, piece, send_r.at[a, k], recv_r.at[a, k], {"fs": target}))
        across = []
        if less:
            for k, owner in enumerate(sources + [far]):
                piece = place(owner, first + parity * kept, less)
                across.append(remote(piece, piece, send_z.at[a, k], recv_z.at[a, k], partner))
        own = pltpu.make_async_copy(
            shard.at[pl.ds(first, count), :], place(f, first, count), local_sem.at[a]
        )
        return direct, relays, across, own

    wide = cv.shape[1] // 2
    side = pl.ds(pl.multiple_of(parity * wide, 128), wide)
    half_rows = ho.shape[0] // 2
    plan = [
        [(even, qd, qd_all, 0), (odd, md, md_all, 0)],
        [(None, ku, ku_all, 4)], [(None, vu, vu_all, 4)], [(None, qu, qu_all, 4)],
        [(None, cv.at[:, side], cv_all, 0)], [(None, cg.at[:, side], cg_all, 0)],
        [(None, ho, ho_all, 4, 1, 0, half_rows)], [(None, ho, ho_all, 4, 1, half_rows, half_rows)],
        [(None, co, co_all, 3, 1, 0, half_rows)], [(None, co, co_all, 0, 1, half_rows, half_rows)],
    ]
    jobs = [[(who[0], job(a, *who[1:])) for who in group] for a, group in enumerate(plan)]
    last = len(jobs) - 1
    ahead = 3

    def each(a, action):
        for condition, parts in jobs[a]:
            if condition is None:
                action(parts)
            else:
                pl.when(condition)(functools.partial(action, parts))

    def begin_array(a):
        def start(parts):
            for copy in parts[0]:
                copy.start()

        if a <= last:
            each(a, start)

    def finish_far(a):
        def go(parts):
            with jax.named_scope(f"far_{a}"):
                for copy in parts[1]:
                    copy.wait_recv()
            for copy in parts[2][len(sources):]:
                copy.start()

        each(a, go)

    def tick(a):
        def go(parts):
            with jax.named_scope(f"direct_{a}"):
                for copy in parts[0]:
                    copy.wait_recv()
            for copy in parts[1]:
                copy.start()

        def swap(parts):
            for copy in parts[2][: len(sources)]:
                copy.start()

        each(a, go)
        begin_array(a + ahead)
        each(a, swap)

    def complete(a):
        def go(parts):
            with jax.named_scope(f"across_{a}"):
                parts[3].wait()
                for copy in parts[2]:
                    copy.wait_recv()

        each(a, go)

    with jax.named_scope("entry"):
        pl.semaphore_wait(barrier, n_fs + n_sp + n_tp - 3)
    x_send.start()
    for a in range(ahead):
        begin_array(a)
    for a in range(last + 1):
        each(a, lambda parts: parts[3].start())
    with jax.named_scope("small_wait"):
        for copy in small:
            copy.wait()
        x_own.wait()

    part = 32

    def norm_block(b):
        @pl.loop(0, rows // part)
        def _(i):
            at = pl.ds(pl.multiple_of(i * part, part), part)
            x = x_all[b, at, :].astype(jnp.float32)
            scale = lax.rsqrt(jnp.mean(x * x, axis=-1, keepdims=True) + epsilon)
            normed[b, at, :] = (x * scale * gain_ref[...]).astype(jnp.bfloat16)

        rr_all[2 * couple + b] = lax.dot_general(
            rope_ref[...], normed[b], (((1,), (1,)), ((), ())), preferred_element_type=jnp.float32
        ).astype(jnp.bfloat16)

    norm_block(parity)
    half_rope = QK_ROPE // 2

    def column(row_ref, col_ref):
        shape = (QK_DIM, QK_DIM)
        here = lax.broadcasted_iota(jnp.int32, shape, 0) == lax.broadcasted_iota(jnp.int32, shape, 1)
        spread_row = jnp.broadcast_to(row_ref[...], shape)
        picked = jnp.sum(jnp.where(here, spread_row, 0.0), axis=1, keepdims=True)
        col_ref[...] = jnp.broadcast_to(picked, col_ref.shape)

    column(qgain_ref, qcol)
    column(kgain_ref, kcol)

    @pl.loop(2 * couple + 2, n_sp)
    def _(j):
        mem_all[j] = jnp.zeros(mem_all.shape[1:], jnp.bfloat16)
        rr_all[j] = jnp.zeros(rr_all.shape[1:], jnp.bfloat16)

    @pl.when(even)
    def _():
        mem_all[s + 1] = jnp.zeros(mem_all.shape[1:], jnp.bfloat16)

    @pl.loop(0, n_sp)
    def _(j):
        key_at = j * rows + lax.broadcasted_iota(jnp.int32, (rows, rows), 0)
        query_at = s * rows + lax.broadcasted_iota(jnp.int32, (rows, rows), 1)
        bias[j] = jnp.where(
            lax.div(key_at, SEG) <= lax.div(query_at, SEG), 0.0, masked_score
        )

    tick(0)
    with jax.named_scope("x_wait"):
        x_send.wait_recv()
    x_forward.start()
    tick(1)
    with jax.named_scope("x_forward"):
        x_forward.wait_recv()
    norm_block(1 - parity)
    tick(2)
    finish_far(0)

    depth = qd.shape[0]

    def project(weight, b, acc):
        acc[...] = jnp.zeros_like(acc)

        @pl.loop(0, n_fs)
        def _(i):
            at = pl.ds(pl.multiple_of(i * depth, depth), depth)
            acc[...] += jnp.dot(
                normed[b, :, at], weight[at, :], preferred_element_type=jnp.float32
            )

    lat = md.shape[1]
    lat_q = qd.shape[1]
    held = pl.ds(pl.multiple_of(t * lat, lat), lat)
    query_across = remote(lq_out, lq_all.at[t], part_sem.at[0], part_sem.at[1], partner)
    query_copy = remote(lq_all.at[t], lq_all.at[t], tp_send.at[0], tp_recv.at[0], twin)
    memory_copy = remote(lm_all.at[t], lm_all.at[t], tp_send.at[1], tp_recv.at[1], twin)
    stat_copy = remote(stats, stats_all, tp_send.at[2], tp_recv.at[2], twin)
    gate_across = remote(gate_out, gate_in, part_sem.at[2], part_sem.at[3], partner)

    complete(0)

    @pl.when(even)
    def _():
        project(qd_all, 1, acc_out.at[:, pl.ds(0, lat_q)])
        lq_out[...] = acc_out[:, :lat_q].astype(jnp.bfloat16)
        query_across.start()
        project(qd_all, 0, acc_out.at[:, pl.ds(0, lat_q)])
        lq_all[t] = acc_out[:, :lat_q].astype(jnp.bfloat16)
        query_copy.start()

    @pl.when(odd)
    def _():
        for b in range(2):
            project(md_all, b, acc_v.at[:, pl.ds(0, lat)])
            lm_all[t, b] = acc_v[:, :lat].astype(jnp.bfloat16)
        memory_copy.start()

    tick(3)

    def normed_columns(parts, width, gain_at, put):
        @pl.loop(0, rows // 128)
        def _(i):
            at = pl.ds(pl.multiple_of(i * 128, 128), 128)
            pieces = [parts(g, at).astype(jnp.float32) for g in range(n_tp)]
            total = sum(jnp.sum(p * p, axis=-1, keepdims=True) for p in pieces)
            scale = lax.rsqrt(total / (width * n_tp) + epsilon)
            for g in range(n_tp):
                shaped = (pieces[g] * scale * gain_at(g * width, width)).astype(jnp.bfloat16)
                put(g * width, width, at, shaped.astype(jnp.float32).T.astype(jnp.bfloat16))

    mine_block = mem_all.at[s, held, :]
    back = remote(
        mem_all.at[2 * couple, held, :], mem_all.at[2 * couple, held, :],
        part_sem.at[4], part_sem.at[5], partner,
    )
    back_forward = remote(mine_block, mine_block, fw_send.at[couples - 1], fw_recv.at[couples - 1], twin)
    pair = pl.ds(2 * couple, 2)
    onward, forwards = [], []
    for d in range(1, couples):
        group = []
        later = lax.rem(couple + d, couples)
        for e in range(2):
            target = {"sp": 2 * later + e}
            group.append((
                remote(
                    mem_all.at[pair, held, :], mem_all.at[pair, held, :],
                    sp_send.at[d - 1, e, 0], sp_recv.at[d - 1, 0], target,
                ),
                remote(
                    rr_all.at[pair], rr_all.at[pair],
                    sp_send.at[d - 1, e, 1], sp_recv.at[d - 1, 1], target,
                ),
            ))
        onward.append(group)
        earlier = mem_all.at[pl.ds(2 * lax.rem(couple + couples - d, couples), 2), held, :]
        forwards.append(remote(earlier, earlier, fw_send.at[d - 1], fw_recv.at[d - 1], twin))

    @pl.when(odd)
    def _():
        with jax.named_scope("memory_wait"):
            memory_copy.wait_recv()
        for b in (1, 0):
            def put_memory(begin, width, at, piece, b=b):
                mem_all[2 * couple + b, begin : begin + width, at] = piece

            normed_columns(
                lambda g, at, b=b: lm_all[g, b, at, :], lat,
                lambda begin, width: mgain_ref[:, begin : begin + width], put_memory,
            )
        for d in range(1, couples):
            @pl.when(couple + d < couples)
            def _(d=d):
                for e in range(2):
                    for copy in onward[d - 1][e]:
                        copy.start()
        back.start()
        with jax.named_scope("query_across"):
            query_across.wait_recv()
        query_copy.start()

    finish_far(1)
    tick(4)

    def put_query(begin, width, at, piece):
        qn_t[begin : begin + width, at] = piece

    with jax.named_scope("query_wait"):
        query_copy.wait_recv()
    normed_columns(
        lambda g, at: lq_all[g, at, :], lat_q,
        lambda begin, width: jnp.concatenate(
            [lgain_ref[r : r + 1, :] for r in range(begin // 128, (begin + width) // 128)], axis=1
        ),
        put_query,
    )
    finish_far(2)

    @pl.when(even)
    def _():
        with jax.named_scope("back_wait"):
            back.wait_recv()
        back_forward.start()

    for d in range(1, couples):
        @pl.when(couple >= d)
        def _(d=d):
            with jax.named_scope(f"behind_{d}"):
                for copy in onward[d - 1][0]:
                    copy.wait_recv()
            forwards[d - 1].start()
    complete(1)
    complete(2)

    @pl.when(even)
    def _():
        with jax.named_scope("back_forward"):
            back_forward.wait_recv()

    for d in range(1, couples):
        @pl.when(couple >= d)
        def _(d=d):
            with jax.named_scope(f"forward_{d}"):
                forwards[d - 1].wait_recv()

    @pl.loop(0, n_sp)
    def _(j):
        k_t[j] = dot_heads(ku_all[...], mem_all[j])
        v_t[j] = dot_heads(vu_all[...], mem_all[j]).astype(jnp.bfloat16)
        shared = rr_all[j].astype(jnp.float32)
        ropesq[j] = jnp.sum(shared * shared, axis=0, keepdims=True)
        shared = shared * kcol[QK_NOPE:, :]
        front, back_half = shared[:half_rope], shared[half_rope:]
        at = pl.ds(pl.multiple_of(j * rows, rows), rows)
        cosine, sine = cos_ref[:, at], sin_ref[:, at]
        turned[j] = jnp.concatenate(
            [front * cosine - back_half * sine, front * sine + back_half * cosine], axis=0
        )

    tick(5)
    finish_far(3)
    tick(6)
    complete(3)
    q_t[...] = dot_heads(qu_all[...], qn_t[...])
    heads = qu.shape[1] // QK_DIM
    here = pl.ds(pl.multiple_of(s * rows, rows), rows)
    score_scale = QK_DIM ** (-0.5)

    def head(h):
        q = q_t[pl.ds(pl.multiple_of(h * QK_DIM, QK_DIM), QK_DIM), :]
        q = q * lax.rsqrt(jnp.mean(q * q, axis=0, keepdims=True) + epsilon) * qcol[...]
        front, back_half = q[QK_NOPE : QK_NOPE + half_rope], q[QK_NOPE + half_rope :]
        cosine, sine = cos_ref[:, here], sin_ref[:, here]
        q = jnp.concatenate(
            [
                q[:QK_NOPE],
                front * cosine - back_half * sine,
                front * sine + back_half * cosine,
            ],
            axis=0,
        ).astype(jnp.bfloat16)
        krow = pl.ds(pl.multiple_of(h * QK_NOPE, QK_NOPE), QK_NOPE)
        vrow = pl.ds(pl.multiple_of(h * V_DIM, V_DIM), V_DIM)
        top = jnp.full((1, rows), masked_score, jnp.float32)
        for j in range(n_sp):
            nope = k_t[j, krow, :]
            scale = lax.rsqrt(
                (jnp.sum(nope * nope, axis=0, keepdims=True) + ropesq[j]) / QK_DIM + epsilon
            )
            key = jnp.concatenate(
                [nope * scale * kcol[:QK_NOPE, :], turned[j] * scale], axis=0
            ).astype(jnp.bfloat16)
            block = dot_heads(key, q) + bias[j]
            scores[j] = block
            top = jnp.maximum(top, jnp.max(block, axis=0, keepdims=True))
        total = jnp.zeros((1, rows), jnp.float32)
        summed = jnp.zeros((V_DIM, rows), jnp.float32)
        for j in range(n_sp):
            weight = jnp.exp((scores[j] - top) * score_scale)
            total = total + jnp.sum(weight, axis=0, keepdims=True)
            summed = summed + jnp.dot(
                v_t[j, vrow, :], weight.astype(jnp.bfloat16),
                preferred_element_type=jnp.float32,
            )
        att_t[vrow, :] = summed / total

    pl.loop(0, heads // 2)(head)
    finish_far(4)
    tick(7)
    pl.loop(heads // 2, heads)(head)
    finish_far(5)
    complete(4)
    complete(5)
    for other_block in (True, False):
        b = 1 - parity if other_block else parity
        project(cv_all, b, acc_v)
        project(cg_all, b, acc_g)
        gated = (acc_v[...] * jax.nn.sigmoid(acc_g[...])).astype(jnp.bfloat16)
        if other_block:
            gate_out[...] = gated
            gate_across.start()
            tick(8)
            finish_far(6)
        else:
            ext[pl.ds(RIM, rows), side] = gated.astype(jnp.float32)
    with jax.named_scope("gate_wait"):
        gate_across.wait_recv()
    ext[
        pl.ds(RIM, rows), pl.ds(pl.multiple_of((1 - parity) * wide, 128), wide)
    ] = gate_in[...].astype(jnp.float32)

    tail[...] = ext[pl.ds(rows, RIM), :].astype(jnp.bfloat16)
    rim_copy = remote(
        tail, rim, rim_sem.at[0], rim_sem.at[1], {"sp": lax.rem(s + 1, n_sp)}
    )

    @pl.when(s < n_sp - 1)
    def _():
        rim_copy.start()

    @pl.when(s > 0)
    def _():
        with jax.named_scope("rim_wait"):
            rim_copy.wait_recv()
        ext[pl.ds(0, RIM), :] = rim[...].astype(jnp.float32)

    @pl.when(s == 0)
    def _():
        ext[pl.ds(0, RIM), :] = jnp.zeros((RIM, ext.shape[1]), jnp.float32)

    tap_count = taps_ref.shape[0]
    block = 64

    def convolve(c):
        cols = pl.ds(pl.multiple_of(c * 128, 128), 128)
        taps = taps_ref[:, cols].astype(jnp.float32)
        for r in range(0, rows, block):
            total = jnp.zeros((block, 128), jnp.float32)
            for j in range(tap_count):
                total = total + ext[
                    pl.ds(r + RIM - (tap_count - 1) + j, block), cols
                ] * taps[j : j + 1, :]
            sums[pl.ds(r, block), cols] = total

    tiles = ext.shape[1] // 128
    pl.loop(0, tiles // 2)(convolve)
    finish_far(7)
    pl.loop(tiles // 2, tiles)(convolve)
    tick(9)

    @pl.loop(0, rows // part)
    def _(i):
        begin = pl.multiple_of(i * part, part)
        values = sums[pl.ds(begin, part), :]
        stats[pl.ds(begin, part), :] = jnp.broadcast_to(
            jnp.sum(values, axis=1, keepdims=True), (part, 128)
        )
        stats[pl.ds(pl.multiple_of(rows + begin, part), part), :] = jnp.broadcast_to(
            jnp.sum(values * values, axis=1, keepdims=True), (part, 128)
        )

    stat_copy.start()
    finish_far(8)
    complete(6)
    complete(7)
    att = att_t[...].T.astype(jnp.bfloat16)
    span = ho.shape[1]

    @pl.loop(0, n_fs)
    def _(i):
        cols = pl.ds(pl.multiple_of(i * span, span), span)
        acc_out[:, cols] = jnp.dot(att, ho_all[:, cols], preferred_element_type=jnp.float32)

    with jax.named_scope("stat_wait"):
        stat_copy.wait_recv()
    channels = ext.shape[1] * n_tp

    @pl.loop(0, rows // part)
    def _(i):
        begin = pl.multiple_of(i * part, part)
        upper = pl.ds(begin, part)
        lower = pl.ds(pl.multiple_of(rows + begin, part), part)
        total = stats[upper, :] + stats_all[upper, :]
        squares = stats[lower, :] + stats_all[lower, :]
        mean = total[:, :1] / channels
        spread = squares[:, :1] / channels - mean * mean
        shaped = (sums[upper, :] - mean) * lax.rsqrt(spread + epsilon)
        conv_s[upper, :] = jax.nn.silu(
            shaped * cgain_ref[...] + cshift_ref[...]
        ).astype(jnp.bfloat16)

    finish_far(last)
    complete(8)

    @pl.loop(0, n_fs)
    def _(i):
        cols = pl.ds(pl.multiple_of(i * span, span), span)
        acc_out[:, cols] += jnp.dot(
            conv_s[:, :half_rows], co_all[:half_rows, cols], preferred_element_type=jnp.float32
        )

    complete(last)
    outs = []
    for i in range(n_fs):
        cols = slice(i * span, (i + 1) * span)
        outs.append(remote(
            mine_ref.at[:, cols], other_ref.at[:, cols], out_send.at[i], out_recv.at[i], twin
        ))
        mine_ref[:, cols] = (
            acc_out[:, cols]
            + jnp.dot(
                conv_s[:, half_rows:], co_all[half_rows:, cols],
                preferred_element_type=jnp.float32,
            )
        ).astype(jnp.bfloat16)
        outs[i].start()

    def drain(parts):
        for copy in parts[0] + parts[1] + parts[2]:
            copy.wait_send()

    for a in range(last + 1):
        each(a, drain)
    for copy in (x_send, x_forward, query_copy, stat_copy, gate_across):
        copy.wait_send()

    @pl.when(even)
    def _():
        query_across.wait_send()
        back_forward.wait_send()

    @pl.when(odd)
    def _():
        memory_copy.wait_send()
        back.wait_send()
        for d in range(1, couples):
            @pl.when(couple + d < couples)
            def _(d=d):
                for e in range(2):
                    for copy in onward[d - 1][e]:
                        copy.wait_send()

    for d in range(1, couples):
        @pl.when(couple >= d)
        def _(d=d):
            forwards[d - 1].wait_send()

    @pl.when(s < n_sp - 1)
    def _():
        rim_copy.wait_send()

    stores = []
    for i in range(n_fs):
        cols = slice(i * span, (i + 1) * span)
        with jax.named_scope(f"out_wait_{i}"):
            outs[i].wait_recv()
        whole_ref[:, cols] = (
            mine_ref[:, cols].astype(jnp.float32) + other_ref[:, cols].astype(jnp.float32)
        ).astype(jnp.bfloat16)
        stores.append(pltpu.make_async_copy(
            whole_ref.at[:, cols], out_hbm.at[:, cols], store_sem.at[i]
        ))
        stores[i].start()
    with jax.named_scope("store_wait"):
        for copy in outs:
            copy.wait_send()
        for copy in stores:
            copy.wait()


def fused_call(
    sizes, x, mix_gain, rope_weight, taps, channel_gain, channel_shift,
    latent_gain, memory_gain, query_gain, key_gain,
    qd, md, cv, cg, qu, ku, vu, ho, co,
):
    n_fs, n_sp, n_tp = sizes
    rows, model = x.shape
    bf16, f32 = jnp.bfloat16, jnp.float32
    hbm = pl.BlockSpec(memory_space=pl.ANY)
    cosine, sine = table_rows(n_sp * rows)
    small = [
        mix_gain[None, :], rope_weight.T, taps, channel_gain[None, :], channel_shift[None, :],
        latent_gain.reshape(-1, 128), memory_gain[None, :], query_gain[None, :],
        key_gain[None, :], jnp.asarray(cosine), jnp.asarray(sine),
    ]

    def whole(w, dim=0, parts=1):
        rows_w, cols_w = w.shape[0], w.shape[1] // parts
        return (rows_w * n_fs, cols_w) if dim == 0 else (rows_w, cols_w * n_fs)

    def scratch(*shape, dtype=f32):
        return pltpu.VMEM(shape, dtype)

    dma = pltpu.SemaphoreType.DMA
    channels, lat = cv.shape[1], md.shape[1] * n_tp
    rope = rope_weight.shape[1]
    couples = n_sp // 2
    spare = max(couples - 1, 1)
    count = 10
    return pl.pallas_call(
        functools.partial(fused_kernel, sizes),
        out_shape=jax.ShapeDtypeStruct((rows, ho.shape[1] * n_fs), bf16),
        in_specs=[hbm] * 21,
        out_specs=hbm,
        scratch_shapes=[scratch(*a.shape, dtype=a.dtype) for a in small] + [
            scratch(*whole(qd), dtype=bf16), scratch(*whole(md), dtype=bf16),
            scratch(*whole(ku), dtype=bf16), scratch(*whole(vu), dtype=bf16),
            scratch(*whole(qu), dtype=bf16), scratch(*whole(cv, 0, 2), dtype=bf16),
            scratch(*whole(cg, 0, 2), dtype=bf16), scratch(*whole(ho, 1), dtype=bf16),
            scratch(*whole(co, 1), dtype=bf16),
            scratch(2, rows, model, dtype=bf16), scratch(2, rows, model, dtype=bf16),
            scratch(n_tp, rows, qd.shape[1], dtype=bf16), scratch(rows, qd.shape[1], dtype=bf16),
            scratch(n_tp, 2, rows, md.shape[1], dtype=bf16),
            scratch(n_sp, lat, rows, dtype=bf16), scratch(n_sp, rope, rows, dtype=bf16),
            scratch(qu.shape[0] * n_fs, rows, dtype=bf16), scratch(qu.shape[1], rows),
            scratch(n_sp, ku.shape[1], rows), scratch(n_sp, vu.shape[1], rows, dtype=bf16),
            scratch(n_sp, rope, rows), scratch(n_sp, 1, rows),
            scratch(QK_DIM, rows), scratch(QK_DIM, rows),
            scratch(n_sp, rows, rows), scratch(n_sp, rows, rows),
            scratch(vu.shape[1], rows), scratch(rows, channels, dtype=bf16),
            scratch(rows, channels // 2), scratch(rows, channels // 2),
            scratch(rows, ho.shape[1] * n_fs),
            scratch(rows, channels // 2, dtype=bf16), scratch(rows, channels // 2, dtype=bf16),
            scratch(rows + RIM, channels), scratch(RIM, channels, dtype=bf16),
            scratch(RIM, channels, dtype=bf16), scratch(rows, channels),
            scratch(2 * rows, 128), scratch(2 * rows, 128),
            *[scratch(rows, ho.shape[1] * n_fs, dtype=bf16)] * 3,
            dma((count, 2)), dma((count, 2)), dma((count, 2)), dma((count, 2)),
            dma((count, 3)), dma((count, 3)), dma((count,)), dma((len(small),)), dma((2,)),
            dma((5,)), dma((6,)), dma((spare, 2, 2)), dma((spare, 2)),
            dma((couples,)), dma((couples,)), dma((3,)), dma((3,)), dma((n_fs,)), dma((n_fs,)), dma((n_fs,)),
        ],
        compiler_params=pltpu.CompilerParams(
            collective_id=1, has_side_effects=True, vmem_limit_bytes=60 * 1024 * 1024
        ),
    )(x, *small, qd, md, ku, vu, qu, cv, cg, ho, co)


def fused_local(
    tokens, mix_gain, query_down, memory_down, rope_weight, query_up, key_up, value_up,
    latent_gain, memory_gain, query_gain, key_gain, conv_value, conv_gate, conv_kernel,
    channel_gain, channel_shift, heads_out, conv_out,
):
    mixed = fused_call(
        (lax.axis_size("fs"), lax.axis_size("sp"), lax.axis_size("tp")),
        tokens[0], mix_gain, rope_weight, conv_kernel, channel_gain, channel_shift,
        latent_gain, memory_gain, query_gain, key_gain,
        query_down, memory_down, conv_value, conv_gate,
        query_up, key_up, value_up, heads_out, conv_out,
    )
    return mixed[None]


def solution(mesh):
    in_specs = (
        P("fs", "sp", None),
        P(),
        P("fs", "tp"),
        P("fs", "tp"),
        P(),
        P("fs", "tp"),
        P("fs", "tp"),
        P("fs", "tp"),
        P(),
        P(),
        P(),
        P(),
        P("fs", "tp"),
        P("fs", "tp"),
        P(None, "tp"),
        P("tp"),
        P("tp"),
        P("tp", "fs"),
        P("tp", "fs"),
    )
    out_specs = P("fs", "sp", None)
    n_fs, n_sp, n_tp = (mesh.shape[axis] for axis in ("fs", "sp", "tp"))
    fits = n_fs == 4 and n_tp == 2 and n_sp in (2, 4)
    body = fused_local if fits else local
    return jax.shard_map(body, mesh=mesh, in_specs=in_specs, out_specs=out_specs, check_vma=False)
```

```python
import functools

import jax
import jax.numpy as jnp
import numpy as np
from jax import lax
from jax.experimental import pallas as pl
from jax.experimental.pallas import tpu as pltpu
from jax.sharding import PartitionSpec as P

MESH_ID = pl.DeviceIdType.MESH

QK_NOPE = 64
QK_ROPE = 32
V_DIM = 64
CONV_W = 1024
SEG = 64
QK_DIM = 96


epsilon = 1e-06
rope_base = 10000.0
masked_score = -1e30


def norm_rows(matrix, scale_vector):
    return (
        matrix
        * lax.rsqrt(jnp.mean(matrix * matrix, axis=-1, keepdims=True) + epsilon)
        * scale_vector
    )


def rope_tables(positions):
    inverse_freq = 1.0 / rope_base ** (jnp.arange(0, QK_ROPE, 2, dtype=jnp.float32) / QK_ROPE)
    angles = positions.astype(jnp.float32)[:, None] * inverse_freq[None, :]
    return (jnp.cos(angles)[:, None, :], jnp.sin(angles)[:, None, :])


def rotate(matrix, cosine_table, sine_table):
    half_width = matrix.shape[-1] // 2
    front_half = matrix[..., :half_width]
    back_half = matrix[..., half_width:]
    return jnp.concatenate(
        [
            front_half * cosine_table - back_half * sine_table,
            front_half * sine_table + back_half * cosine_table,
        ],
        axis=-1,
    )


def heads_query(latent, weight, scale_vector, cosine_table, sine_table):
    row_count = latent.shape[0]
    projected = jnp.dot(latent, weight, preferred_element_type=jnp.float32)
    projected = norm_rows(
        projected.reshape(row_count, weight.shape[1] // QK_DIM, QK_DIM), scale_vector
    )
    turned = rotate(projected[..., QK_NOPE:], cosine_table, sine_table)
    return jnp.concatenate([projected[..., :QK_NOPE], turned], axis=-1).astype(jnp.bfloat16)


def heads_key(latent, rope_rows, weight, scale_vector, cosine_table, sine_table):
    row_count = latent.shape[0]
    head_count = weight.shape[1] // QK_NOPE
    nope_part = jnp.dot(latent, weight, preferred_element_type=jnp.float32).reshape(
        row_count, head_count, QK_NOPE
    )
    shared = jnp.broadcast_to(
        rope_rows.astype(jnp.float32)[:, None, :], (row_count, head_count, QK_ROPE)
    )
    joined = norm_rows(jnp.concatenate([nope_part, shared], axis=-1), scale_vector)
    turned = rotate(joined[..., QK_NOPE:], cosine_table, sine_table)
    return jnp.concatenate([joined[..., :QK_NOPE], turned], axis=-1).astype(jnp.bfloat16)


RIM = 32


def relayed_rows(rows, paired):
    return (rows * 5 // 16) // 16 * 16 if paired else 0


def gather_kernel(
    sizes,
    x_ref, gain_ref, rope_ref, taps_ref, cgain_ref, cshift_ref,
    qd, md, cv, cg, qu, ku, vu, ho, co,
    lq_all, lm_all, rr_all, conv_ref, qu_all, ku_all, vu_all, ho_all, co_all,
    qd_all, md_all, cv_all, cg_all, normed, acc_q, acc_m, acc_v, acc_g, ext, tail, rim,
    sums, stats, stats_all,
    send_d, recv_d, send_r, recv_r, send_z, recv_z, local_sem, rim_sem,
    sp_send, sp_recv, rr_send, rr_recv, tp_send, tp_recv,
):
    n_fs, n_sp, n_tp = sizes
    paired = n_sp % 2 == 0
    f = lax.axis_index("fs")
    s = lax.axis_index("sp")
    t = lax.axis_index("tp")
    parity = lax.rem(s, 2)
    partner = s + 1 - 2 * parity

    barrier = pltpu.get_barrier_semaphore()
    for axis, at, count in (("fs", f, n_fs), ("sp", s, n_sp), ("tp", t, n_tp)):
        for k in range(1, count):
            pl.semaphore_signal(
                barrier, inc=1, device_id={axis: lax.rem(at + k, count)}, device_id_type=MESH_ID
            )
    pl.semaphore_wait(barrier, n_fs + n_sp + n_tp - 3)

    jobs = [
        (qd, qd_all, 0), (md, md_all, 0), (cv, cv_all, 0), (cg, cg_all, 0),
        (qu, qu_all, 0), (ku, ku_all, 0), (vu, vu_all, 0), (ho, ho_all, 1), (co, co_all, 1),
    ]
    last = len(jobs) - 1
    ahead = 4

    def place(whole, shard, dim, owner, start, count):
        rows, cols = shard.shape
        if dim == 0:
            return whole.at[pl.ds(pl.multiple_of(owner * rows + start, 16), count), :]
        return whole.at[
            pl.ds(pl.multiple_of(start, 16), count),
            pl.ds(pl.multiple_of(owner * cols, 128), cols),
        ]

    square = n_fs == 4
    if square:
        near_x = f + 1 - 2 * lax.rem(f, 2)
        near_y = lax.rem(f + 2, 4)
        far = lax.rem(near_x + 2, 4)
        targets = sources = [near_x, near_y]
    else:
        targets = [lax.rem(f + k, n_fs) for k in range(1, n_fs)]
        sources = [lax.rem(f + n_fs - k, n_fs) for k in range(1, n_fs)]

    direct, far_copies, over_sp, own = [], [], [], []
    for a, (shard, whole, dim) in enumerate(jobs):
        rows = shard.shape[0]
        less = 0 if a == last else relayed_rows(rows, paired)
        start = parity * less
        count = rows - less
        direct.append([
            pltpu.make_async_remote_copy(
                src_ref=shard.at[pl.ds(pl.multiple_of(start, 16), count), :],
                dst_ref=place(whole, shard, dim, f, start, count),
                send_sem=send_d.at[a, k], recv_sem=recv_d.at[a, k],
                device_id={"fs": target}, device_id_type=MESH_ID,
            )
            for k, target in enumerate(targets)
        ])
        halves = []
        if square:
            half = (count // 2 + 15) // 16 * 16
            for k, (owner, target, begin, size) in enumerate((
                (near_y, near_x, start, half), (near_x, near_y, start + half, count - half)
            )):
                piece = place(whole, shard, dim, owner, begin, size)
                halves.append(pltpu.make_async_remote_copy(
                    src_ref=piece, dst_ref=piece,
                    send_sem=send_r.at[a, k], recv_sem=recv_r.at[a, k],
                    device_id={"fs": target}, device_id_type=MESH_ID,
                ))
        far_copies.append(halves)
        across = []
        if less:
            lack = parity * (rows - less)
            for k, owner in enumerate(sources + ([far] if square else [])):
                piece = place(whole, shard, dim, owner, lack, less)
                across.append(pltpu.make_async_remote_copy(
                    src_ref=piece, dst_ref=piece,
                    send_sem=send_z.at[a, k], recv_sem=recv_z.at[a, k],
                    device_id={"sp": partner}, device_id_type=MESH_ID,
                ))
        over_sp.append(across)
        own.append(pltpu.make_async_copy(
            shard, place(whole, shard, dim, f, 0, rows), local_sem.at[a]
        ))

    def begin_array(a):
        if a <= last:
            for copy in direct[a]:
                copy.start()

    def finish_far(a):
        for copy in far_copies[a]:
            copy.wait_recv()
        for copy in over_sp[a][len(sources):]:
            copy.start()

    def tick(a):
        for copy in direct[a]:
            copy.wait_recv()
        for copy in far_copies[a]:
            copy.start()
        begin_array(a + ahead)
        for copy in over_sp[a][: len(sources)]:
            copy.start()
        if a >= 1:
            finish_far(a - 1)

    def complete(a):
        own[a].wait()
        for copy in over_sp[a]:
            copy.wait_recv()

    for a in range(ahead):
        begin_array(a)
    for copy in own:
        copy.start()

    rows = x_ref.shape[0]
    part = 32

    @pl.loop(0, rows // part)
    def _(i):
        at = pl.ds(pl.multiple_of(i * part, part), part)
        x = x_ref[at, :].astype(jnp.float32)
        scale = lax.rsqrt(jnp.mean(x * x, axis=-1, keepdims=True) + epsilon)
        normed[at, :] = (x * scale * gain_ref[...]).astype(jnp.bfloat16)

    depth = qd.shape[0]

    def project(weight, acc):
        acc[...] = jnp.zeros_like(acc)

        @pl.loop(0, n_fs)
        def _(i):
            at = pl.ds(pl.multiple_of(i * depth, depth), depth)
            acc[...] += jnp.dot(
                normed[:, at], weight[at, :], preferred_element_type=jnp.float32
            )

    mine = pl.ds(pl.multiple_of(s * rows, 16), rows)
    rr_all[mine, :] = jnp.dot(
        normed[...], rope_ref[...], preferred_element_type=jnp.float32
    ).astype(jnp.bfloat16)
    tick(0)
    tick(1)
    tick(2)
    complete(0)
    project(qd_all, acc_q)
    lq_all[t, :, :] = acc_q[...].astype(jnp.bfloat16)
    tick(3)
    complete(1)
    project(md_all, acc_m)
    lm_all[t, mine, :] = acc_m[...].astype(jnp.bfloat16)
    tick(4)
    complete(2)
    project(cv_all, acc_v)

    exchanges, passes = [], []
    for k in range(1, n_sp):
        peer = {"sp": lax.rem(s + k, n_sp)}
        exchanges.append(pltpu.make_async_remote_copy(
            src_ref=lm_all.at[t, mine, :], dst_ref=lm_all.at[t, mine, :],
            send_sem=sp_send.at[k - 1], recv_sem=sp_recv.at[k - 1],
            device_id=peer, device_id_type=MESH_ID,
        ))
        exchanges.append(pltpu.make_async_remote_copy(
            src_ref=rr_all.at[mine, :], dst_ref=rr_all.at[mine, :],
            send_sem=rr_send.at[k - 1], recv_sem=rr_recv.at[k - 1],
            device_id=peer, device_id_type=MESH_ID,
        ))
    tp_peers = [{"tp": lax.rem(t + k, n_tp)} for k in range(1, n_tp)]

    def to_tp(kind, source, landing):
        return [
            pltpu.make_async_remote_copy(
                src_ref=source, dst_ref=landing(k),
                send_sem=tp_send.at[kind, k], recv_sem=tp_recv.at[kind, k],
                device_id=peer, device_id_type=MESH_ID,
            )
            for k, peer in enumerate(tp_peers)
        ]

    query_copies = to_tp(0, lq_all.at[t], lambda k: lq_all.at[t])
    memory_copies = to_tp(1, lm_all.at[t], lambda k: lm_all.at[t])
    stat_copies = to_tp(2, stats, lambda k: stats_all.at[k])
    for copy in exchanges + query_copies:
        copy.start()
    tick(5)
    complete(3)
    project(cg_all, acc_g)

    @pl.loop(0, rows // part)
    def _(i):
        at = pl.ds(pl.multiple_of(i * part, part), part)
        gated = (acc_v[at, :] * jax.nn.sigmoid(acc_g[at, :])).astype(jnp.bfloat16)
        ext[pl.ds(pl.multiple_of(RIM + i * part, part), part), :] = gated.astype(jnp.float32)

    tail[...] = ext[pl.ds(rows, RIM), :].astype(jnp.bfloat16)
    rim_copy = pltpu.make_async_remote_copy(
        src_ref=tail, dst_ref=rim, send_sem=rim_sem.at[0], recv_sem=rim_sem.at[1],
        device_id={"sp": lax.rem(s + 1, n_sp)}, device_id_type=MESH_ID,
    )
    tick(6)

    @pl.when(s < n_sp - 1)
    def _():
        rim_copy.start()

    for copy in exchanges:
        copy.wait_recv()
    for copy in memory_copies:
        copy.start()

    @pl.when(s > 0)
    def _():
        rim_copy.wait_recv()
        ext[pl.ds(0, RIM), :] = rim[...].astype(jnp.float32)

    @pl.when(s == 0)
    def _():
        ext[pl.ds(0, RIM), :] = jnp.zeros((RIM, ext.shape[1]), jnp.float32)

    tap_count = taps_ref.shape[0]
    block = 64

    def convolve(c):
        cols = pl.ds(pl.multiple_of(c * 128, 128), 128)
        taps = taps_ref[:, cols].astype(jnp.float32)
        for r in range(0, rows, block):
            total = jnp.zeros((block, 128), jnp.float32)
            for j in range(tap_count):
                total = total + ext[
                    pl.ds(r + RIM - (tap_count - 1) + j, block), cols
                ] * taps[j : j + 1, :]
            sums[pl.ds(r, block), cols] = total

    tiles = ext.shape[1] // 128
    pl.loop(0, tiles // 2)(convolve)
    tick(7)
    pl.loop(tiles // 2, tiles)(convolve)

    @pl.loop(0, rows // part)
    def _(i):
        begin = pl.multiple_of(i * part, part)
        values = sums[pl.ds(begin, part), :]
        stats[pl.ds(begin, part), :] = jnp.broadcast_to(
            jnp.sum(values, axis=1, keepdims=True), (part, 128)
        )
        stats[pl.ds(pl.multiple_of(rows + begin, part), part), :] = jnp.broadcast_to(
            jnp.sum(values * values, axis=1, keepdims=True), (part, 128)
        )

    tick(8)
    for copy in stat_copies:
        copy.start()
    for copy in stat_copies:
        copy.wait_recv()

    channels = ext.shape[1] * n_tp

    @pl.loop(0, rows // part)
    def _(i):
        begin = pl.multiple_of(i * part, part)
        upper = pl.ds(begin, part)
        lower = pl.ds(pl.multiple_of(rows + begin, part), part)
        total, squares = stats[upper, :], stats[lower, :]
        for k in range(n_tp - 1):
            total = total + stats_all[k, upper, :]
            squares = squares + stats_all[k, lower, :]
        mean = total[:, :1] / channels
        spread = squares[:, :1] / channels - mean * mean
        shaped = (sums[upper, :] - mean) * lax.rsqrt(spread + epsilon)
        conv_ref[upper, :] = jax.nn.silu(
            shaped * cgain_ref[...] + cshift_ref[...]
        ).astype(jnp.bfloat16)

    finish_far(last)
    for a in range(4, last + 1):
        complete(a)
    for copy in query_copies + memory_copies:
        copy.wait_recv()
    for group in direct + far_copies + over_sp:
        for copy in group:
            copy.wait_send()
    for copy in exchanges + query_copies + memory_copies + stat_copies:
        copy.wait_send()

    @pl.when(s < n_sp - 1)
    def _():
        rim_copy.wait_send()


def gather_and_project(
    sizes, x, mix_gain, rope_weight, taps, channel_gain, channel_shift,
    qd, md, cv, cg, qu, ku, vu, ho, co,
):
    n_fs, n_sp, n_tp = sizes
    rows = x.shape[0]
    bf16, f32 = jnp.bfloat16, jnp.float32
    vmem = pl.BlockSpec(memory_space=pltpu.VMEM)
    hbm = pl.BlockSpec(memory_space=pl.ANY)

    def whole(w, dim=0):
        return (w.shape[0] * n_fs, w.shape[1]) if dim == 0 else (w.shape[0], w.shape[1] * n_fs)

    out_shapes = [
        ((n_tp, rows, qd.shape[1]), bf16), ((n_tp, n_sp * rows, md.shape[1]), bf16),
        ((n_sp * rows, rope_weight.shape[1]), bf16), ((rows, cv.shape[1]), bf16),
        (whole(qu), bf16), (whole(ku), bf16), (whole(vu), bf16),
        (whole(ho, 1), bf16), (whole(co, 1), bf16),
    ]
    dma = pltpu.SemaphoreType.DMA
    tp_others = max(n_tp - 1, 1)
    sp_others = max(n_sp - 1, 1)
    return pl.pallas_call(
        functools.partial(gather_kernel, sizes),
        out_shape=[jax.ShapeDtypeStruct(*o) for o in out_shapes],
        in_specs=[vmem] * 6 + [hbm] * 9,
        out_specs=[vmem] * 9,
        scratch_shapes=[
            pltpu.VMEM(whole(qd), bf16), pltpu.VMEM(whole(md), bf16),
            pltpu.VMEM(whole(cv), bf16), pltpu.VMEM(whole(cg), bf16),
            pltpu.VMEM(x.shape, bf16), pltpu.VMEM((rows, qd.shape[1]), f32),
            pltpu.VMEM((rows, md.shape[1]), f32),
            pltpu.VMEM((rows, cv.shape[1]), f32), pltpu.VMEM((rows, cv.shape[1]), f32),
            pltpu.VMEM((rows + RIM, cv.shape[1]), f32),
            pltpu.VMEM((RIM, cv.shape[1]), bf16), pltpu.VMEM((RIM, cv.shape[1]), bf16),
            pltpu.VMEM((rows, cv.shape[1]), f32), pltpu.VMEM((2 * rows, 128), f32),
            pltpu.VMEM((tp_others, 2 * rows, 128), f32),
            dma((9, n_fs - 1)), dma((9, n_fs - 1)), dma((9, 2)), dma((9, 2)),
            dma((9, n_fs - 1)), dma((9, n_fs - 1)), dma((9,)), dma((2,)),
            dma((sp_others,)), dma((sp_others,)), dma((sp_others,)), dma((sp_others,)),
            dma((3, tp_others)), dma((3, tp_others)),
        ],
        compiler_params=pltpu.CompilerParams(
            collective_id=0, has_side_effects=True, vmem_limit_bytes=56 * 1024 * 1024
        ),
    )(
        x, mix_gain[None, :], rope_weight, taps, channel_gain[None, :], channel_shift[None, :],
        qd, md, cv, cg, qu, ku, vu, ho, co,
    )


def key_block(key_count):
    block_size = key_count
    while block_size > 2048 and block_size % 2 == 0:
        block_size = block_size // 2
    return block_size


def sum_groups(partial):
    count = lax.axis_size("tp")
    if count != 2:
        return lax.psum(partial, "tp")
    other = lax.ppermute(partial, "tp", [(0, 1), (1, 0)])
    return (partial.astype(jnp.float32) + other.astype(jnp.float32)).astype(jnp.bfloat16)


def local(
    tokens,
    mix_gain,
    query_down,
    memory_down,
    rope_weight,
    query_up,
    key_up,
    value_up,
    latent_gain,
    memory_gain,
    query_gain,
    key_gain,
    conv_value,
    conv_gate,
    conv_kernel,
    channel_gain,
    channel_shift,
    heads_out,
    conv_out,
):
    own_rows = tokens[0]
    (
        query_parts, memory_parts, rope_piece, conv_result,
        up_query, up_keys, up_values, out_heads, out_conv,
    ) = gather_and_project(
        (lax.axis_size("fs"), lax.axis_size("sp"), lax.axis_size("tp")),
        own_rows, mix_gain, rope_weight, conv_kernel, channel_gain, channel_shift,
        query_down, memory_down, conv_value, conv_gate,
        query_up, key_up, value_up, heads_out, conv_out,
    )
    row_count = own_rows.shape[0]
    whole_query = jnp.concatenate(list(query_parts), axis=1)
    whole_memory = jnp.concatenate(list(memory_parts), axis=1)
    query_normed = norm_rows(whole_query.astype(jnp.float32), latent_gain).astype(jnp.bfloat16)
    memory_piece = norm_rows(whole_memory.astype(jnp.float32), memory_gain).astype(jnp.bfloat16)
    positions = lax.axis_index("sp") * row_count + jnp.arange(row_count, dtype=jnp.int32)
    cosine_table, sine_table = rope_tables(positions)
    queries = heads_query(query_normed, up_query, query_gain, cosine_table, sine_table)
    head_count = queries.shape[1]
    query_segment = positions // SEG
    score_scale = QK_DIM ** (-0.5)
    def attend(state_carry, key_rows, value_rows, key_pos):
        running_max, row_total, weighted = state_carry
        scores = (
            jnp.einsum("qhd,khd->qhk", queries, key_rows, preferred_element_type=jnp.float32)
            * score_scale
        )
        allowed = ((key_pos // SEG)[None, :] <= query_segment[:, None])[:, None, :]
        scores = jnp.where(allowed, scores, masked_score)
        new_max = jnp.maximum(running_max, jnp.max(scores, axis=2))
        weights = jnp.where(allowed, jnp.exp(scores - new_max[:, :, None]), 0.0)
        factor = jnp.exp(running_max - new_max)
        row_total = row_total * factor + jnp.sum(weights, axis=2)
        weighted = weighted * factor[:, :, None] + jnp.einsum(
            "qhk,khd->qhd",
            weights.astype(jnp.bfloat16),
            value_rows,
            preferred_element_type=jnp.float32,
        )
        return (new_max, row_total, weighted)

    initial = (
        jnp.full((row_count, head_count), masked_score, jnp.float32),
        jnp.zeros((row_count, head_count), jnp.float32),
        jnp.zeros((row_count, head_count, V_DIM), jnp.float32),
    )
    def block_keys(block_start, block_size):
        memory_block = lax.dynamic_slice_in_dim(memory_piece, block_start, block_size, 0)
        rope_block = lax.dynamic_slice_in_dim(rope_piece, block_start, block_size, 0)
        key_pos = block_start + jnp.arange(block_size, dtype=jnp.int32)
        cosine_keys, sine_keys = rope_tables(key_pos)
        key_rows = heads_key(memory_block, rope_block, up_keys, key_gain, cosine_keys, sine_keys)
        value_rows = (
            jnp.dot(memory_block, up_values, preferred_element_type=jnp.float32)
            .astype(jnp.bfloat16)
            .reshape(block_size, head_count, V_DIM)
        )
        return (key_rows, value_rows, key_pos)

    key_count = memory_piece.shape[0]
    block_size = key_block(key_count)

    def step(block_index, running):
        key_rows, value_rows, key_pos = block_keys(block_index * block_size, block_size)
        return attend(running, key_rows, value_rows, key_pos)

    final_state = lax.fori_loop(0, key_count // block_size, step, initial)
    running_max, row_total, weighted = final_state
    attention = (
        (weighted / row_total[:, :, None])
        .astype(jnp.bfloat16)
        .reshape(row_count, head_count * V_DIM)
    )
    mixer_rows = jnp.concatenate([attention, conv_result], axis=1)
    out_weight = jnp.concatenate([out_heads, out_conv], axis=0)
    partial_sum = jnp.dot(mixer_rows, out_weight, preferred_element_type=jnp.float32)
    mixed = sum_groups(partial_sum.astype(jnp.bfloat16))
    return mixed[None]


def table_rows(count):
    inverse_freq = 1.0 / np.float32(rope_base) ** (
        np.arange(0, QK_ROPE, 2, dtype=np.float32) / np.float32(QK_ROPE)
    )
    angles = inverse_freq[:, None] * np.arange(count, dtype=np.float32)[None, :]
    angles = angles.astype(np.float64)
    return np.cos(angles).astype(np.float32), np.sin(angles).astype(np.float32)


def dot_heads(left, right):
    return lax.dot_general(
        left, right, (((0,), (0,)), ((), ())), preferred_element_type=jnp.float32
    )


def swapped_rows(count, part):
    return (count * part // 16) // 16 * 16


def fused_kernel(
    sizes,
    x_hbm, gain_hbm, rope_hbm, taps_hbm, cgain_hbm, cshift_hbm,
    lgain_hbm, mgain_hbm, qgain_hbm, kgain_hbm, cos_hbm, sin_hbm,
    qd, md, ku, vu, qu, cv, cg, ho, co,
    mine_hbm, other_hbm,
    gain_ref, rope_ref, taps_ref, cgain_ref, cshift_ref,
    lgain_ref, mgain_ref, qgain_ref, kgain_ref, cos_ref, sin_ref,
    qd_all, md_all, ku_all, vu_all, qu_all, cv_all, cg_all, ho_all, co_all,
    x_all, normed, lq_all, lm_all, mem_all, rr_all, qn_t, q_t, k_t, v_t,
    turned, ropesq, qcol, kcol, bias, scores,
    att_t, att_out, att_all, conv_s, acc_v, acc_out, gate_out, gate_in, ext, rim_out, rim, sums, stats, stats_all,
    mine_ref,
    send_d, recv_d, send_r, recv_r, send_z, recv_z, local_sem, small_sem, rim_sem, x_sem,
    part_sem, sp_send, sp_recv, fw_send, fw_recv, tp_send, tp_recv, out_send, out_recv, store_sem,
):
    n_fs, n_sp, n_tp = sizes
    f = lax.axis_index("fs")
    s = lax.axis_index("sp")
    t = lax.axis_index("tp")
    parity = lax.rem(s, 2)
    couple = lax.div(s, 2)
    couples = n_sp // 2
    partner = {"sp": s + 1 - 2 * parity}
    twin = {"tp": 1 - t}
    even, odd = parity == 0, parity == 1

    barrier = pltpu.get_barrier_semaphore()
    for axis, at, count in (("fs", f, n_fs), ("sp", s, n_sp), ("tp", t, n_tp)):
        for k in range(1, count):
            pl.semaphore_signal(
                barrier, inc=1, device_id={axis: lax.rem(at + k, count)}, device_id_type=MESH_ID
            )

    slots = 3
    rows = x_hbm.shape[0]
    x_own = pltpu.make_async_copy(x_hbm, x_all.at[parity], x_sem.at[0])
    x_own.start()
    small = [
        pltpu.make_async_copy(source, landing, small_sem.at[i % slots])
        for i, (source, landing) in enumerate((
            (gain_hbm, gain_ref), (rope_hbm, rope_ref), (taps_hbm, taps_ref),
            (cgain_hbm, cgain_ref), (cshift_hbm, cshift_ref), (lgain_hbm, lgain_ref),
            (mgain_hbm, mgain_ref), (qgain_hbm, qgain_ref), (kgain_hbm, kgain_ref),
            (cos_hbm, cos_ref), (sin_hbm, sin_ref),
        ))
    ]
    for copy in small[:slots]:
        copy.start()

    def remote(source, landing, send, recv, device):
        return pltpu.make_async_remote_copy(
            src_ref=source, dst_ref=landing, send_sem=send, recv_sem=recv,
            device_id=device, device_id_type=MESH_ID,
        )

    share = rows // n_tp
    slab = pl.ds(pl.multiple_of(t * share, 16), share)
    x_send = remote(
        x_hbm.at[slab, :], x_all.at[parity, slab, :], x_sem.at[1], x_sem.at[2], partner
    )
    theirs = x_all.at[1 - parity, slab, :]
    x_forward = remote(theirs, theirs, x_sem.at[3], x_sem.at[4], twin)

    near_x = f + 1 - 2 * lax.rem(f, 2)
    near_y = lax.rem(f + 2, 4)
    far = lax.rem(near_x + 2, 4)
    sources = [near_x, near_y]

    def job(a, shard, whole, swap=None, dim=0, first=0, count=None):
        depth, cols = shard.shape
        count = depth if count is None else count
        lane, mine, lacking, giving = swap or (0, 0, 0, 0)
        lack, give = swapped_rows(count, lacking), swapped_rows(count, giving)
        kept = count - lack

        def place(owner, start, size):
            if dim == 0:
                return whole.at[pl.ds(pl.multiple_of(owner * depth + start, 16), size), :]
            return whole.at[
                pl.ds(pl.multiple_of(start, 16), size),
                pl.ds(pl.multiple_of(owner * cols, 128), cols),
            ]

        start = first + mine * lack
        direct = [
            remote(
                shard.at[pl.ds(start, kept), :], place(f, start, kept),
                send_d.at[a % slots, k], recv_d.at[a, k], {"fs": target},
            )
            for k, target in enumerate(sources)
        ]
        half = (kept // 2 + 15) // 16 * 16
        relays = []
        for k, (owner, target, begin, size) in enumerate((
            (near_y, near_x, start, half), (near_x, near_y, start + half, kept - half)
        )):
            piece = place(owner, begin, size)
            relays.append(remote(
                piece, piece, send_r.at[a % slots, k], recv_r.at[a, k], {"fs": target}
            ))
        gives, lacks = [], []
        if swap:
            for k, owner in enumerate(sources + [far]):
                sems = (send_z.at[lane, k], recv_z.at[lane, k], partner)
                if give:
                    piece = place(owner, first + mine * (count - give), give)
                    gives.append(remote(piece, piece, *sems))
                if lack:
                    piece = place(owner, first + (1 - mine) * kept, lack)
                    lacks.append(remote(piece, piece, *sems))
        own = pltpu.make_async_copy(
            shard.at[pl.ds(first, count), :], place(f, first, count), local_sem.at[a % slots]
        )
        return direct, relays, gives, own, lacks

    def half_columns(shard):
        width = shard.shape[1] // 2
        return shard.at[:, pl.ds(pl.multiple_of(parity * width, 128), width)]

    wide = cv.shape[1] // 2
    side = pl.ds(pl.multiple_of(parity * wide, 128), wide)
    half_rows = ho.shape[0] // 2
    last_rows = half_rows // 4

    def swapping(lane, even_lacks, odd_lacks, *rest):
        shard, whole, *rest = rest
        return [
            (even, shard, whole, (lane, 0, even_lacks, odd_lacks), *rest),
            (odd, shard, whole, (lane, 1, odd_lacks, even_lacks), *rest),
        ]

    plan = [
        [(even, qd, qd_all), (odd, md, md_all)],
        [(None, half_columns(ku), ku_all)], [(None, half_columns(vu), vu_all)],
        [(None, half_columns(qu), qu_all)],
        swapping(0, 8, 8, ho, ho_all, 1, 0, half_rows),
        [(None, half_columns(cv), cv_all)], [(None, half_columns(cg), cg_all)],
        swapping(1, 8, 8, ho, ho_all, 1, half_rows, half_rows),
        swapping(2, 6, 4, co, co_all, 1, 0, half_rows),
        [(None, co, co_all, None, 1, half_rows, half_rows - last_rows)],
        [(None, co, co_all, None, 1, 2 * half_rows - last_rows, last_rows)],
    ]
    jobs = [[(who[0], job(a, *who[1:])) for who in group] for a, group in enumerate(plan)]
    last = len(jobs) - 1
    lanes = [a for a, group in enumerate(plan) if len(group[0]) > 3 and group[0][3]]

    def each(a, action):
        for condition, parts in jobs[a]:
            if condition is None:
                action(parts)
            else:
                pl.when(condition)(functools.partial(action, parts))

    def sent(a, kind):
        def go(parts):
            for copy in parts[kind]:
                copy.wait_send()

        if a >= 0:
            each(a, go)

    def begin_array(a):
        def start(parts):
            for copy in parts[0]:
                copy.start()
            parts[3].start()

        if a <= last:
            sent(a - slots, 0)
            each(a, start)

    def finish_far(a):
        def go(parts):
            with jax.named_scope(f"far_{a}"):
                for copy in parts[1]:
                    copy.wait_recv()
            for copy in parts[2][len(sources):]:
                copy.start()

        each(a, go)

    def tick(a):
        def go(parts):
            with jax.named_scope(f"direct_{a}"):
                for copy in parts[0]:
                    copy.wait_recv()
                parts[3].wait()
            for copy in parts[1]:
                copy.start()

        def swap(parts):
            for copy in parts[2][: len(sources)]:
                copy.start()

        sent(a - slots, 1)
        each(a, go)
        begin_array(a + slots)
        if a in lanes:
            each(a, swap)

    def complete(a):
        def go(parts):
            with jax.named_scope(f"across_{a}"):
                for copy in parts[4]:
                    copy.wait_recv()

        each(a, go)

    with jax.named_scope("entry"):
        pl.semaphore_wait(barrier, n_fs + n_sp + n_tp - 3)
    x_send.start()
    for a in range(slots):
        begin_array(a)
    with jax.named_scope("small_wait"):
        for r in range(0, len(small), slots):
            if r:
                for copy in small[r : r + slots]:
                    copy.start()
            for copy in small[r : r + slots]:
                copy.wait()
        x_own.wait()

    part = 32

    def norm_block(b):
        @pl.loop(0, rows // part)
        def _(i):
            at = pl.ds(pl.multiple_of(i * part, part), part)
            x = x_all[b, at, :].astype(jnp.float32)
            scale = lax.rsqrt(jnp.mean(x * x, axis=-1, keepdims=True) + epsilon)
            normed[b, at, :] = (x * scale * gain_ref[...]).astype(jnp.bfloat16)

        rr_all[2 * couple + b] = lax.dot_general(
            rope_ref[...], normed[b], (((1,), (1,)), ((), ())), preferred_element_type=jnp.float32
        ).astype(jnp.bfloat16)

    norm_block(parity)
    half_rope = QK_ROPE // 2

    def column(row_ref, col_ref):
        shape = (QK_DIM, QK_DIM)
        here = lax.broadcasted_iota(jnp.int32, shape, 0) == lax.broadcasted_iota(jnp.int32, shape, 1)
        spread_row = jnp.broadcast_to(row_ref[...], shape)
        picked = jnp.sum(jnp.where(here, spread_row, 0.0), axis=1, keepdims=True)
        col_ref[...] = jnp.broadcast_to(picked, col_ref.shape)

    column(qgain_ref, qcol)
    column(kgain_ref, kcol)

    @pl.loop(2 * couple + 2, n_sp)
    def _(j):
        mem_all[j] = jnp.zeros(mem_all.shape[1:], jnp.bfloat16)
        rr_all[j] = jnp.zeros(rr_all.shape[1:], jnp.bfloat16)

    @pl.loop(0, n_sp)
    def _(j):
        shape = (rows, 2 * rows)
        key_at = j * rows + lax.broadcasted_iota(jnp.int32, shape, 0)
        query_at = 2 * couple * rows + lax.broadcasted_iota(jnp.int32, shape, 1)
        bias[j] = jnp.where(
            lax.div(key_at, SEG) <= lax.div(query_at, SEG), 0.0, masked_score
        )

    tick(0)
    with jax.named_scope("x_wait"):
        x_send.wait_recv()
    x_forward.start()
    tick(1)
    with jax.named_scope("x_forward"):
        x_forward.wait_recv()
    norm_block(1 - parity)
    tick(2)
    finish_far(0)

    def project(weight, b):
        return jnp.dot(normed[b], weight[...], preferred_element_type=jnp.float32)

    lat = md.shape[1]
    lat_q = qd.shape[1]
    held = pl.ds(pl.multiple_of(t * lat, lat), lat)
    query_across = remote(lq_all.at[t], lq_all.at[t], part_sem.at[0], part_sem.at[1], partner)
    query_copy = remote(lq_all.at[t], lq_all.at[t], tp_send.at[0], tp_recv.at[0], twin)
    memory_copy = remote(lm_all.at[t], lm_all.at[t], tp_send.at[1], tp_recv.at[1], twin)
    stat_copy = remote(stats, stats_all, tp_send.at[2], tp_recv.at[2], twin)
    gate_across = remote(gate_out, gate_in, part_sem.at[2], part_sem.at[3], partner)

    complete(0)

    @pl.when(even)
    def _():
        for b in range(2):
            lq_all[t, b] = project(qd_all, b).astype(jnp.bfloat16)
        query_across.start()
        query_copy.start()

    @pl.when(odd)
    def _():
        for b in range(2):
            lm_all[t, b] = project(md_all, b).astype(jnp.bfloat16)
        memory_copy.start()

    tick(3)

    def normed_columns(parts, width, gain_at, put):
        @pl.loop(0, rows // 128)
        def _(i):
            at = pl.ds(pl.multiple_of(i * 128, 128), 128)
            pieces = [parts(g, at).astype(jnp.float32) for g in range(n_tp)]
            total = sum(jnp.sum(p * p, axis=-1, keepdims=True) for p in pieces)
            scale = lax.rsqrt(total / (width * n_tp) + epsilon)
            for g in range(n_tp):
                shaped = (pieces[g] * scale * gain_at(g * width, width)).astype(jnp.bfloat16)
                put(g * width, width, at, shaped.astype(jnp.float32).T.astype(jnp.bfloat16))

    pair = pl.ds(2 * couple, 2)
    both = mem_all.at[pair, held, :]
    back = remote(both, both, part_sem.at[4], part_sem.at[5], partner)
    back_forward = remote(both, both, fw_send.at[couples - 1], fw_recv.at[couples - 1], twin)
    onward, forwards = [], []
    for d in range(1, couples):
        group = []
        later = lax.rem(couple + d, couples)
        for e in range(2):
            target = {"sp": 2 * later + e}
            group.append((
                remote(
                    mem_all.at[pair, held, :], mem_all.at[pair, held, :],
                    sp_send.at[d - 1, e, 0], sp_recv.at[d - 1, 0], target,
                ),
                remote(
                    rr_all.at[pair], rr_all.at[pair],
                    sp_send.at[d - 1, e, 1], sp_recv.at[d - 1, 1], target,
                ),
            ))
        onward.append(group)
        earlier = mem_all.at[pl.ds(2 * lax.rem(couple + couples - d, couples), 2), held, :]
        forwards.append(remote(earlier, earlier, fw_send.at[d - 1], fw_recv.at[d - 1], twin))

    @pl.when(odd)
    def _():
        with jax.named_scope("memory_wait"):
            memory_copy.wait_recv()
        for b in (1, 0):
            def put_memory(begin, width, at, piece, b=b):
                mem_all[2 * couple + b, begin : begin + width, at] = piece

            normed_columns(
                lambda g, at, b=b: lm_all[g, b, at, :], lat,
                lambda begin, width: mgain_ref[:, begin : begin + width], put_memory,
            )
        for d in range(1, couples):
            @pl.when(couple + d < couples)
            def _(d=d):
                for e in range(2):
                    for copy in onward[d - 1][e]:
                        copy.start()
        back.start()

    finish_far(1)
    tick(4)
    finish_far(2)

    @pl.when(even)
    def _():
        with jax.named_scope("back_wait"):
            back.wait_recv()
        back_forward.start()

    tick(5)
    finish_far(3)

    @pl.when(odd)
    def _():
        with jax.named_scope("query_across"):
            query_across.wait_recv()
        query_copy.start()


    @pl.when(even)
    def _():
        with jax.named_scope("back_forward"):
            back_forward.wait_recv()

    def expand(j):
        k_t[j] = dot_heads(ku_all[...], mem_all[j])
        v_t[j] = dot_heads(vu_all[...], mem_all[j]).astype(jnp.bfloat16)
        shared = rr_all[j].astype(jnp.float32)
        ropesq[j] = jnp.sum(shared * shared, axis=0, keepdims=True)
        shared = shared * kcol[QK_NOPE:, :]
        front, back_half = shared[:half_rope], shared[half_rope:]
        at = pl.ds(pl.multiple_of(j * rows, rows), rows)
        cosine, sine = cos_ref[:, at], sin_ref[:, at]
        turned[j] = jnp.concatenate(
            [front * cosine - back_half * sine, front * sine + back_half * cosine], axis=0
        )

    pl.loop(2 * couple, n_sp)(expand)
    for d in range(1, couples):
        @pl.when(couple >= d)
        def _(d=d):
            with jax.named_scope(f"behind_{d}"):
                for copy in onward[d - 1][0]:
                    copy.wait_recv()
            forwards[d - 1].start()
    tick(6)
    finish_far(4)
    with jax.named_scope("query_wait"):
        query_copy.wait_recv()
    for b in range(2):
        def put_query(begin, width, at, piece, b=b):
            at = pl.ds(pl.multiple_of(b * rows + at.start, 128), at.size)
            qn_t[begin : begin + width, at] = piece

        normed_columns(
            lambda g, at, b=b: lq_all[g, b, at, :], lat_q,
            lambda begin, width: jnp.concatenate(
                [lgain_ref[r : r + 1, :] for r in range(begin // 128, (begin + width) // 128)],
                axis=1,
            ),
            put_query,
        )
    for d in range(1, couples):
        @pl.when(couple >= d)
        def _(d=d):
            with jax.named_scope(f"forward_{d}"):
                forwards[d - 1].wait_recv()
    pl.loop(0, 2 * couple)(expand)
    q_t[...] = dot_heads(qu_all[...], qn_t[...])
    heads = qu.shape[1] // 2 // QK_DIM
    here = pl.ds(pl.multiple_of(2 * couple * rows, rows), 2 * rows)
    score_scale = QK_DIM ** (-0.5)

    def head(h):
        q = q_t[pl.ds(pl.multiple_of(h * QK_DIM, QK_DIM), QK_DIM), :]
        q = q * lax.rsqrt(jnp.mean(q * q, axis=0, keepdims=True) + epsilon) * qcol[...]
        front, back_half = q[QK_NOPE : QK_NOPE + half_rope], q[QK_NOPE + half_rope :]
        cosine, sine = cos_ref[:, here], sin_ref[:, here]
        q = jnp.concatenate(
            [
                q[:QK_NOPE],
                front * cosine - back_half * sine,
                front * sine + back_half * cosine,
            ],
            axis=0,
        ).astype(jnp.bfloat16)
        krow = pl.ds(pl.multiple_of(h * QK_NOPE, QK_NOPE), QK_NOPE)
        vrow = pl.ds(pl.multiple_of(h * V_DIM, V_DIM), V_DIM)
        top = jnp.full((1, 2 * rows), masked_score, jnp.float32)
        for j in range(n_sp):
            nope = k_t[j, krow, :]
            scale = lax.rsqrt(
                (jnp.sum(nope * nope, axis=0, keepdims=True) + ropesq[j]) / QK_DIM + epsilon
            )
            key = jnp.concatenate(
                [nope * scale * kcol[:QK_NOPE, :], turned[j] * scale], axis=0
            ).astype(jnp.bfloat16)
            block = dot_heads(key, q) + bias[j]
            scores[j] = block
            top = jnp.maximum(top, jnp.max(block, axis=0, keepdims=True))
        total = jnp.zeros((1, 2 * rows), jnp.float32)
        summed = jnp.zeros((V_DIM, 2 * rows), jnp.float32)
        for j in range(n_sp):
            weight = jnp.exp((scores[j] - top) * score_scale)
            total = total + jnp.sum(weight, axis=0, keepdims=True)
            summed = summed + jnp.dot(
                v_t[j, vrow, :], weight.astype(jnp.bfloat16),
                preferred_element_type=jnp.float32,
            )
        att_t[vrow, :] = summed / total

    pl.loop(0, heads // 2)(head)
    tick(7)
    finish_far(5)
    for b in range(2):
        acc_v[b] = project(cv_all, b)
    pl.loop(heads // 2, heads)(head)
    value_rows = heads * V_DIM
    own_rows = pl.ds(pl.multiple_of(parity * value_rows, value_rows), value_rows)
    their_lanes = pl.ds(pl.multiple_of((1 - parity) * rows, rows), rows)
    own_lanes = pl.ds(pl.multiple_of(parity * rows, rows), rows)
    att_across = remote(
        att_out, att_all.at[own_rows, :], part_sem.at[6], part_sem.at[7], partner
    )
    att_out[...] = att_t[:, their_lanes].astype(jnp.bfloat16)
    att_across.start()
    att_all[own_rows, :] = att_t[:, own_lanes].astype(jnp.bfloat16)
    tick(8)
    finish_far(6)
    opposite = pl.ds(pl.multiple_of((1 - parity) * wide, 128), wide)
    body_rows, halo = pl.ds(RIM, rows), pl.ds(0, RIM)

    def gate(b):
        gates = project(cg_all, b)
        return (acc_v[b] * jax.nn.sigmoid(gates)).astype(jnp.bfloat16)

    end = slice(rows - RIM, rows)
    later_rim = remote(
        rim_out, rim.at[parity], rim_sem.at[0], rim_sem.at[1 + parity],
        {"sp": 2 * lax.rem(couple + 1, couples)},
    )
    has_later, has_earlier = couple < couples - 1, jnp.logical_and(even, couple > 0)
    lower = gate(0)

    @pl.when(even)
    def _():
        ext[body_rows, side] = lower.astype(jnp.float32)
        ext[halo, :] = jnp.zeros((RIM, ext.shape[1]), jnp.float32)
        gate_out[halo, :] = lower[end]

    @pl.when(odd)
    def _():
        gate_out[halo, :] = jnp.zeros((RIM, wide), jnp.bfloat16)
        gate_out[body_rows, :] = lower
        gate_across.start()
        ext[halo, side] = lower[end].astype(jnp.float32)

    upper = gate(1)
    rim_out[...] = upper[end]

    @pl.when(has_later)
    def _():
        later_rim.start()

    @pl.when(even)
    def _():
        gate_out[body_rows, :] = upper
        gate_across.start()

    @pl.when(odd)
    def _():
        ext[body_rows, side] = upper.astype(jnp.float32)

    tick(9)

    @pl.when(has_earlier)
    def _():
        with jax.named_scope("rim_wait"):
            for g in range(2):
                remote(
                    rim_out, rim.at[g], rim_sem.at[0], rim_sem.at[1 + g], partner
                ).wait_recv()
        for g in range(2):
            ext[halo, g * wide : (g + 1) * wide] = rim[g].astype(jnp.float32)

    tap_count = taps_ref.shape[0]
    block = 64

    def convolve(c):
        cols = pl.ds(pl.multiple_of(c * 128, 128), 128)
        taps = taps_ref[:, cols].astype(jnp.float32)
        for r in range(0, rows, block):
            total = jnp.zeros((block, 128), jnp.float32)
            for j in range(tap_count):
                total = total + ext[
                    pl.ds(r + RIM - (tap_count - 1) + j, block), cols
                ] * taps[j : j + 1, :]
            sums[pl.ds(r, block), cols] = total

    tiles = wide // 128
    pl.loop(parity * tiles, (parity + 1) * tiles)(convolve)
    with jax.named_scope("gate_wait"):
        gate_across.wait_recv()
    ext[body_rows, opposite] = gate_in[body_rows, :].astype(jnp.float32)

    @pl.when(odd)
    def _():
        ext[halo, opposite] = gate_in[halo, :].astype(jnp.float32)

    finish_far(7)
    pl.loop((1 - parity) * tiles, (2 - parity) * tiles)(convolve)
    finish_far(8)
    tick(10)

    @pl.loop(0, rows // part)
    def _(i):
        begin = pl.multiple_of(i * part, part)
        values = sums[pl.ds(begin, part), :]
        stats[pl.ds(begin, part), :] = jnp.broadcast_to(
            jnp.sum(values, axis=1, keepdims=True), (part, 128)
        )
        stats[pl.ds(pl.multiple_of(rows + begin, part), part), :] = jnp.broadcast_to(
            jnp.sum(values * values, axis=1, keepdims=True), (part, 128)
        )

    stat_copy.start()
    with jax.named_scope("att_wait"):
        att_across.wait_recv()
    att = att_all[...].astype(jnp.float32).T.astype(jnp.bfloat16)
    span = ho.shape[1]

    def gain_rows(left, weight, begin, size=half_rows, first=False):
        band = slice(begin, begin + size)

        @pl.loop(0, n_fs)
        def _(i):
            cols = pl.ds(pl.multiple_of(i * span, span), span)
            product = jnp.dot(left[:, band], weight[band, cols], preferred_element_type=jnp.float32)
            acc_out[:, cols] = product if first else acc_out[:, cols] + product

    complete(4)
    gain_rows(att, ho_all, 0, first=True)
    with jax.named_scope("stat_wait"):
        stat_copy.wait_recv()
    channels = ext.shape[1] * n_tp

    @pl.loop(0, rows // part)
    def _(i):
        begin = pl.multiple_of(i * part, part)
        upper = pl.ds(begin, part)
        lower = pl.ds(pl.multiple_of(rows + begin, part), part)
        total = stats[upper, :] + stats_all[upper, :]
        squares = stats[lower, :] + stats_all[lower, :]
        mean = total[:, :1] / channels
        spread = squares[:, :1] / channels - mean * mean
        shaped = (sums[upper, :] - mean) * lax.rsqrt(spread + epsilon)
        conv_s[upper, :] = jax.nn.silu(
            shaped * cgain_ref[...] + cshift_ref[...]
        ).astype(jnp.bfloat16)

    complete(7)
    gain_rows(att, ho_all, half_rows)
    complete(8)
    gain_rows(conv_s, co_all, 0)
    finish_far(9)
    gain_rows(conv_s, co_all, half_rows, half_rows - last_rows)
    rest = slice(2 * half_rows - last_rows, 2 * half_rows)
    outs, stores = [], []
    for i, owner in enumerate([f, near_x, near_y, far]):
        cols = pl.ds(pl.multiple_of(owner * span, span), span)
        outs.append(remote(
            mine_ref.at[:, cols], other_hbm.at[:, cols], out_send.at[i], out_recv.at[i], twin
        ))
        stores.append(pltpu.make_async_copy(
            mine_ref.at[:, cols], mine_hbm.at[:, cols], store_sem.at[i]
        ))
        if i == n_fs - 1:
            finish_far(last)
        mine_ref[:, cols] = (
            acc_out[:, cols]
            + jnp.dot(
                conv_s[:, rest], co_all[rest, cols],
                preferred_element_type=jnp.float32,
            )
        ).astype(jnp.bfloat16)
        outs[i].start()
        stores[i].start()

    for a in range(last + 1 - slots, last + 1):
        sent(a, 0)
        sent(a, 1)
    for a in lanes:
        sent(a, 2)
    for copy in (x_send, x_forward, query_copy, stat_copy, gate_across, att_across):
        copy.wait_send()

    @pl.when(even)
    def _():
        query_across.wait_send()
        back_forward.wait_send()

    @pl.when(odd)
    def _():
        memory_copy.wait_send()
        back.wait_send()
        for d in range(1, couples):
            @pl.when(couple + d < couples)
            def _(d=d):
                for e in range(2):
                    for copy in onward[d - 1][e]:
                        copy.wait_send()

    for d in range(1, couples):
        @pl.when(couple >= d)
        def _(d=d):
            forwards[d - 1].wait_send()

    @pl.when(has_later)
    def _():
        later_rim.wait_send()

    with jax.named_scope("out_wait"):
        for copy in outs + stores:
            copy.wait()


def join_kernel(mine_hbm, other_hbm, out_hbm, mine, other, whole, loads, stores):
    rows = mine.shape[0]
    pieces = loads.shape[0]
    step = rows // pieces

    def copies(i):
        at = pl.ds(i * step, step)
        return (
            pltpu.make_async_copy(mine_hbm.at[at, :], mine.at[at, :], loads.at[i, 0]),
            pltpu.make_async_copy(other_hbm.at[at, :], other.at[at, :], loads.at[i, 1]),
            pltpu.make_async_copy(whole.at[at, :], out_hbm.at[at, :], stores.at[i]),
        )

    plan = [copies(i) for i in range(pieces)]
    for one, two, _ in plan:
        one.start()
        two.start()
    for i, (one, two, back) in enumerate(plan):
        one.wait()
        two.wait()
        at = pl.ds(i * step, step)
        whole[at, :] = (
            mine[at, :].astype(jnp.float32) + other[at, :].astype(jnp.float32)
        ).astype(jnp.bfloat16)
        back.start()
    for _, _, back in plan:
        back.wait()


def join(mine, other):
    pieces = 4
    buffer = pltpu.VMEM(mine.shape, mine.dtype)
    dma = pltpu.SemaphoreType.DMA
    hbm = pl.BlockSpec(memory_space=pl.ANY)
    return pl.pallas_call(
        join_kernel,
        out_shape=jax.ShapeDtypeStruct(mine.shape, mine.dtype),
        in_specs=[hbm] * 2,
        out_specs=hbm,
        scratch_shapes=[buffer] * 3 + [dma((pieces, 2)), dma((pieces,))],
        compiler_params=pltpu.CompilerParams(vmem_limit_bytes=60 * 1024 * 1024),
    )(mine, other)


def fused_call(
    sizes, x, mix_gain, rope_weight, taps, channel_gain, channel_shift,
    latent_gain, memory_gain, query_gain, key_gain,
    qd, md, cv, cg, qu, ku, vu, ho, co,
):
    n_fs, n_sp, n_tp = sizes
    rows, model = x.shape
    bf16, f32 = jnp.bfloat16, jnp.float32
    hbm = pl.BlockSpec(memory_space=pl.ANY)
    cosine, sine = table_rows(n_sp * rows)
    small = [
        mix_gain[None, :], rope_weight.T, taps, channel_gain[None, :], channel_shift[None, :],
        latent_gain.reshape(-1, 128), memory_gain[None, :], query_gain[None, :],
        key_gain[None, :], jnp.asarray(cosine), jnp.asarray(sine),
    ]

    def whole(w, dim=0, parts=1):
        rows_w, cols_w = w.shape[0], w.shape[1] // parts
        return (rows_w * n_fs, cols_w) if dim == 0 else (rows_w, cols_w * n_fs)

    def scratch(*shape, dtype=f32):
        return pltpu.VMEM(shape, dtype)

    dma = pltpu.SemaphoreType.DMA
    channels, lat = cv.shape[1], md.shape[1] * n_tp
    rope = rope_weight.shape[1]
    couples = n_sp // 2
    spare = max(couples - 1, 1)
    count, slots = 11, 3
    return pl.pallas_call(
        functools.partial(fused_kernel, sizes),
        out_shape=[jax.ShapeDtypeStruct((rows, ho.shape[1] * n_fs), bf16)] * 2,
        in_specs=[hbm] * 21,
        out_specs=[hbm] * 2,
        scratch_shapes=[scratch(*a.shape, dtype=a.dtype) for a in small] + [
            scratch(*whole(qd), dtype=bf16), scratch(*whole(md), dtype=bf16),
            scratch(*whole(ku, 0, 2), dtype=bf16), scratch(*whole(vu, 0, 2), dtype=bf16),
            scratch(*whole(qu, 0, 2), dtype=bf16), scratch(*whole(cv, 0, 2), dtype=bf16),
            scratch(*whole(cg, 0, 2), dtype=bf16), scratch(*whole(ho, 1), dtype=bf16),
            scratch(*whole(co, 1), dtype=bf16),
            scratch(2, rows, model, dtype=bf16), scratch(2, rows, model, dtype=bf16),
            scratch(n_tp, 2, rows, qd.shape[1], dtype=bf16),
            scratch(n_tp, 2, rows, md.shape[1], dtype=bf16),
            scratch(n_sp, lat, rows, dtype=bf16), scratch(n_sp, rope, rows, dtype=bf16),
            scratch(qu.shape[0] * n_fs, 2 * rows, dtype=bf16), scratch(qu.shape[1] // 2, 2 * rows),
            scratch(n_sp, ku.shape[1] // 2, rows),
            scratch(n_sp, vu.shape[1] // 2, rows, dtype=bf16),
            scratch(n_sp, rope, rows), scratch(n_sp, 1, rows),
            scratch(QK_DIM, 2 * rows), scratch(QK_DIM, rows),
            scratch(n_sp, rows, 2 * rows), scratch(n_sp, rows, 2 * rows),
            scratch(vu.shape[1] // 2, 2 * rows), scratch(vu.shape[1] // 2, rows, dtype=bf16),
            scratch(vu.shape[1], rows, dtype=bf16), scratch(rows, channels, dtype=bf16),
            scratch(2, rows, channels // 2),
            scratch(rows, ho.shape[1] * n_fs),
            scratch(rows + RIM, channels // 2, dtype=bf16),
            scratch(rows + RIM, channels // 2, dtype=bf16),
            scratch(rows + RIM, channels), scratch(RIM, channels // 2, dtype=bf16),
            scratch(2, RIM, channels // 2, dtype=bf16), scratch(rows, channels),
            scratch(2 * rows, 128), scratch(2 * rows, 128),
            scratch(rows, ho.shape[1] * n_fs, dtype=bf16),
            dma((slots, 2)), dma((count, 2)), dma((slots, 2)), dma((count, 2)),
            dma((slots, 3)), dma((slots, 3)), dma((slots,)), dma((slots,)), dma((3,)),
            dma((5,)), dma((8,)), dma((spare, 2, 2)), dma((spare, 2)),
            dma((couples,)), dma((couples,)), dma((3,)), dma((3,)), dma((n_fs,)), dma((n_fs,)), dma((n_fs,)),
        ],
        compiler_params=pltpu.CompilerParams(
            collective_id=1, has_side_effects=True, vmem_limit_bytes=60 * 1024 * 1024
        ),
    )(x, *small, qd, md, ku, vu, qu, cv, cg, ho, co)


def fused_local(
    tokens, mix_gain, query_down, memory_down, rope_weight, query_up, key_up, value_up,
    latent_gain, memory_gain, query_gain, key_gain, conv_value, conv_gate, conv_kernel,
    channel_gain, channel_shift, heads_out, conv_out,
):
    mine, other = fused_call(
        (lax.axis_size("fs"), lax.axis_size("sp"), lax.axis_size("tp")),
        tokens[0], mix_gain, rope_weight, conv_kernel, channel_gain, channel_shift,
        latent_gain, memory_gain, query_gain, key_gain,
        query_down, memory_down, conv_value, conv_gate,
        query_up, key_up, value_up, heads_out, conv_out,
    )
    return join(mine, other)[None]


def solution(mesh):
    in_specs = (
        P("fs", "sp", None),
        P(),
        P("fs", "tp"),
        P("fs", "tp"),
        P(),
        P("fs", "tp"),
        P("fs", "tp"),
        P("fs", "tp"),
        P(),
        P(),
        P(),
        P(),
        P("fs", "tp"),
        P("fs", "tp"),
        P(None, "tp"),
        P("tp"),
        P("tp"),
        P("tp", "fs"),
        P("tp", "fs"),
    )
    out_specs = P("fs", "sp", None)
    n_fs, n_sp, n_tp = (mesh.shape[axis] for axis in ("fs", "sp", "tp"))
    fits = n_fs == 4 and n_tp == 2 and n_sp in (2, 4)
    body = fused_local if fits else local
    return jax.shard_map(body, mesh=mesh, in_specs=in_specs, out_specs=out_specs, check_vma=False)
```

```python
import functools

import jax
import jax.numpy as jnp
import numpy as np
from jax import lax
from jax.experimental import pallas as pl
from jax.experimental.pallas import tpu as pltpu
from jax.sharding import PartitionSpec as P

MESH_ID = pl.DeviceIdType.MESH

QK_NOPE = 64
QK_ROPE = 32
V_DIM = 64
CONV_W = 1024
SEG = 64
QK_DIM = 96


epsilon = 1e-06
rope_base = 10000.0
masked_score = -1e30


def norm_rows(matrix, scale_vector):
    return (
        matrix
        * lax.rsqrt(jnp.mean(matrix * matrix, axis=-1, keepdims=True) + epsilon)
        * scale_vector
    )


def rope_tables(positions):
    inverse_freq = 1.0 / rope_base ** (jnp.arange(0, QK_ROPE, 2, dtype=jnp.float32) / QK_ROPE)
    angles = positions.astype(jnp.float32)[:, None] * inverse_freq[None, :]
    return (jnp.cos(angles)[:, None, :], jnp.sin(angles)[:, None, :])


def rotate(matrix, cosine_table, sine_table):
    half_width = matrix.shape[-1] // 2
    front_half = matrix[..., :half_width]
    back_half = matrix[..., half_width:]
    return jnp.concatenate(
        [
            front_half * cosine_table - back_half * sine_table,
            front_half * sine_table + back_half * cosine_table,
        ],
        axis=-1,
    )


def heads_query(latent, weight, scale_vector, cosine_table, sine_table):
    row_count = latent.shape[0]
    projected = jnp.dot(latent, weight, preferred_element_type=jnp.float32)
    projected = norm_rows(
        projected.reshape(row_count, weight.shape[1] // QK_DIM, QK_DIM), scale_vector
    )
    turned = rotate(projected[..., QK_NOPE:], cosine_table, sine_table)
    return jnp.concatenate([projected[..., :QK_NOPE], turned], axis=-1).astype(jnp.bfloat16)


def heads_key(latent, rope_rows, weight, scale_vector, cosine_table, sine_table):
    row_count = latent.shape[0]
    head_count = weight.shape[1] // QK_NOPE
    nope_part = jnp.dot(latent, weight, preferred_element_type=jnp.float32).reshape(
        row_count, head_count, QK_NOPE
    )
    shared = jnp.broadcast_to(
        rope_rows.astype(jnp.float32)[:, None, :], (row_count, head_count, QK_ROPE)
    )
    joined = norm_rows(jnp.concatenate([nope_part, shared], axis=-1), scale_vector)
    turned = rotate(joined[..., QK_NOPE:], cosine_table, sine_table)
    return jnp.concatenate([joined[..., :QK_NOPE], turned], axis=-1).astype(jnp.bfloat16)


RIM = 32


def relayed_rows(rows, paired):
    return (rows * 5 // 16) // 16 * 16 if paired else 0


def gather_kernel(
    sizes,
    x_ref, gain_ref, rope_ref, taps_ref, cgain_ref, cshift_ref,
    qd, md, cv, cg, qu, ku, vu, ho, co,
    lq_all, lm_all, rr_all, conv_ref, qu_all, ku_all, vu_all, ho_all, co_all,
    qd_all, md_all, cv_all, cg_all, normed, acc_q, acc_m, acc_v, acc_g, ext, tail, rim,
    sums, stats, stats_all,
    send_d, recv_d, send_r, recv_r, send_z, recv_z, local_sem, rim_sem,
    sp_send, sp_recv, rr_send, rr_recv, tp_send, tp_recv,
):
    n_fs, n_sp, n_tp = sizes
    paired = n_sp % 2 == 0
    f = lax.axis_index("fs")
    s = lax.axis_index("sp")
    t = lax.axis_index("tp")
    parity = lax.rem(s, 2)
    partner = s + 1 - 2 * parity

    barrier = pltpu.get_barrier_semaphore()
    for axis, at, count in (("fs", f, n_fs), ("sp", s, n_sp), ("tp", t, n_tp)):
        for k in range(1, count):
            pl.semaphore_signal(
                barrier, inc=1, device_id={axis: lax.rem(at + k, count)}, device_id_type=MESH_ID
            )
    pl.semaphore_wait(barrier, n_fs + n_sp + n_tp - 3)

    jobs = [
        (qd, qd_all, 0), (md, md_all, 0), (cv, cv_all, 0), (cg, cg_all, 0),
        (qu, qu_all, 0), (ku, ku_all, 0), (vu, vu_all, 0), (ho, ho_all, 1), (co, co_all, 1),
    ]
    last = len(jobs) - 1
    ahead = 4

    def place(whole, shard, dim, owner, start, count):
        rows, cols = shard.shape
        if dim == 0:
            return whole.at[pl.ds(pl.multiple_of(owner * rows + start, 16), count), :]
        return whole.at[
            pl.ds(pl.multiple_of(start, 16), count),
            pl.ds(pl.multiple_of(owner * cols, 128), cols),
        ]

    square = n_fs == 4
    if square:
        near_x = f + 1 - 2 * lax.rem(f, 2)
        near_y = lax.rem(f + 2, 4)
        far = lax.rem(near_x + 2, 4)
        targets = sources = [near_x, near_y]
    else:
        targets = [lax.rem(f + k, n_fs) for k in range(1, n_fs)]
        sources = [lax.rem(f + n_fs - k, n_fs) for k in range(1, n_fs)]

    direct, far_copies, over_sp, own = [], [], [], []
    for a, (shard, whole, dim) in enumerate(jobs):
        rows = shard.shape[0]
        less = 0 if a == last else relayed_rows(rows, paired)
        start = parity * less
        count = rows - less
        direct.append([
            pltpu.make_async_remote_copy(
                src_ref=shard.at[pl.ds(pl.multiple_of(start, 16), count), :],
                dst_ref=place(whole, shard, dim, f, start, count),
                send_sem=send_d.at[a, k], recv_sem=recv_d.at[a, k],
                device_id={"fs": target}, device_id_type=MESH_ID,
            )
            for k, target in enumerate(targets)
        ])
        halves = []
        if square:
            half = (count // 2 + 15) // 16 * 16
            for k, (owner, target, begin, size) in enumerate((
                (near_y, near_x, start, half), (near_x, near_y, start + half, count - half)
            )):
                piece = place(whole, shard, dim, owner, begin, size)
                halves.append(pltpu.make_async_remote_copy(
                    src_ref=piece, dst_ref=piece,
                    send_sem=send_r.at[a, k], recv_sem=recv_r.at[a, k],
                    device_id={"fs": target}, device_id_type=MESH_ID,
                ))
        far_copies.append(halves)
        across = []
        if less:
            lack = parity * (rows - less)
            for k, owner in enumerate(sources + ([far] if square else [])):
                piece = place(whole, shard, dim, owner, lack, less)
                across.append(pltpu.make_async_remote_copy(
                    src_ref=piece, dst_ref=piece,
                    send_sem=send_z.at[a, k], recv_sem=recv_z.at[a, k],
                    device_id={"sp": partner}, device_id_type=MESH_ID,
                ))
        over_sp.append(across)
        own.append(pltpu.make_async_copy(
            shard, place(whole, shard, dim, f, 0, rows), local_sem.at[a]
        ))

    def begin_array(a):
        if a <= last:
            for copy in direct[a]:
                copy.start()

    def finish_far(a):
        for copy in far_copies[a]:
            copy.wait_recv()
        for copy in over_sp[a][len(sources):]:
            copy.start()

    def tick(a):
        for copy in direct[a]:
            copy.wait_recv()
        for copy in far_copies[a]:
            copy.start()
        begin_array(a + ahead)
        for copy in over_sp[a][: len(sources)]:
            copy.start()
        if a >= 1:
            finish_far(a - 1)

    def complete(a):
        own[a].wait()
        for copy in over_sp[a]:
            copy.wait_recv()

    for a in range(ahead):
        begin_array(a)
    for copy in own:
        copy.start()

    rows = x_ref.shape[0]
    part = 32

    @pl.loop(0, rows // part)
    def _(i):
        at = pl.ds(pl.multiple_of(i * part, part), part)
        x = x_ref[at, :].astype(jnp.float32)
        scale = lax.rsqrt(jnp.mean(x * x, axis=-1, keepdims=True) + epsilon)
        normed[at, :] = (x * scale * gain_ref[...]).astype(jnp.bfloat16)

    depth = qd.shape[0]

    def project(weight, acc):
        acc[...] = jnp.zeros_like(acc)

        @pl.loop(0, n_fs)
        def _(i):
            at = pl.ds(pl.multiple_of(i * depth, depth), depth)
            acc[...] += jnp.dot(
                normed[:, at], weight[at, :], preferred_element_type=jnp.float32
            )

    mine = pl.ds(pl.multiple_of(s * rows, 16), rows)
    rr_all[mine, :] = jnp.dot(
        normed[...], rope_ref[...], preferred_element_type=jnp.float32
    ).astype(jnp.bfloat16)
    tick(0)
    tick(1)
    tick(2)
    complete(0)
    project(qd_all, acc_q)
    lq_all[t, :, :] = acc_q[...].astype(jnp.bfloat16)
    tick(3)
    complete(1)
    project(md_all, acc_m)
    lm_all[t, mine, :] = acc_m[...].astype(jnp.bfloat16)
    tick(4)
    complete(2)
    project(cv_all, acc_v)

    exchanges, passes = [], []
    for k in range(1, n_sp):
        peer = {"sp": lax.rem(s + k, n_sp)}
        exchanges.append(pltpu.make_async_remote_copy(
            src_ref=lm_all.at[t, mine, :], dst_ref=lm_all.at[t, mine, :],
            send_sem=sp_send.at[k - 1], recv_sem=sp_recv.at[k - 1],
            device_id=peer, device_id_type=MESH_ID,
        ))
        exchanges.append(pltpu.make_async_remote_copy(
            src_ref=rr_all.at[mine, :], dst_ref=rr_all.at[mine, :],
            send_sem=rr_send.at[k - 1], recv_sem=rr_recv.at[k - 1],
            device_id=peer, device_id_type=MESH_ID,
        ))
    tp_peers = [{"tp": lax.rem(t + k, n_tp)} for k in range(1, n_tp)]

    def to_tp(kind, source, landing):
        return [
            pltpu.make_async_remote_copy(
                src_ref=source, dst_ref=landing(k),
                send_sem=tp_send.at[kind, k], recv_sem=tp_recv.at[kind, k],
                device_id=peer, device_id_type=MESH_ID,
            )
            for k, peer in enumerate(tp_peers)
        ]

    query_copies = to_tp(0, lq_all.at[t], lambda k: lq_all.at[t])
    memory_copies = to_tp(1, lm_all.at[t], lambda k: lm_all.at[t])
    stat_copies = to_tp(2, stats, lambda k: stats_all.at[k])
    for copy in exchanges + query_copies:
        copy.start()
    tick(5)
    complete(3)
    project(cg_all, acc_g)

    @pl.loop(0, rows // part)
    def _(i):
        at = pl.ds(pl.multiple_of(i * part, part), part)
        gated = (acc_v[at, :] * jax.nn.sigmoid(acc_g[at, :])).astype(jnp.bfloat16)
        ext[pl.ds(pl.multiple_of(RIM + i * part, part), part), :] = gated.astype(jnp.float32)

    tail[...] = ext[pl.ds(rows, RIM), :].astype(jnp.bfloat16)
    rim_copy = pltpu.make_async_remote_copy(
        src_ref=tail, dst_ref=rim, send_sem=rim_sem.at[0], recv_sem=rim_sem.at[1],
        device_id={"sp": lax.rem(s + 1, n_sp)}, device_id_type=MESH_ID,
    )
    tick(6)

    @pl.when(s < n_sp - 1)
    def _():
        rim_copy.start()

    for copy in exchanges:
        copy.wait_recv()
    for copy in memory_copies:
        copy.start()

    @pl.when(s > 0)
    def _():
        rim_copy.wait_recv()
        ext[pl.ds(0, RIM), :] = rim[...].astype(jnp.float32)

    @pl.when(s == 0)
    def _():
        ext[pl.ds(0, RIM), :] = jnp.zeros((RIM, ext.shape[1]), jnp.float32)

    tap_count = taps_ref.shape[0]
    block = 64

    def convolve(c):
        cols = pl.ds(pl.multiple_of(c * 128, 128), 128)
        taps = taps_ref[:, cols].astype(jnp.float32)
        for r in range(0, rows, block):
            total = jnp.zeros((block, 128), jnp.float32)
            for j in range(tap_count):
                total = total + ext[
                    pl.ds(r + RIM - (tap_count - 1) + j, block), cols
                ] * taps[j : j + 1, :]
            sums[pl.ds(r, block), cols] = total

    tiles = ext.shape[1] // 128
    pl.loop(0, tiles // 2)(convolve)
    tick(7)
    pl.loop(tiles // 2, tiles)(convolve)

    @pl.loop(0, rows // part)
    def _(i):
        begin = pl.multiple_of(i * part, part)
        values = sums[pl.ds(begin, part), :]
        stats[pl.ds(begin, part), :] = jnp.broadcast_to(
            jnp.sum(values, axis=1, keepdims=True), (part, 128)
        )
        stats[pl.ds(pl.multiple_of(rows + begin, part), part), :] = jnp.broadcast_to(
            jnp.sum(values * values, axis=1, keepdims=True), (part, 128)
        )

    tick(8)
    for copy in stat_copies:
        copy.start()
    for copy in stat_copies:
        copy.wait_recv()

    channels = ext.shape[1] * n_tp

    @pl.loop(0, rows // part)
    def _(i):
        begin = pl.multiple_of(i * part, part)
        upper = pl.ds(begin, part)
        lower = pl.ds(pl.multiple_of(rows + begin, part), part)
        total, squares = stats[upper, :], stats[lower, :]
        for k in range(n_tp - 1):
            total = total + stats_all[k, upper, :]
            squares = squares + stats_all[k, lower, :]
        mean = total[:, :1] / channels
        spread = squares[:, :1] / channels - mean * mean
        shaped = (sums[upper, :] - mean) * lax.rsqrt(spread + epsilon)
        conv_ref[upper, :] = jax.nn.silu(
            shaped * cgain_ref[...] + cshift_ref[...]
        ).astype(jnp.bfloat16)

    finish_far(last)
    for a in range(4, last + 1):
        complete(a)
    for copy in query_copies + memory_copies:
        copy.wait_recv()
    for group in direct + far_copies + over_sp:
        for copy in group:
            copy.wait_send()
    for copy in exchanges + query_copies + memory_copies + stat_copies:
        copy.wait_send()

    @pl.when(s < n_sp - 1)
    def _():
        rim_copy.wait_send()


def gather_and_project(
    sizes, x, mix_gain, rope_weight, taps, channel_gain, channel_shift,
    qd, md, cv, cg, qu, ku, vu, ho, co,
):
    n_fs, n_sp, n_tp = sizes
    rows = x.shape[0]
    bf16, f32 = jnp.bfloat16, jnp.float32
    vmem = pl.BlockSpec(memory_space=pltpu.VMEM)
    hbm = pl.BlockSpec(memory_space=pl.ANY)

    def whole(w, dim=0):
        return (w.shape[0] * n_fs, w.shape[1]) if dim == 0 else (w.shape[0], w.shape[1] * n_fs)

    out_shapes = [
        ((n_tp, rows, qd.shape[1]), bf16), ((n_tp, n_sp * rows, md.shape[1]), bf16),
        ((n_sp * rows, rope_weight.shape[1]), bf16), ((rows, cv.shape[1]), bf16),
        (whole(qu), bf16), (whole(ku), bf16), (whole(vu), bf16),
        (whole(ho, 1), bf16), (whole(co, 1), bf16),
    ]
    dma = pltpu.SemaphoreType.DMA
    tp_others = max(n_tp - 1, 1)
    sp_others = max(n_sp - 1, 1)
    return pl.pallas_call(
        functools.partial(gather_kernel, sizes),
        out_shape=[jax.ShapeDtypeStruct(*o) for o in out_shapes],
        in_specs=[vmem] * 6 + [hbm] * 9,
        out_specs=[vmem] * 9,
        scratch_shapes=[
            pltpu.VMEM(whole(qd), bf16), pltpu.VMEM(whole(md), bf16),
            pltpu.VMEM(whole(cv), bf16), pltpu.VMEM(whole(cg), bf16),
            pltpu.VMEM(x.shape, bf16), pltpu.VMEM((rows, qd.shape[1]), f32),
            pltpu.VMEM((rows, md.shape[1]), f32),
            pltpu.VMEM((rows, cv.shape[1]), f32), pltpu.VMEM((rows, cv.shape[1]), f32),
            pltpu.VMEM((rows + RIM, cv.shape[1]), f32),
            pltpu.VMEM((RIM, cv.shape[1]), bf16), pltpu.VMEM((RIM, cv.shape[1]), bf16),
            pltpu.VMEM((rows, cv.shape[1]), f32), pltpu.VMEM((2 * rows, 128), f32),
            pltpu.VMEM((tp_others, 2 * rows, 128), f32),
            dma((9, n_fs - 1)), dma((9, n_fs - 1)), dma((9, 2)), dma((9, 2)),
            dma((9, n_fs - 1)), dma((9, n_fs - 1)), dma((9,)), dma((2,)),
            dma((sp_others,)), dma((sp_others,)), dma((sp_others,)), dma((sp_others,)),
            dma((3, tp_others)), dma((3, tp_others)),
        ],
        compiler_params=pltpu.CompilerParams(
            collective_id=0, has_side_effects=True, vmem_limit_bytes=56 * 1024 * 1024
        ),
    )(
        x, mix_gain[None, :], rope_weight, taps, channel_gain[None, :], channel_shift[None, :],
        qd, md, cv, cg, qu, ku, vu, ho, co,
    )


def key_block(key_count):
    block_size = key_count
    while block_size > 2048 and block_size % 2 == 0:
        block_size = block_size // 2
    return block_size


def sum_groups(partial):
    count = lax.axis_size("tp")
    if count != 2:
        return lax.psum(partial, "tp")
    other = lax.ppermute(partial, "tp", [(0, 1), (1, 0)])
    return (partial.astype(jnp.float32) + other.astype(jnp.float32)).astype(jnp.bfloat16)


def local(
    tokens,
    mix_gain,
    query_down,
    memory_down,
    rope_weight,
    query_up,
    key_up,
    value_up,
    latent_gain,
    memory_gain,
    query_gain,
    key_gain,
    conv_value,
    conv_gate,
    conv_kernel,
    channel_gain,
    channel_shift,
    heads_out,
    conv_out,
):
    own_rows = tokens[0]
    (
        query_parts, memory_parts, rope_piece, conv_result,
        up_query, up_keys, up_values, out_heads, out_conv,
    ) = gather_and_project(
        (lax.axis_size("fs"), lax.axis_size("sp"), lax.axis_size("tp")),
        own_rows, mix_gain, rope_weight, conv_kernel, channel_gain, channel_shift,
        query_down, memory_down, conv_value, conv_gate,
        query_up, key_up, value_up, heads_out, conv_out,
    )
    row_count = own_rows.shape[0]
    whole_query = jnp.concatenate(list(query_parts), axis=1)
    whole_memory = jnp.concatenate(list(memory_parts), axis=1)
    query_normed = norm_rows(whole_query.astype(jnp.float32), latent_gain).astype(jnp.bfloat16)
    memory_piece = norm_rows(whole_memory.astype(jnp.float32), memory_gain).astype(jnp.bfloat16)
    positions = lax.axis_index("sp") * row_count + jnp.arange(row_count, dtype=jnp.int32)
    cosine_table, sine_table = rope_tables(positions)
    queries = heads_query(query_normed, up_query, query_gain, cosine_table, sine_table)
    head_count = queries.shape[1]
    query_segment = positions // SEG
    score_scale = QK_DIM ** (-0.5)
    def attend(state_carry, key_rows, value_rows, key_pos):
        running_max, row_total, weighted = state_carry
        scores = (
            jnp.einsum("qhd,khd->qhk", queries, key_rows, preferred_element_type=jnp.float32)
            * score_scale
        )
        allowed = ((key_pos // SEG)[None, :] <= query_segment[:, None])[:, None, :]
        scores = jnp.where(allowed, scores, masked_score)
        new_max = jnp.maximum(running_max, jnp.max(scores, axis=2))
        weights = jnp.where(allowed, jnp.exp(scores - new_max[:, :, None]), 0.0)
        factor = jnp.exp(running_max - new_max)
        row_total = row_total * factor + jnp.sum(weights, axis=2)
        weighted = weighted * factor[:, :, None] + jnp.einsum(
            "qhk,khd->qhd",
            weights.astype(jnp.bfloat16),
            value_rows,
            preferred_element_type=jnp.float32,
        )
        return (new_max, row_total, weighted)

    initial = (
        jnp.full((row_count, head_count), masked_score, jnp.float32),
        jnp.zeros((row_count, head_count), jnp.float32),
        jnp.zeros((row_count, head_count, V_DIM), jnp.float32),
    )
    def block_keys(block_start, block_size):
        memory_block = lax.dynamic_slice_in_dim(memory_piece, block_start, block_size, 0)
        rope_block = lax.dynamic_slice_in_dim(rope_piece, block_start, block_size, 0)
        key_pos = block_start + jnp.arange(block_size, dtype=jnp.int32)
        cosine_keys, sine_keys = rope_tables(key_pos)
        key_rows = heads_key(memory_block, rope_block, up_keys, key_gain, cosine_keys, sine_keys)
        value_rows = (
            jnp.dot(memory_block, up_values, preferred_element_type=jnp.float32)
            .astype(jnp.bfloat16)
            .reshape(block_size, head_count, V_DIM)
        )
        return (key_rows, value_rows, key_pos)

    key_count = memory_piece.shape[0]
    block_size = key_block(key_count)

    def step(block_index, running):
        key_rows, value_rows, key_pos = block_keys(block_index * block_size, block_size)
        return attend(running, key_rows, value_rows, key_pos)

    final_state = lax.fori_loop(0, key_count // block_size, step, initial)
    running_max, row_total, weighted = final_state
    attention = (
        (weighted / row_total[:, :, None])
        .astype(jnp.bfloat16)
        .reshape(row_count, head_count * V_DIM)
    )
    mixer_rows = jnp.concatenate([attention, conv_result], axis=1)
    out_weight = jnp.concatenate([out_heads, out_conv], axis=0)
    partial_sum = jnp.dot(mixer_rows, out_weight, preferred_element_type=jnp.float32)
    mixed = sum_groups(partial_sum.astype(jnp.bfloat16))
    return mixed[None]


def table_rows(count):
    inverse_freq = 1.0 / np.float32(rope_base) ** (
        np.arange(0, QK_ROPE, 2, dtype=np.float32) / np.float32(QK_ROPE)
    )
    angles = inverse_freq[:, None] * np.arange(count, dtype=np.float32)[None, :]
    angles = angles.astype(np.float64)
    return np.cos(angles).astype(np.float32), np.sin(angles).astype(np.float32)


def dot_heads(left, right):
    return lax.dot_general(
        left, right, (((0,), (0,)), ((), ())), preferred_element_type=jnp.float32
    )


def swapped_rows(count, part):
    return (count * part // 16) // 16 * 16


def fused_kernel(
    sizes,
    x_hbm, gain_hbm, rope_hbm, taps_hbm, cgain_hbm, cshift_hbm,
    lgain_hbm, mgain_hbm, qgain_hbm, kgain_hbm, cos_hbm, sin_hbm,
    qd, md, ku, vu, qu, cv, cg, ho, co,
    mine_hbm, other_hbm,
    gain_ref, rope_ref, taps_ref, cgain_ref, cshift_ref,
    lgain_ref, mgain_ref, qgain_ref, kgain_ref, cos_ref, sin_ref,
    qd_all, md_all, ku_all, vu_all, qu_all, cv_all, cg_all, ho_all, co_all,
    x_all, normed, lq_all, lm_all, mem_all, rr_all, qn_t, q_t, k_t, v_t,
    turned, ropesq, qcol, kcol, bias, scores,
    att_t, att_out, att_all, conv_s, acc_v, acc_out, gate_out, gate_in, ext, rim_out, rim, sums, stats, stats_all,
    mine_ref,
    send_d, recv_d, send_r, recv_r, send_z, recv_z, local_sem, small_sem, rim_sem, x_sem,
    part_sem, sp_send, sp_recv, fw_send, fw_recv, tp_send, tp_recv, out_send, out_recv, store_sem, known,
):
    n_fs, n_sp, n_tp = sizes
    f = lax.axis_index("fs")
    s = lax.axis_index("sp")
    t = lax.axis_index("tp")
    parity = lax.rem(s, 2)
    couple = lax.div(s, 2)
    couples = n_sp // 2
    partner = {"sp": s + 1 - 2 * parity}
    twin = {"tp": 1 - t}
    even, odd = parity == 0, parity == 1

    near_x = f + 1 - 2 * lax.rem(f, 2)
    near_y = lax.rem(f + 2, 4)
    far = lax.rem(near_x + 2, 4)
    sources = [near_x, near_y]
    has_below, has_above = s > 0, s < n_sp - 1

    barrier = pltpu.get_barrier_semaphore()

    def greet(device):
        pl.semaphore_signal(barrier, inc=1, device_id=device, device_id_type=MESH_ID)

    for device in (twin, {"fs": near_x}, {"fs": near_y}):
        greet(device)
    pl.when(has_below)(lambda: greet({"sp": s - 1}))
    pl.when(has_above)(lambda: greet({"sp": s + 1}))

    slots = 3
    rows = x_hbm.shape[0]
    x_own = pltpu.make_async_copy(x_hbm, x_all.at[parity], x_sem.at[0])
    x_own.start()
    small = [
        pltpu.make_async_copy(source, landing, small_sem.at[i % slots])
        for i, (source, landing) in enumerate((
            (gain_hbm, gain_ref), (rope_hbm, rope_ref), (taps_hbm, taps_ref),
            (cgain_hbm, cgain_ref), (cshift_hbm, cshift_ref), (lgain_hbm, lgain_ref),
            (mgain_hbm, mgain_ref), (qgain_hbm, qgain_ref), (kgain_hbm, kgain_ref),
            (cos_hbm, cos_ref), (sin_hbm, sin_ref),
        ))
    ]
    for copy in small[:slots]:
        copy.start()

    def remote(source, landing, send, recv, device):
        return pltpu.make_async_remote_copy(
            src_ref=source, dst_ref=landing, send_sem=send, recv_sem=recv,
            device_id=device, device_id_type=MESH_ID,
        )

    share = rows // n_tp
    slab = pl.ds(pl.multiple_of(t * share, 16), share)
    x_send = remote(
        x_hbm.at[slab, :], x_all.at[parity, slab, :], x_sem.at[1], x_sem.at[2], partner
    )
    theirs = x_all.at[1 - parity, slab, :]
    x_forward = remote(theirs, theirs, x_sem.at[3], x_sem.at[4], twin)

    def job(a, shard, whole, swap=None, dim=0, first=0, count=None):
        depth, cols = shard.shape
        count = depth if count is None else count
        lane, mine, lacking, giving = swap or (0, 0, 0, 0)
        lack, give = swapped_rows(count, lacking), swapped_rows(count, giving)
        kept = count - lack

        def place(owner, start, size):
            if dim == 0:
                return whole.at[pl.ds(pl.multiple_of(owner * depth + start, 16), size), :]
            return whole.at[
                pl.ds(pl.multiple_of(start, 16), size),
                pl.ds(pl.multiple_of(owner * cols, 128), cols),
            ]

        start = first + mine * lack
        direct = [
            remote(
                shard.at[pl.ds(start, kept), :], place(f, start, kept),
                send_d.at[a % slots, k], recv_d.at[a, k], {"fs": target},
            )
            for k, target in enumerate(sources)
        ]
        half = (kept // 2 + 15) // 16 * 16
        relays = []
        for k, (owner, target, begin, size) in enumerate((
            (near_y, near_x, start, half), (near_x, near_y, start + half, kept - half)
        )):
            piece = place(owner, begin, size)
            relays.append(remote(
                piece, piece, send_r.at[a % slots, k], recv_r.at[a, k], {"fs": target}
            ))
        gives, lacks = [], []
        if swap:
            for k, owner in enumerate(sources + [far]):
                sems = (send_z.at[lane, k], recv_z.at[lane, k], partner)
                if give:
                    piece = place(owner, first + mine * (count - give), give)
                    gives.append(remote(piece, piece, *sems))
                if lack:
                    piece = place(owner, first + (1 - mine) * kept, lack)
                    lacks.append(remote(piece, piece, *sems))
        own = pltpu.make_async_copy(
            shard.at[pl.ds(first, count), :], place(f, first, count), local_sem.at[a % slots]
        )
        return direct, relays, gives, own, lacks

    def half_columns(shard):
        width = shard.shape[1] // 2
        return shard.at[:, pl.ds(pl.multiple_of(parity * width, 128), width)]

    wide = cv.shape[1] // 2
    side = pl.ds(pl.multiple_of(parity * wide, 128), wide)
    half_rows = ho.shape[0] // 2
    last_rows = half_rows // 4
    first_rows = half_rows * 10 // 8

    def swapping(lane, even_lacks, odd_lacks, *rest):
        shard, whole, *rest = rest
        return [
            (even, shard, whole, (lane, 0, even_lacks, odd_lacks), *rest),
            (odd, shard, whole, (lane, 1, odd_lacks, even_lacks), *rest),
        ]

    plan = [
        [(even, qd, qd_all), (odd, md, md_all)],
        [(None, half_columns(ku), ku_all)], [(None, half_columns(vu), vu_all)],
        [(None, half_columns(qu), qu_all)],
        swapping(0, 8, 8, ho, ho_all, 1, 0, first_rows),
        [(None, half_columns(cv), cv_all)], [(None, half_columns(cg), cg_all)],
        swapping(1, 8, 8, ho, ho_all, 1, first_rows, 2 * half_rows - first_rows),
        swapping(2, 5, 4, co, co_all, 1, 0, half_rows),
        [(None, co, co_all, None, 1, half_rows, half_rows - last_rows)],
        [(None, co, co_all, None, 1, 2 * half_rows - last_rows, last_rows)],
    ]
    jobs = [[(who[0], job(a, *who[1:])) for who in group] for a, group in enumerate(plan)]
    last = len(jobs) - 1
    lanes = [a for a, group in enumerate(plan) if len(group[0]) > 3 and group[0][3]]

    def each(a, action):
        for condition, parts in jobs[a]:
            if condition is None:
                action(parts)
            else:
                pl.when(condition)(functools.partial(action, parts))

    def sent(a, kind):
        def go(parts):
            for copy in parts[kind]:
                copy.wait_send()

        if a >= 0:
            each(a, go)

    def begin_array(a):
        def start(parts):
            for copy in parts[0]:
                copy.start()
            parts[3].start()

        if a <= last:
            sent(a - slots, 0)
            each(a, start)

    def finish_far(a):
        def go(parts):
            with jax.named_scope(f"far_{a}"):
                for copy in parts[1]:
                    copy.wait_recv()
            for copy in parts[2][len(sources):]:
                copy.start()

        each(a, go)

    def swap_near(a):
        def swap(parts):
            for copy in parts[2][: len(sources)]:
                copy.start()

        if a in lanes:
            each(a, swap)

    begins = {0: [3], 1: [4], 2: [5], 3: [6], 5: [7], 6: [8], 7: [9], 8: [10]}

    def tick(a):
        def go(parts):
            with jax.named_scope(f"direct_{a}"):
                for copy in parts[0]:
                    copy.wait_recv()
                parts[3].wait()
            for copy in parts[1]:
                copy.start()

        sent(a - slots, 1)
        each(a, go)
        for later in begins.get(a, ()):
            begin_array(later)
        swap_near(a)

    def complete(a, which=slice(None)):
        def go(parts):
            with jax.named_scope(f"across_{a}"):
                for copy in parts[4][which]:
                    copy.wait_recv()

        each(a, go)

    with jax.named_scope("entry"):
        pl.semaphore_wait(
            barrier, 3 + has_below.astype(jnp.int32) + has_above.astype(jnp.int32)
        )
    x_send.start()
    for a in range(slots):
        begin_array(a)

    @pl.when(jnp.logical_and(has_below, has_above))
    def _():
        pl.semaphore_signal(
            known.at[0], inc=1, device_id={"sp": s - 1}, device_id_type=MESH_ID
        )

    with jax.named_scope("small_wait"):
        for r in range(0, len(small), slots):
            if r:
                for copy in small[r : r + slots]:
                    copy.start()
            for copy in small[r : r + slots]:
                copy.wait()
        x_own.wait()

    part = 32

    def norm_block(b):
        @pl.loop(0, rows // part)
        def _(i):
            at = pl.ds(pl.multiple_of(i * part, part), part)
            x = x_all[b, at, :].astype(jnp.float32)
            scale = lax.rsqrt(jnp.mean(x * x, axis=-1, keepdims=True) + epsilon)
            normed[b, at, :] = (x * scale * gain_ref[...]).astype(jnp.bfloat16)

        rr_all[2 * couple + b] = lax.dot_general(
            rope_ref[...], normed[b], (((1,), (1,)), ((), ())), preferred_element_type=jnp.float32
        ).astype(jnp.bfloat16)

    norm_block(parity)
    half_rope = QK_ROPE // 2

    def column(row_ref, col_ref):
        shape = (QK_DIM, QK_DIM)
        here = lax.broadcasted_iota(jnp.int32, shape, 0) == lax.broadcasted_iota(jnp.int32, shape, 1)
        spread_row = jnp.broadcast_to(row_ref[...], shape)
        picked = jnp.sum(jnp.where(here, spread_row, 0.0), axis=1, keepdims=True)
        col_ref[...] = jnp.broadcast_to(picked, col_ref.shape)

    column(qgain_ref, qcol)
    column(kgain_ref, kcol)

    @pl.loop(2 * couple + 2, n_sp)
    def _(j):
        mem_all[j] = jnp.zeros(mem_all.shape[1:], jnp.bfloat16)
        rr_all[j] = jnp.zeros(rr_all.shape[1:], jnp.bfloat16)

    @pl.loop(0, n_sp)
    def _(j):
        shape = (rows, 2 * rows)
        key_at = j * rows + lax.broadcasted_iota(jnp.int32, shape, 0)
        query_at = 2 * couple * rows + lax.broadcasted_iota(jnp.int32, shape, 1)
        bias[j] = jnp.where(
            lax.div(key_at, SEG) <= lax.div(query_at, SEG), 0.0, masked_score
        )

    tick(0)
    with jax.named_scope("x_wait"):
        x_send.wait_recv()
    x_forward.start()
    tick(1)
    with jax.named_scope("x_forward"):
        x_forward.wait_recv()
    norm_block(1 - parity)
    tick(2)
    finish_far(0)

    @pl.when(s < n_sp - 2)
    def _():
        pl.semaphore_wait(known.at[0], 1)


    def project(weight, b):
        return jnp.dot(normed[b], weight[...], preferred_element_type=jnp.float32)

    lat = md.shape[1]
    lat_q = qd.shape[1]
    held = pl.ds(pl.multiple_of(t * lat, lat), lat)
    query_across = remote(lq_all.at[t], lq_all.at[t], part_sem.at[0], part_sem.at[1], partner)
    query_copy = remote(lq_all.at[t], lq_all.at[t], tp_send.at[0], tp_recv.at[0], twin)
    memory_copy = remote(lm_all.at[t], lm_all.at[t], tp_send.at[1], tp_recv.at[1], twin)
    stat_copy = remote(stats, stats_all, tp_send.at[2], tp_recv.at[2], twin)
    gate_across = remote(gate_out, gate_in, part_sem.at[2], part_sem.at[3], partner)

    complete(0)

    @pl.when(even)
    def _():
        for b in range(2):
            lq_all[t, b] = project(qd_all, b).astype(jnp.bfloat16)
        query_across.start()
        query_copy.start()

    @pl.when(odd)
    def _():
        for b in range(2):
            lm_all[t, b] = project(md_all, b).astype(jnp.bfloat16)
        memory_copy.start()

    tick(3)

    def normed_columns(parts, width, gain_at, put):
        @pl.loop(0, rows // 128)
        def _(i):
            at = pl.ds(pl.multiple_of(i * 128, 128), 128)
            pieces = [parts(g, at).astype(jnp.float32) for g in range(n_tp)]
            total = sum(jnp.sum(p * p, axis=-1, keepdims=True) for p in pieces)
            scale = lax.rsqrt(total / (width * n_tp) + epsilon)
            for g in range(n_tp):
                shaped = (pieces[g] * scale * gain_at(g * width, width)).astype(jnp.bfloat16)
                put(g * width, width, at, shaped.astype(jnp.float32).T.astype(jnp.bfloat16))

    pair = pl.ds(2 * couple, 2)
    both = mem_all.at[pair, held, :]
    back = remote(both, both, part_sem.at[4], part_sem.at[5], partner)
    back_forward = remote(both, both, fw_send.at[couples - 1], fw_recv.at[couples - 1], twin)
    onward, forwards = [], []
    for d in range(1, couples):
        group = []
        later = lax.rem(couple + d, couples)
        for e in range(2):
            target = {"sp": 2 * later + e}
            group.append((
                remote(
                    mem_all.at[pair, held, :], mem_all.at[pair, held, :],
                    sp_send.at[d - 1, e, 0], sp_recv.at[d - 1, 0], target,
                ),
                remote(
                    rr_all.at[pair], rr_all.at[pair],
                    sp_send.at[d - 1, e, 1], sp_recv.at[d - 1, 1], target,
                ),
            ))
        onward.append(group)
        earlier = mem_all.at[pl.ds(2 * lax.rem(couple + couples - d, couples), 2), held, :]
        forwards.append(remote(earlier, earlier, fw_send.at[d - 1], fw_recv.at[d - 1], twin))

    @pl.when(odd)
    def _():
        with jax.named_scope("memory_wait"):
            memory_copy.wait_recv()
        for b in (1, 0):
            def put_memory(begin, width, at, piece, b=b):
                mem_all[2 * couple + b, begin : begin + width, at] = piece

            normed_columns(
                lambda g, at, b=b: lm_all[g, b, at, :], lat,
                lambda begin, width: mgain_ref[:, begin : begin + width], put_memory,
            )
        for d in range(1, couples):
            @pl.when(couple + d < couples)
            def _(d=d):
                for e in range(2):
                    for copy in onward[d - 1][e]:
                        copy.start()
        back.start()

    finish_far(1)
    tick(4)
    finish_far(2)

    @pl.when(even)
    def _():
        with jax.named_scope("back_wait"):
            back.wait_recv()
        back_forward.start()

    tick(5)
    finish_far(3)

    @pl.when(odd)
    def _():
        with jax.named_scope("query_across"):
            query_across.wait_recv()
        query_copy.start()


    @pl.when(even)
    def _():
        with jax.named_scope("back_forward"):
            back_forward.wait_recv()

    def expand(j):
        k_t[j] = dot_heads(ku_all[...], mem_all[j])
        v_t[j] = dot_heads(vu_all[...], mem_all[j]).astype(jnp.bfloat16)
        shared = rr_all[j].astype(jnp.float32)
        ropesq[j] = jnp.sum(shared * shared, axis=0, keepdims=True)
        shared = shared * kcol[QK_NOPE:, :]
        front, back_half = shared[:half_rope], shared[half_rope:]
        at = pl.ds(pl.multiple_of(j * rows, rows), rows)
        cosine, sine = cos_ref[:, at], sin_ref[:, at]
        turned[j] = jnp.concatenate(
            [front * cosine - back_half * sine, front * sine + back_half * cosine], axis=0
        )

    pl.loop(2 * couple, n_sp)(expand)
    for d in range(1, couples):
        @pl.when(couple >= d)
        def _(d=d):
            with jax.named_scope(f"behind_{d}"):
                for copy in onward[d - 1][0]:
                    copy.wait_recv()
            forwards[d - 1].start()
    with jax.named_scope("query_wait"):
        query_copy.wait_recv()
    for b in range(2):
        def put_query(begin, width, at, piece, b=b):
            at = pl.ds(pl.multiple_of(b * rows + at.start, 128), at.size)
            qn_t[begin : begin + width, at] = piece

        normed_columns(
            lambda g, at, b=b: lq_all[g, b, at, :], lat_q,
            lambda begin, width: jnp.concatenate(
                [lgain_ref[r : r + 1, :] for r in range(begin // 128, (begin + width) // 128)],
                axis=1,
            ),
            put_query,
        )
    for d in range(1, couples):
        @pl.when(couple >= d)
        def _(d=d):
            with jax.named_scope(f"forward_{d}"):
                forwards[d - 1].wait_recv()
    pl.loop(0, 2 * couple)(expand)
    q_t[...] = dot_heads(qu_all[...], qn_t[...])
    tick(6)
    finish_far(4)
    heads = qu.shape[1] // 2 // QK_DIM
    here = pl.ds(pl.multiple_of(2 * couple * rows, rows), 2 * rows)
    score_scale = QK_DIM ** (-0.5)

    def head(h):
        q = q_t[pl.ds(pl.multiple_of(h * QK_DIM, QK_DIM), QK_DIM), :]
        q = q * lax.rsqrt(jnp.mean(q * q, axis=0, keepdims=True) + epsilon) * qcol[...]
        front, back_half = q[QK_NOPE : QK_NOPE + half_rope], q[QK_NOPE + half_rope :]
        cosine, sine = cos_ref[:, here], sin_ref[:, here]
        q = jnp.concatenate(
            [
                q[:QK_NOPE],
                front * cosine - back_half * sine,
                front * sine + back_half * cosine,
            ],
            axis=0,
        ).astype(jnp.bfloat16)
        krow = pl.ds(pl.multiple_of(h * QK_NOPE, QK_NOPE), QK_NOPE)
        vrow = pl.ds(pl.multiple_of(h * V_DIM, V_DIM), V_DIM)
        top = jnp.full((1, 2 * rows), masked_score, jnp.float32)
        for j in range(n_sp):
            nope = k_t[j, krow, :]
            scale = lax.rsqrt(
                (jnp.sum(nope * nope, axis=0, keepdims=True) + ropesq[j]) / QK_DIM + epsilon
            )
            key = jnp.concatenate(
                [nope * scale * kcol[:QK_NOPE, :], turned[j] * scale], axis=0
            ).astype(jnp.bfloat16)
            block = dot_heads(key, q) + bias[j]
            scores[j] = block
            top = jnp.maximum(top, jnp.max(block, axis=0, keepdims=True))
        total = jnp.zeros((1, 2 * rows), jnp.float32)
        summed = jnp.zeros((V_DIM, 2 * rows), jnp.float32)
        for j in range(n_sp):
            weight = jnp.exp((scores[j] - top) * score_scale)
            total = total + jnp.sum(weight, axis=0, keepdims=True)
            summed = summed + jnp.dot(
                v_t[j, vrow, :], weight.astype(jnp.bfloat16),
                preferred_element_type=jnp.float32,
            )
        att_t[vrow, :] = summed / total

    pl.loop(0, heads // 2)(head)
    finish_far(5)
    for b in range(2):
        acc_v[b] = project(cv_all, b)
    tick(7)
    pl.loop(heads // 2, heads)(head)
    value_rows = heads * V_DIM
    own_rows = pl.ds(pl.multiple_of(parity * value_rows, value_rows), value_rows)
    their_lanes = pl.ds(pl.multiple_of((1 - parity) * rows, rows), rows)
    own_lanes = pl.ds(pl.multiple_of(parity * rows, rows), rows)
    att_across = remote(
        att_out, att_all.at[own_rows, :], part_sem.at[6], part_sem.at[7], partner
    )
    att_out[...] = att_t[:, their_lanes].astype(jnp.bfloat16)
    att_across.start()
    att_all[own_rows, :] = att_t[:, own_lanes].astype(jnp.bfloat16)
    finish_far(6)
    opposite = pl.ds(pl.multiple_of((1 - parity) * wide, 128), wide)
    body_rows, halo = pl.ds(RIM, rows), pl.ds(0, RIM)

    def gate(b):
        gates = project(cg_all, b)
        return (acc_v[b] * jax.nn.sigmoid(gates)).astype(jnp.bfloat16)

    end = slice(rows - RIM, rows)
    later_rim = remote(
        rim_out, rim.at[parity], rim_sem.at[0], rim_sem.at[1 + parity],
        {"sp": 2 * lax.rem(couple + 1, couples)},
    )
    has_later, has_earlier = couple < couples - 1, jnp.logical_and(even, couple > 0)
    lower = gate(0)

    @pl.when(even)
    def _():
        ext[body_rows, side] = lower.astype(jnp.float32)
        ext[halo, :] = jnp.zeros((RIM, ext.shape[1]), jnp.float32)
        gate_out[halo, :] = lower[end]

    @pl.when(odd)
    def _():
        gate_out[halo, :] = jnp.zeros((RIM, wide), jnp.bfloat16)
        gate_out[body_rows, :] = lower
        gate_across.start()
        ext[halo, side] = lower[end].astype(jnp.float32)

    upper = gate(1)
    rim_out[...] = upper[end]

    @pl.when(has_later)
    def _():
        later_rim.start()

    @pl.when(even)
    def _():
        gate_out[body_rows, :] = upper
        gate_across.start()

    @pl.when(odd)
    def _():
        ext[body_rows, side] = upper.astype(jnp.float32)

    tick(8)

    @pl.when(has_earlier)
    def _():
        with jax.named_scope("rim_wait"):
            for g in range(2):
                remote(
                    rim_out, rim.at[g], rim_sem.at[0], rim_sem.at[1 + g], partner
                ).wait_recv()
        for g in range(2):
            ext[halo, g * wide : (g + 1) * wide] = rim[g].astype(jnp.float32)

    tap_count = taps_ref.shape[0]
    block = 64

    lead = RIM - (tap_count - 1)

    def convolve(c):
        cols = pl.ds(pl.multiple_of(c * 128, 128), 128)
        taps = taps_ref[:, cols].astype(jnp.float32)
        for r in range(0, rows, block):
            total = jnp.zeros((block, 128), jnp.float32)
            for shift in range(8):
                height = block + (8 if shift else 0)
                partial = jnp.zeros((height, 128), jnp.float32)
                for offset in range(shift, RIM + 1, 8):
                    if offset >= lead:
                        tap = taps[offset - lead : offset - lead + 1, :]
                        partial = partial + ext[pl.ds(r + offset - shift, height), cols] * tap
                total = total + partial[shift : shift + block]
            sums[pl.ds(r, block), cols] = total

    tiles = wide // 128
    pl.loop(parity * tiles, (parity + 1) * tiles)(convolve)
    with jax.named_scope("gate_wait"):
        gate_across.wait_recv()
    ext[body_rows, opposite] = gate_in[body_rows, :].astype(jnp.float32)

    @pl.when(odd)
    def _():
        ext[halo, opposite] = gate_in[halo, :].astype(jnp.float32)

    pl.loop((1 - parity) * tiles, (2 - parity) * tiles)(convolve)
    finish_far(7)

    @pl.loop(0, rows // part)
    def _(i):
        begin = pl.multiple_of(i * part, part)
        values = sums[pl.ds(begin, part), :]
        stats[pl.ds(begin, part), :] = jnp.broadcast_to(
            jnp.sum(values, axis=1, keepdims=True), (part, 128)
        )
        stats[pl.ds(pl.multiple_of(rows + begin, part), part), :] = jnp.broadcast_to(
            jnp.sum(values * values, axis=1, keepdims=True), (part, 128)
        )

    stat_copy.start()
    tick(9)
    with jax.named_scope("att_wait"):
        att_across.wait_recv()
    att = att_all[...].astype(jnp.float32).T.astype(jnp.bfloat16)
    span = ho.shape[1]

    complete(4)

    @pl.loop(0, n_fs)
    def _(i):
        cols = pl.ds(pl.multiple_of(i * span, span), span)
        acc_out[:, cols] = jnp.dot(
            att[:, :first_rows], ho_all[:first_rows, cols], preferred_element_type=jnp.float32
        )

    finish_far(8)
    with jax.named_scope("stat_wait"):
        stat_copy.wait_recv()
    channels = ext.shape[1] * n_tp

    @pl.loop(0, rows // part)
    def _(i):
        begin = pl.multiple_of(i * part, part)
        upper = pl.ds(begin, part)
        lower = pl.ds(pl.multiple_of(rows + begin, part), part)
        total = stats[upper, :] + stats_all[upper, :]
        squares = stats[lower, :] + stats_all[lower, :]
        mean = total[:, :1] / channels
        spread = squares[:, :1] / channels - mean * mean
        shaped = (sums[upper, :] - mean) * lax.rsqrt(spread + epsilon)
        conv_s[upper, :] = jax.nn.silu(
            shaped * cgain_ref[...] + cshift_ref[...]
        ).astype(jnp.bfloat16)

    tick(10)
    outs, stores = [], []
    for i, owner in enumerate([f, near_x, near_y, far]):
        cols = pl.ds(pl.multiple_of(owner * span, span), span)
        outs.append(remote(
            mine_ref.at[:, cols], other_hbm.at[:, cols], out_send.at[i], out_recv.at[i], twin
        ))
        stores.append(pltpu.make_async_copy(
            mine_ref.at[:, cols], mine_hbm.at[:, cols], store_sem.at[i]
        ))
        if i == 1:
            complete(7, slice(0, len(sources)))
            complete(8, slice(0, len(sources)))
        if i == n_fs - 1:
            finish_far(9)
            finish_far(last)
            complete(7, slice(len(sources), None))
            complete(8, slice(len(sources), None))
        mine_ref[:, cols] = (
            acc_out[:, cols]
            + jnp.dot(att[:, first_rows:], ho_all[first_rows:, cols], preferred_element_type=jnp.float32)
            + jnp.dot(conv_s[...], co_all[:, cols], preferred_element_type=jnp.float32)
        ).astype(jnp.bfloat16)
        outs[i].start()
        stores[i].start()

    for a in range(last + 1 - slots, last + 1):
        sent(a, 0)
        sent(a, 1)
    for a in lanes:
        sent(a, 2)
    for copy in (x_send, x_forward, query_copy, stat_copy, gate_across, att_across):
        copy.wait_send()

    @pl.when(even)
    def _():
        query_across.wait_send()
        back_forward.wait_send()

    @pl.when(odd)
    def _():
        memory_copy.wait_send()
        back.wait_send()
        for d in range(1, couples):
            @pl.when(couple + d < couples)
            def _(d=d):
                for e in range(2):
                    for copy in onward[d - 1][e]:
                        copy.wait_send()

    for d in range(1, couples):
        @pl.when(couple >= d)
        def _(d=d):
            forwards[d - 1].wait_send()

    @pl.when(has_later)
    def _():
        later_rim.wait_send()

    with jax.named_scope("out_wait"):
        for copy in outs + stores:
            copy.wait()


def join_kernel(mine_hbm, other_hbm, out_hbm, mine, other, whole, loads, stores):
    rows = mine.shape[0]
    pieces = loads.shape[0]
    step = rows // pieces

    def copies(i):
        at = pl.ds(i * step, step)
        return (
            pltpu.make_async_copy(mine_hbm.at[at, :], mine.at[at, :], loads.at[i, 0]),
            pltpu.make_async_copy(other_hbm.at[at, :], other.at[at, :], loads.at[i, 1]),
            pltpu.make_async_copy(whole.at[at, :], out_hbm.at[at, :], stores.at[i]),
        )

    plan = [copies(i) for i in range(pieces)]
    for one, two, _ in plan:
        one.start()
        two.start()
    for i, (one, two, back) in enumerate(plan):
        one.wait()
        two.wait()
        at = pl.ds(i * step, step)
        whole[at, :] = (
            mine[at, :].astype(jnp.float32) + other[at, :].astype(jnp.float32)
        ).astype(jnp.bfloat16)
        back.start()
    for _, _, back in plan:
        back.wait()


def join(mine, other):
    pieces = 4
    buffer = pltpu.VMEM(mine.shape, mine.dtype)
    dma = pltpu.SemaphoreType.DMA
    hbm = pl.BlockSpec(memory_space=pl.ANY)
    return pl.pallas_call(
        join_kernel,
        out_shape=jax.ShapeDtypeStruct(mine.shape, mine.dtype),
        in_specs=[hbm] * 2,
        out_specs=hbm,
        scratch_shapes=[buffer] * 3 + [dma((pieces, 2)), dma((pieces,))],
        compiler_params=pltpu.CompilerParams(vmem_limit_bytes=60 * 1024 * 1024),
    )(mine, other)


def fused_call(
    sizes, x, mix_gain, rope_weight, taps, channel_gain, channel_shift,
    latent_gain, memory_gain, query_gain, key_gain,
    qd, md, cv, cg, qu, ku, vu, ho, co,
):
    n_fs, n_sp, n_tp = sizes
    rows, model = x.shape
    bf16, f32 = jnp.bfloat16, jnp.float32
    hbm = pl.BlockSpec(memory_space=pl.ANY)
    cosine, sine = table_rows(n_sp * rows)
    small = [
        mix_gain[None, :], rope_weight.T, taps, channel_gain[None, :], channel_shift[None, :],
        latent_gain.reshape(-1, 128), memory_gain[None, :], query_gain[None, :],
        key_gain[None, :], jnp.asarray(cosine), jnp.asarray(sine),
    ]

    def whole(w, dim=0, parts=1):
        rows_w, cols_w = w.shape[0], w.shape[1] // parts
        return (rows_w * n_fs, cols_w) if dim == 0 else (rows_w, cols_w * n_fs)

    def scratch(*shape, dtype=f32):
        return pltpu.VMEM(shape, dtype)

    dma = pltpu.SemaphoreType.DMA
    channels, lat = cv.shape[1], md.shape[1] * n_tp
    rope = rope_weight.shape[1]
    couples = n_sp // 2
    spare = max(couples - 1, 1)
    count, slots = 11, 3
    return pl.pallas_call(
        functools.partial(fused_kernel, sizes),
        out_shape=[jax.ShapeDtypeStruct((rows, ho.shape[1] * n_fs), bf16)] * 2,
        in_specs=[hbm] * 21,
        out_specs=[hbm] * 2,
        scratch_shapes=[scratch(*a.shape, dtype=a.dtype) for a in small] + [
            scratch(*whole(qd), dtype=bf16), scratch(*whole(md), dtype=bf16),
            scratch(*whole(ku, 0, 2), dtype=bf16), scratch(*whole(vu, 0, 2), dtype=bf16),
            scratch(*whole(qu, 0, 2), dtype=bf16), scratch(*whole(cv, 0, 2), dtype=bf16),
            scratch(*whole(cg, 0, 2), dtype=bf16), scratch(*whole(ho, 1), dtype=bf16),
            scratch(*whole(co, 1), dtype=bf16),
            scratch(2, rows, model, dtype=bf16), scratch(2, rows, model, dtype=bf16),
            scratch(n_tp, 2, rows, qd.shape[1], dtype=bf16),
            scratch(n_tp, 2, rows, md.shape[1], dtype=bf16),
            scratch(n_sp, lat, rows, dtype=bf16), scratch(n_sp, rope, rows, dtype=bf16),
            scratch(qu.shape[0] * n_fs, 2 * rows, dtype=bf16), scratch(qu.shape[1] // 2, 2 * rows),
            scratch(n_sp, ku.shape[1] // 2, rows),
            scratch(n_sp, vu.shape[1] // 2, rows, dtype=bf16),
            scratch(n_sp, rope, rows), scratch(n_sp, 1, rows),
            scratch(QK_DIM, 2 * rows), scratch(QK_DIM, rows),
            scratch(n_sp, rows, 2 * rows), scratch(n_sp, rows, 2 * rows),
            scratch(vu.shape[1] // 2, 2 * rows), scratch(vu.shape[1] // 2, rows, dtype=bf16),
            scratch(vu.shape[1], rows, dtype=bf16), scratch(rows, channels, dtype=bf16),
            scratch(2, rows, channels // 2),
            scratch(rows, ho.shape[1] * n_fs),
            scratch(rows + RIM, channels // 2, dtype=bf16),
            scratch(rows + RIM, channels // 2, dtype=bf16),
            scratch(rows + RIM, channels), scratch(RIM, channels // 2, dtype=bf16),
            scratch(2, RIM, channels // 2, dtype=bf16), scratch(rows, channels),
            scratch(2 * rows, 128), scratch(2 * rows, 128),
            scratch(rows, ho.shape[1] * n_fs, dtype=bf16),
            dma((slots, 2)), dma((count, 2)), dma((slots, 2)), dma((count, 2)),
            dma((slots, 3)), dma((slots, 3)), dma((slots,)), dma((slots,)), dma((3,)),
            dma((5,)), dma((8,)), dma((spare, 2, 2)), dma((spare, 2)),
            dma((couples,)), dma((couples,)), dma((3,)), dma((3,)), dma((n_fs,)), dma((n_fs,)), dma((n_fs,)),
            pltpu.SemaphoreType.REGULAR((1,)),
        ],
        compiler_params=pltpu.CompilerParams(
            collective_id=1, has_side_effects=True, vmem_limit_bytes=60 * 1024 * 1024
        ),
    )(x, *small, qd, md, ku, vu, qu, cv, cg, ho, co)


def fused_local(
    tokens, mix_gain, query_down, memory_down, rope_weight, query_up, key_up, value_up,
    latent_gain, memory_gain, query_gain, key_gain, conv_value, conv_gate, conv_kernel,
    channel_gain, channel_shift, heads_out, conv_out,
):
    mine, other = fused_call(
        (lax.axis_size("fs"), lax.axis_size("sp"), lax.axis_size("tp")),
        tokens[0], mix_gain, rope_weight, conv_kernel, channel_gain, channel_shift,
        latent_gain, memory_gain, query_gain, key_gain,
        query_down, memory_down, conv_value, conv_gate,
        query_up, key_up, value_up, heads_out, conv_out,
    )
    return join(mine, other)[None]


def solution(mesh):
    in_specs = (
        P("fs", "sp", None),
        P(),
        P("fs", "tp"),
        P("fs", "tp"),
        P(),
        P("fs", "tp"),
        P("fs", "tp"),
        P("fs", "tp"),
        P(),
        P(),
        P(),
        P(),
        P("fs", "tp"),
        P("fs", "tp"),
        P(None, "tp"),
        P("tp"),
        P("tp"),
        P("tp", "fs"),
        P("tp", "fs"),
    )
    out_specs = P("fs", "sp", None)
    n_fs, n_sp, n_tp = (mesh.shape[axis] for axis in ("fs", "sp", "tp"))
    fits = n_fs == 4 and n_tp == 2 and n_sp in (2, 4)
    body = fused_local if fits else local
    return jax.shard_map(body, mesh=mesh, in_specs=in_specs, out_specs=out_specs, check_vma=False)
```

```python
import functools

import jax
import jax.numpy as jnp
import numpy as np
from jax import lax
from jax.experimental import pallas as pl
from jax.experimental.pallas import tpu as pltpu
from jax.sharding import PartitionSpec as P

MESH_ID = pl.DeviceIdType.MESH

QK_NOPE = 64
QK_ROPE = 32
V_DIM = 64
CONV_W = 1024
SEG = 64
QK_DIM = 96


epsilon = 1e-06
rope_base = 10000.0
masked_score = -1e30


def norm_rows(matrix, scale_vector):
    return (
        matrix
        * lax.rsqrt(jnp.mean(matrix * matrix, axis=-1, keepdims=True) + epsilon)
        * scale_vector
    )


def rope_tables(positions):
    inverse_freq = 1.0 / rope_base ** (jnp.arange(0, QK_ROPE, 2, dtype=jnp.float32) / QK_ROPE)
    angles = positions.astype(jnp.float32)[:, None] * inverse_freq[None, :]
    return (jnp.cos(angles)[:, None, :], jnp.sin(angles)[:, None, :])


def rotate(matrix, cosine_table, sine_table):
    half_width = matrix.shape[-1] // 2
    front_half = matrix[..., :half_width]
    back_half = matrix[..., half_width:]
    return jnp.concatenate(
        [
            front_half * cosine_table - back_half * sine_table,
            front_half * sine_table + back_half * cosine_table,
        ],
        axis=-1,
    )


def heads_query(latent, weight, scale_vector, cosine_table, sine_table):
    row_count = latent.shape[0]
    projected = jnp.dot(latent, weight, preferred_element_type=jnp.float32)
    projected = norm_rows(
        projected.reshape(row_count, weight.shape[1] // QK_DIM, QK_DIM), scale_vector
    )
    turned = rotate(projected[..., QK_NOPE:], cosine_table, sine_table)
    return jnp.concatenate([projected[..., :QK_NOPE], turned], axis=-1).astype(jnp.bfloat16)


def heads_key(latent, rope_rows, weight, scale_vector, cosine_table, sine_table):
    row_count = latent.shape[0]
    head_count = weight.shape[1] // QK_NOPE
    nope_part = jnp.dot(latent, weight, preferred_element_type=jnp.float32).reshape(
        row_count, head_count, QK_NOPE
    )
    shared = jnp.broadcast_to(
        rope_rows.astype(jnp.float32)[:, None, :], (row_count, head_count, QK_ROPE)
    )
    joined = norm_rows(jnp.concatenate([nope_part, shared], axis=-1), scale_vector)
    turned = rotate(joined[..., QK_NOPE:], cosine_table, sine_table)
    return jnp.concatenate([joined[..., :QK_NOPE], turned], axis=-1).astype(jnp.bfloat16)


RIM = 32


def relayed_rows(rows, paired):
    return (rows * 5 // 16) // 16 * 16 if paired else 0


def gather_kernel(
    sizes,
    x_ref, gain_ref, rope_ref, taps_ref, cgain_ref, cshift_ref,
    qd, md, cv, cg, qu, ku, vu, ho, co,
    lq_all, lm_all, rr_all, conv_ref, qu_all, ku_all, vu_all, ho_all, co_all,
    qd_all, md_all, cv_all, cg_all, normed, acc_q, acc_m, acc_v, acc_g, ext, tail, rim,
    sums, stats, stats_all,
    send_d, recv_d, send_r, recv_r, send_z, recv_z, local_sem, rim_sem,
    sp_send, sp_recv, rr_send, rr_recv, tp_send, tp_recv,
):
    n_fs, n_sp, n_tp = sizes
    paired = n_sp % 2 == 0
    f = lax.axis_index("fs")
    s = lax.axis_index("sp")
    t = lax.axis_index("tp")
    parity = lax.rem(s, 2)
    partner = s + 1 - 2 * parity

    barrier = pltpu.get_barrier_semaphore()
    for axis, at, count in (("fs", f, n_fs), ("sp", s, n_sp), ("tp", t, n_tp)):
        for k in range(1, count):
            pl.semaphore_signal(
                barrier, inc=1, device_id={axis: lax.rem(at + k, count)}, device_id_type=MESH_ID
            )
    pl.semaphore_wait(barrier, n_fs + n_sp + n_tp - 3)

    jobs = [
        (qd, qd_all, 0), (md, md_all, 0), (cv, cv_all, 0), (cg, cg_all, 0),
        (qu, qu_all, 0), (ku, ku_all, 0), (vu, vu_all, 0), (ho, ho_all, 1), (co, co_all, 1),
    ]
    last = len(jobs) - 1
    ahead = 4

    def place(whole, shard, dim, owner, start, count):
        rows, cols = shard.shape
        if dim == 0:
            return whole.at[pl.ds(pl.multiple_of(owner * rows + start, 16), count), :]
        return whole.at[
            pl.ds(pl.multiple_of(start, 16), count),
            pl.ds(pl.multiple_of(owner * cols, 128), cols),
        ]

    square = n_fs == 4
    if square:
        near_x = f + 1 - 2 * lax.rem(f, 2)
        near_y = lax.rem(f + 2, 4)
        far = lax.rem(near_x + 2, 4)
        targets = sources = [near_x, near_y]
    else:
        targets = [lax.rem(f + k, n_fs) for k in range(1, n_fs)]
        sources = [lax.rem(f + n_fs - k, n_fs) for k in range(1, n_fs)]

    direct, far_copies, over_sp, own = [], [], [], []
    for a, (shard, whole, dim) in enumerate(jobs):
        rows = shard.shape[0]
        less = 0 if a == last else relayed_rows(rows, paired)
        start = parity * less
        count = rows - less
        direct.append([
            pltpu.make_async_remote_copy(
                src_ref=shard.at[pl.ds(pl.multiple_of(start, 16), count), :],
                dst_ref=place(whole, shard, dim, f, start, count),
                send_sem=send_d.at[a, k], recv_sem=recv_d.at[a, k],
                device_id={"fs": target}, device_id_type=MESH_ID,
            )
            for k, target in enumerate(targets)
        ])
        halves = []
        if square:
            half = (count // 2 + 15) // 16 * 16
            for k, (owner, target, begin, size) in enumerate((
                (near_y, near_x, start, half), (near_x, near_y, start + half, count - half)
            )):
                piece = place(whole, shard, dim, owner, begin, size)
                halves.append(pltpu.make_async_remote_copy(
                    src_ref=piece, dst_ref=piece,
                    send_sem=send_r.at[a, k], recv_sem=recv_r.at[a, k],
                    device_id={"fs": target}, device_id_type=MESH_ID,
                ))
        far_copies.append(halves)
        across = []
        if less:
            lack = parity * (rows - less)
            for k, owner in enumerate(sources + ([far] if square else [])):
                piece = place(whole, shard, dim, owner, lack, less)
                across.append(pltpu.make_async_remote_copy(
                    src_ref=piece, dst_ref=piece,
                    send_sem=send_z.at[a, k], recv_sem=recv_z.at[a, k],
                    device_id={"sp": partner}, device_id_type=MESH_ID,
                ))
        over_sp.append(across)
        own.append(pltpu.make_async_copy(
            shard, place(whole, shard, dim, f, 0, rows), local_sem.at[a]
        ))

    def begin_array(a):
        if a <= last:
            for copy in direct[a]:
                copy.start()

    def finish_far(a):
        for copy in far_copies[a]:
            copy.wait_recv()
        for copy in over_sp[a][len(sources):]:
            copy.start()

    def tick(a):
        for copy in direct[a]:
            copy.wait_recv()
        for copy in far_copies[a]:
            copy.start()
        begin_array(a + ahead)
        for copy in over_sp[a][: len(sources)]:
            copy.start()
        if a >= 1:
            finish_far(a - 1)

    def complete(a):
        own[a].wait()
        for copy in over_sp[a]:
            copy.wait_recv()

    for a in range(ahead):
        begin_array(a)
    for copy in own:
        copy.start()

    rows = x_ref.shape[0]
    part = 32

    @pl.loop(0, rows // part)
    def _(i):
        at = pl.ds(pl.multiple_of(i * part, part), part)
        x = x_ref[at, :].astype(jnp.float32)
        scale = lax.rsqrt(jnp.mean(x * x, axis=-1, keepdims=True) + epsilon)
        normed[at, :] = (x * scale * gain_ref[...]).astype(jnp.bfloat16)

    depth = qd.shape[0]

    def project(weight, acc):
        acc[...] = jnp.zeros_like(acc)

        @pl.loop(0, n_fs)
        def _(i):
            at = pl.ds(pl.multiple_of(i * depth, depth), depth)
            acc[...] += jnp.dot(
                normed[:, at], weight[at, :], preferred_element_type=jnp.float32
            )

    mine = pl.ds(pl.multiple_of(s * rows, 16), rows)
    rr_all[mine, :] = jnp.dot(
        normed[...], rope_ref[...], preferred_element_type=jnp.float32
    ).astype(jnp.bfloat16)
    tick(0)
    tick(1)
    tick(2)
    complete(0)
    project(qd_all, acc_q)
    lq_all[t, :, :] = acc_q[...].astype(jnp.bfloat16)
    tick(3)
    complete(1)
    project(md_all, acc_m)
    lm_all[t, mine, :] = acc_m[...].astype(jnp.bfloat16)
    tick(4)
    complete(2)
    project(cv_all, acc_v)

    exchanges, passes = [], []
    for k in range(1, n_sp):
        peer = {"sp": lax.rem(s + k, n_sp)}
        exchanges.append(pltpu.make_async_remote_copy(
            src_ref=lm_all.at[t, mine, :], dst_ref=lm_all.at[t, mine, :],
            send_sem=sp_send.at[k - 1], recv_sem=sp_recv.at[k - 1],
            device_id=peer, device_id_type=MESH_ID,
        ))
        exchanges.append(pltpu.make_async_remote_copy(
            src_ref=rr_all.at[mine, :], dst_ref=rr_all.at[mine, :],
            send_sem=rr_send.at[k - 1], recv_sem=rr_recv.at[k - 1],
            device_id=peer, device_id_type=MESH_ID,
        ))
    tp_peers = [{"tp": lax.rem(t + k, n_tp)} for k in range(1, n_tp)]

    def to_tp(kind, source, landing):
        return [
            pltpu.make_async_remote_copy(
                src_ref=source, dst_ref=landing(k),
                send_sem=tp_send.at[kind, k], recv_sem=tp_recv.at[kind, k],
                device_id=peer, device_id_type=MESH_ID,
            )
            for k, peer in enumerate(tp_peers)
        ]

    query_copies = to_tp(0, lq_all.at[t], lambda k: lq_all.at[t])
    memory_copies = to_tp(1, lm_all.at[t], lambda k: lm_all.at[t])
    stat_copies = to_tp(2, stats, lambda k: stats_all.at[k])
    for copy in exchanges + query_copies:
        copy.start()
    tick(5)
    complete(3)
    project(cg_all, acc_g)

    @pl.loop(0, rows // part)
    def _(i):
        at = pl.ds(pl.multiple_of(i * part, part), part)
        gated = (acc_v[at, :] * jax.nn.sigmoid(acc_g[at, :])).astype(jnp.bfloat16)
        ext[pl.ds(pl.multiple_of(RIM + i * part, part), part), :] = gated.astype(jnp.float32)

    tail[...] = ext[pl.ds(rows, RIM), :].astype(jnp.bfloat16)
    rim_copy = pltpu.make_async_remote_copy(
        src_ref=tail, dst_ref=rim, send_sem=rim_sem.at[0], recv_sem=rim_sem.at[1],
        device_id={"sp": lax.rem(s + 1, n_sp)}, device_id_type=MESH_ID,
    )
    tick(6)

    @pl.when(s < n_sp - 1)
    def _():
        rim_copy.start()

    for copy in exchanges:
        copy.wait_recv()
    for copy in memory_copies:
        copy.start()

    @pl.when(s > 0)
    def _():
        rim_copy.wait_recv()
        ext[pl.ds(0, RIM), :] = rim[...].astype(jnp.float32)

    @pl.when(s == 0)
    def _():
        ext[pl.ds(0, RIM), :] = jnp.zeros((RIM, ext.shape[1]), jnp.float32)

    tap_count = taps_ref.shape[0]
    block = 64

    def convolve(c):
        cols = pl.ds(pl.multiple_of(c * 128, 128), 128)
        taps = taps_ref[:, cols].astype(jnp.float32)
        for r in range(0, rows, block):
            total = jnp.zeros((block, 128), jnp.float32)
            for j in range(tap_count):
                total = total + ext[
                    pl.ds(r + RIM - (tap_count - 1) + j, block), cols
                ] * taps[j : j + 1, :]
            sums[pl.ds(r, block), cols] = total

    tiles = ext.shape[1] // 128
    pl.loop(0, tiles // 2)(convolve)
    tick(7)
    pl.loop(tiles // 2, tiles)(convolve)

    @pl.loop(0, rows // part)
    def _(i):
        begin = pl.multiple_of(i * part, part)
        values = sums[pl.ds(begin, part), :]
        stats[pl.ds(begin, part), :] = jnp.broadcast_to(
            jnp.sum(values, axis=1, keepdims=True), (part, 128)
        )
        stats[pl.ds(pl.multiple_of(rows + begin, part), part), :] = jnp.broadcast_to(
            jnp.sum(values * values, axis=1, keepdims=True), (part, 128)
        )

    tick(8)
    for copy in stat_copies:
        copy.start()
    for copy in stat_copies:
        copy.wait_recv()

    channels = ext.shape[1] * n_tp

    @pl.loop(0, rows // part)
    def _(i):
        begin = pl.multiple_of(i * part, part)
        upper = pl.ds(begin, part)
        lower = pl.ds(pl.multiple_of(rows + begin, part), part)
        total, squares = stats[upper, :], stats[lower, :]
        for k in range(n_tp - 1):
            total = total + stats_all[k, upper, :]
            squares = squares + stats_all[k, lower, :]
        mean = total[:, :1] / channels
        spread = squares[:, :1] / channels - mean * mean
        shaped = (sums[upper, :] - mean) * lax.rsqrt(spread + epsilon)
        conv_ref[upper, :] = jax.nn.silu(
            shaped * cgain_ref[...] + cshift_ref[...]
        ).astype(jnp.bfloat16)

    finish_far(last)
    for a in range(4, last + 1):
        complete(a)
    for copy in query_copies + memory_copies:
        copy.wait_recv()
    for group in direct + far_copies + over_sp:
        for copy in group:
            copy.wait_send()
    for copy in exchanges + query_copies + memory_copies + stat_copies:
        copy.wait_send()

    @pl.when(s < n_sp - 1)
    def _():
        rim_copy.wait_send()


def gather_and_project(
    sizes, x, mix_gain, rope_weight, taps, channel_gain, channel_shift,
    qd, md, cv, cg, qu, ku, vu, ho, co,
):
    n_fs, n_sp, n_tp = sizes
    rows = x.shape[0]
    bf16, f32 = jnp.bfloat16, jnp.float32
    vmem = pl.BlockSpec(memory_space=pltpu.VMEM)
    hbm = pl.BlockSpec(memory_space=pl.ANY)

    def whole(w, dim=0):
        return (w.shape[0] * n_fs, w.shape[1]) if dim == 0 else (w.shape[0], w.shape[1] * n_fs)

    out_shapes = [
        ((n_tp, rows, qd.shape[1]), bf16), ((n_tp, n_sp * rows, md.shape[1]), bf16),
        ((n_sp * rows, rope_weight.shape[1]), bf16), ((rows, cv.shape[1]), bf16),
        (whole(qu), bf16), (whole(ku), bf16), (whole(vu), bf16),
        (whole(ho, 1), bf16), (whole(co, 1), bf16),
    ]
    dma = pltpu.SemaphoreType.DMA
    tp_others = max(n_tp - 1, 1)
    sp_others = max(n_sp - 1, 1)
    return pl.pallas_call(
        functools.partial(gather_kernel, sizes),
        out_shape=[jax.ShapeDtypeStruct(*o) for o in out_shapes],
        in_specs=[vmem] * 6 + [hbm] * 9,
        out_specs=[vmem] * 9,
        scratch_shapes=[
            pltpu.VMEM(whole(qd), bf16), pltpu.VMEM(whole(md), bf16),
            pltpu.VMEM(whole(cv), bf16), pltpu.VMEM(whole(cg), bf16),
            pltpu.VMEM(x.shape, bf16), pltpu.VMEM((rows, qd.shape[1]), f32),
            pltpu.VMEM((rows, md.shape[1]), f32),
            pltpu.VMEM((rows, cv.shape[1]), f32), pltpu.VMEM((rows, cv.shape[1]), f32),
            pltpu.VMEM((rows + RIM, cv.shape[1]), f32),
            pltpu.VMEM((RIM, cv.shape[1]), bf16), pltpu.VMEM((RIM, cv.shape[1]), bf16),
            pltpu.VMEM((rows, cv.shape[1]), f32), pltpu.VMEM((2 * rows, 128), f32),
            pltpu.VMEM((tp_others, 2 * rows, 128), f32),
            dma((9, n_fs - 1)), dma((9, n_fs - 1)), dma((9, 2)), dma((9, 2)),
            dma((9, n_fs - 1)), dma((9, n_fs - 1)), dma((9,)), dma((2,)),
            dma((sp_others,)), dma((sp_others,)), dma((sp_others,)), dma((sp_others,)),
            dma((3, tp_others)), dma((3, tp_others)),
        ],
        compiler_params=pltpu.CompilerParams(
            collective_id=0, has_side_effects=True, vmem_limit_bytes=56 * 1024 * 1024
        ),
    )(
        x, mix_gain[None, :], rope_weight, taps, channel_gain[None, :], channel_shift[None, :],
        qd, md, cv, cg, qu, ku, vu, ho, co,
    )


def key_block(key_count):
    block_size = key_count
    while block_size > 2048 and block_size % 2 == 0:
        block_size = block_size // 2
    return block_size


def sum_groups(partial):
    count = lax.axis_size("tp")
    if count != 2:
        return lax.psum(partial, "tp")
    other = lax.ppermute(partial, "tp", [(0, 1), (1, 0)])
    return (partial.astype(jnp.float32) + other.astype(jnp.float32)).astype(jnp.bfloat16)


def local(
    tokens,
    mix_gain,
    query_down,
    memory_down,
    rope_weight,
    query_up,
    key_up,
    value_up,
    latent_gain,
    memory_gain,
    query_gain,
    key_gain,
    conv_value,
    conv_gate,
    conv_kernel,
    channel_gain,
    channel_shift,
    heads_out,
    conv_out,
):
    own_rows = tokens[0]
    (
        query_parts, memory_parts, rope_piece, conv_result,
        up_query, up_keys, up_values, out_heads, out_conv,
    ) = gather_and_project(
        (lax.axis_size("fs"), lax.axis_size("sp"), lax.axis_size("tp")),
        own_rows, mix_gain, rope_weight, conv_kernel, channel_gain, channel_shift,
        query_down, memory_down, conv_value, conv_gate,
        query_up, key_up, value_up, heads_out, conv_out,
    )
    row_count = own_rows.shape[0]
    whole_query = jnp.concatenate(list(query_parts), axis=1)
    whole_memory = jnp.concatenate(list(memory_parts), axis=1)
    query_normed = norm_rows(whole_query.astype(jnp.float32), latent_gain).astype(jnp.bfloat16)
    memory_piece = norm_rows(whole_memory.astype(jnp.float32), memory_gain).astype(jnp.bfloat16)
    positions = lax.axis_index("sp") * row_count + jnp.arange(row_count, dtype=jnp.int32)
    cosine_table, sine_table = rope_tables(positions)
    queries = heads_query(query_normed, up_query, query_gain, cosine_table, sine_table)
    head_count = queries.shape[1]
    query_segment = positions // SEG
    score_scale = QK_DIM ** (-0.5)
    def attend(state_carry, key_rows, value_rows, key_pos):
        running_max, row_total, weighted = state_carry
        scores = (
            jnp.einsum("qhd,khd->qhk", queries, key_rows, preferred_element_type=jnp.float32)
            * score_scale
        )
        allowed = ((key_pos // SEG)[None, :] <= query_segment[:, None])[:, None, :]
        scores = jnp.where(allowed, scores, masked_score)
        new_max = jnp.maximum(running_max, jnp.max(scores, axis=2))
        weights = jnp.where(allowed, jnp.exp(scores - new_max[:, :, None]), 0.0)
        factor = jnp.exp(running_max - new_max)
        row_total = row_total * factor + jnp.sum(weights, axis=2)
        weighted = weighted * factor[:, :, None] + jnp.einsum(
            "qhk,khd->qhd",
            weights.astype(jnp.bfloat16),
            value_rows,
            preferred_element_type=jnp.float32,
        )
        return (new_max, row_total, weighted)

    initial = (
        jnp.full((row_count, head_count), masked_score, jnp.float32),
        jnp.zeros((row_count, head_count), jnp.float32),
        jnp.zeros((row_count, head_count, V_DIM), jnp.float32),
    )
    def block_keys(block_start, block_size):
        memory_block = lax.dynamic_slice_in_dim(memory_piece, block_start, block_size, 0)
        rope_block = lax.dynamic_slice_in_dim(rope_piece, block_start, block_size, 0)
        key_pos = block_start + jnp.arange(block_size, dtype=jnp.int32)
        cosine_keys, sine_keys = rope_tables(key_pos)
        key_rows = heads_key(memory_block, rope_block, up_keys, key_gain, cosine_keys, sine_keys)
        value_rows = (
            jnp.dot(memory_block, up_values, preferred_element_type=jnp.float32)
            .astype(jnp.bfloat16)
            .reshape(block_size, head_count, V_DIM)
        )
        return (key_rows, value_rows, key_pos)

    key_count = memory_piece.shape[0]
    block_size = key_block(key_count)

    def step(block_index, running):
        key_rows, value_rows, key_pos = block_keys(block_index * block_size, block_size)
        return attend(running, key_rows, value_rows, key_pos)

    final_state = lax.fori_loop(0, key_count // block_size, step, initial)
    running_max, row_total, weighted = final_state
    attention = (
        (weighted / row_total[:, :, None])
        .astype(jnp.bfloat16)
        .reshape(row_count, head_count * V_DIM)
    )
    mixer_rows = jnp.concatenate([attention, conv_result], axis=1)
    out_weight = jnp.concatenate([out_heads, out_conv], axis=0)
    partial_sum = jnp.dot(mixer_rows, out_weight, preferred_element_type=jnp.float32)
    mixed = sum_groups(partial_sum.astype(jnp.bfloat16))
    return mixed[None]


def table_rows(count):
    inverse_freq = 1.0 / np.float32(rope_base) ** (
        np.arange(0, QK_ROPE, 2, dtype=np.float32) / np.float32(QK_ROPE)
    )
    angles = inverse_freq[:, None] * np.arange(count, dtype=np.float32)[None, :]
    angles = angles.astype(np.float64)
    return np.cos(angles).astype(np.float32), np.sin(angles).astype(np.float32)


def dot_heads(left, right):
    return lax.dot_general(
        left, right, (((0,), (0,)), ((), ())), preferred_element_type=jnp.float32
    )


def swapped_rows(count, part):
    return (count * part // 16) // 16 * 16


def fused_kernel(
    sizes,
    x_hbm, gain_hbm, rope_hbm, taps_hbm, cgain_hbm, cshift_hbm,
    lgain_hbm, mgain_hbm, qgain_hbm, kgain_hbm, cos_hbm, sin_hbm,
    qd, md, ku, vu, qu, cv, cg, ho, co,
    mine_ref, other_ref,
    gain_ref, rope_ref, taps_ref, cgain_ref, cshift_ref,
    lgain_ref, mgain_ref, qgain_ref, kgain_ref, cos_ref, sin_ref,
    qd_all, md_all, ku_all, vu_all, qu_all, cv_all, cg_all, ho_all, co_all,
    x_all, normed, lq_all, lm_all, mem_all, rr_all, qn_t, q_t, k_t, v_t,
    turned, ropesq, qcol, kcol, bias, scores,
    att_t, att_out, att_all, conv_s, acc_v, acc_out, gate_out, gate_in, ext, rim_out, rim, sums, stats, stats_all,
    send_d, recv_d, send_r, recv_r, send_z, recv_z, local_sem, small_sem, rim_sem, x_sem,
    part_sem, sp_send, sp_recv, fw_send, fw_recv, tp_send, tp_recv, out_send, out_recv, known,
):
    n_fs, n_sp, n_tp = sizes
    f = lax.axis_index("fs")
    s = lax.axis_index("sp")
    t = lax.axis_index("tp")
    parity = lax.rem(s, 2)
    couple = lax.div(s, 2)
    couples = n_sp // 2
    partner = {"sp": s + 1 - 2 * parity}
    twin = {"tp": 1 - t}
    even, odd = parity == 0, parity == 1

    near_x = f + 1 - 2 * lax.rem(f, 2)
    near_y = lax.rem(f + 2, 4)
    far = lax.rem(near_x + 2, 4)
    sources = [near_x, near_y]
    has_below, has_above = s > 0, s < n_sp - 1

    barrier = pltpu.get_barrier_semaphore()

    def greet(device):
        pl.semaphore_signal(barrier, inc=1, device_id=device, device_id_type=MESH_ID)

    for device in (twin, {"fs": near_x}, {"fs": near_y}):
        greet(device)
    pl.when(has_below)(lambda: greet({"sp": s - 1}))
    pl.when(has_above)(lambda: greet({"sp": s + 1}))

    slots = 3
    rows = x_hbm.shape[0]
    x_own = pltpu.make_async_copy(x_hbm, x_all.at[parity], x_sem.at[0])
    x_own.start()
    small = [
        pltpu.make_async_copy(source, landing, small_sem.at[i % slots])
        for i, (source, landing) in enumerate((
            (gain_hbm, gain_ref), (rope_hbm, rope_ref), (taps_hbm, taps_ref),
            (cgain_hbm, cgain_ref), (cshift_hbm, cshift_ref), (lgain_hbm, lgain_ref),
            (mgain_hbm, mgain_ref), (qgain_hbm, qgain_ref), (kgain_hbm, kgain_ref),
            (cos_hbm, cos_ref), (sin_hbm, sin_ref),
        ))
    ]
    for copy in small[:slots]:
        copy.start()

    def remote(source, landing, send, recv, device):
        return pltpu.make_async_remote_copy(
            src_ref=source, dst_ref=landing, send_sem=send, recv_sem=recv,
            device_id=device, device_id_type=MESH_ID,
        )

    share = rows // n_tp
    slab = pl.ds(pl.multiple_of(t * share, 16), share)
    x_send = remote(
        x_hbm.at[slab, :], x_all.at[parity, slab, :], x_sem.at[1], x_sem.at[2], partner
    )
    theirs = x_all.at[1 - parity, slab, :]
    x_forward = remote(theirs, theirs, x_sem.at[3], x_sem.at[4], twin)

    def job(a, shard, whole, swap=None, dim=0, first=0, count=None):
        depth, cols = shard.shape
        count = depth if count is None else count
        lane, mine, lacking, giving = swap or (0, 0, 0, 0)
        lack, give = swapped_rows(count, lacking), swapped_rows(count, giving)
        kept = count - lack

        def place(owner, start, size):
            if dim == 0:
                return whole.at[pl.ds(pl.multiple_of(owner * depth + start, 16), size), :]
            return whole.at[
                pl.ds(pl.multiple_of(start, 16), size),
                pl.ds(pl.multiple_of(owner * cols, 128), cols),
            ]

        start = first + mine * lack
        direct = [
            remote(
                shard.at[pl.ds(start, kept), :], place(f, start, kept),
                send_d.at[a % slots, k], recv_d.at[a, k], {"fs": target},
            )
            for k, target in enumerate(sources)
        ]
        half = (kept // 2 + 15) // 16 * 16
        relays = []
        for k, (owner, target, begin, size) in enumerate((
            (near_y, near_x, start, half), (near_x, near_y, start + half, kept - half)
        )):
            piece = place(owner, begin, size)
            relays.append(remote(
                piece, piece, send_r.at[a % slots, k], recv_r.at[a, k], {"fs": target}
            ))
        gives, lacks = [], []
        if swap:
            for k, owner in enumerate(sources + [far]):
                sems = (send_z.at[lane, k], recv_z.at[lane, k], partner)
                if give:
                    piece = place(owner, first + mine * (count - give), give)
                    gives.append(remote(piece, piece, *sems))
                if lack:
                    piece = place(owner, first + (1 - mine) * kept, lack)
                    lacks.append(remote(piece, piece, *sems))
        own = pltpu.make_async_copy(
            shard.at[pl.ds(first, count), :], place(f, first, count), local_sem.at[a % slots]
        )
        return direct, relays, gives, own, lacks

    def half_columns(shard):
        width = shard.shape[1] // 2
        return shard.at[:, pl.ds(pl.multiple_of(parity * width, 128), width)]

    wide = cv.shape[1] // 2
    side = pl.ds(pl.multiple_of(parity * wide, 128), wide)
    half_rows = ho.shape[0] // 2
    last_rows = half_rows // 4
    first_rows = half_rows * 12 // 8

    def swapping(lane, even_lacks, odd_lacks, *rest):
        shard, whole, *rest = rest
        return [
            (even, shard, whole, (lane, 0, even_lacks, odd_lacks), *rest),
            (odd, shard, whole, (lane, 1, odd_lacks, even_lacks), *rest),
        ]

    plan = [
        [(even, qd, qd_all), (odd, md, md_all)],
        [(None, half_columns(ku), ku_all)], [(None, half_columns(vu), vu_all)],
        [(None, half_columns(qu), qu_all)],
        swapping(0, 8, 8, ho, ho_all, 1, 0, first_rows),
        [(None, half_columns(cv), cv_all)], [(None, half_columns(cg), cg_all)],
        swapping(1, 8, 4, ho, ho_all, 1, first_rows, 2 * half_rows - first_rows),
        swapping(2, 6, 2, co, co_all, 1, 0, half_rows),
        [(None, co, co_all, None, 1, half_rows, half_rows - last_rows)],
        [(None, co, co_all, None, 1, 2 * half_rows - last_rows, last_rows)],
    ]
    jobs = [[(who[0], job(a, *who[1:])) for who in group] for a, group in enumerate(plan)]
    last = len(jobs) - 1
    lanes = [a for a, group in enumerate(plan) if len(group[0]) > 3 and group[0][3]]

    def each(a, action):
        for condition, parts in jobs[a]:
            if condition is None:
                action(parts)
            else:
                pl.when(condition)(functools.partial(action, parts))

    def sent(a, kind):
        def go(parts):
            for copy in parts[kind]:
                copy.wait_send()

        if a >= 0:
            each(a, go)

    def begin_array(a):
        def start(parts):
            for copy in parts[0]:
                copy.start()
            parts[3].start()

        if a <= last:
            sent(a - slots, 0)
            each(a, start)

    def finish_far(a):
        def go(parts):
            with jax.named_scope(f"far_{a}"):
                for copy in parts[1]:
                    copy.wait_recv()
            for copy in parts[2][len(sources):]:
                copy.start()

        each(a, go)

    def swap_near(a):
        def swap(parts):
            for copy in parts[2][: len(sources)]:
                copy.start()

        if a in lanes:
            each(a, swap)

    begins = {0: [3], 1: [4], 2: [5], 3: [6], 5: [7], 6: [8], 7: [9], 8: [10]}

    def tick(a):
        def go(parts):
            with jax.named_scope(f"direct_{a}"):
                for copy in parts[0]:
                    copy.wait_recv()
                parts[3].wait()
            for copy in parts[1]:
                copy.start()

        sent(a - slots, 1)
        each(a, go)
        for later in begins.get(a, ()):
            begin_array(later)
        swap_near(a)

    def complete(a, which=slice(None)):
        def go(parts):
            with jax.named_scope(f"across_{a}"):
                for copy in parts[4][which]:
                    copy.wait_recv()

        each(a, go)

    with jax.named_scope("entry"):
        pl.semaphore_wait(
            barrier, 3 + has_below.astype(jnp.int32) + has_above.astype(jnp.int32)
        )
    x_send.start()
    for a in range(slots):
        begin_array(a)

    @pl.when(jnp.logical_and(has_below, has_above))
    def _():
        pl.semaphore_signal(
            known.at[0], inc=1, device_id={"sp": s - 1}, device_id_type=MESH_ID
        )

    with jax.named_scope("small_wait"):
        for r in range(0, len(small), slots):
            if r:
                for copy in small[r : r + slots]:
                    copy.start()
            for copy in small[r : r + slots]:
                copy.wait()
        x_own.wait()

    part = 32

    def norm_block(b):
        @pl.loop(0, rows // part)
        def _(i):
            at = pl.ds(pl.multiple_of(i * part, part), part)
            x = x_all[b, at, :].astype(jnp.float32)
            scale = lax.rsqrt(jnp.mean(x * x, axis=-1, keepdims=True) + epsilon)
            normed[b, at, :] = (x * scale * gain_ref[...]).astype(jnp.bfloat16)

        rr_all[2 * couple + b] = lax.dot_general(
            rope_ref[...], normed[b], (((1,), (1,)), ((), ())), preferred_element_type=jnp.float32
        ).astype(jnp.bfloat16)

    norm_block(parity)
    half_rope = QK_ROPE // 2

    def column(row_ref, col_ref):
        shape = (QK_DIM, QK_DIM)
        here = lax.broadcasted_iota(jnp.int32, shape, 0) == lax.broadcasted_iota(jnp.int32, shape, 1)
        spread_row = jnp.broadcast_to(row_ref[...], shape)
        picked = jnp.sum(jnp.where(here, spread_row, 0.0), axis=1, keepdims=True)
        col_ref[...] = jnp.broadcast_to(picked, col_ref.shape)

    column(qgain_ref, qcol)
    column(kgain_ref, kcol)

    @pl.loop(2 * couple + 2, n_sp)
    def _(j):
        mem_all[j] = jnp.zeros(mem_all.shape[1:], jnp.bfloat16)
        rr_all[j] = jnp.zeros(rr_all.shape[1:], jnp.bfloat16)

    @pl.loop(0, n_sp)
    def _(j):
        shape = (rows, 2 * rows)
        key_at = j * rows + lax.broadcasted_iota(jnp.int32, shape, 0)
        query_at = 2 * couple * rows + lax.broadcasted_iota(jnp.int32, shape, 1)
        bias[j] = jnp.where(
            lax.div(key_at, SEG) <= lax.div(query_at, SEG), 0.0, masked_score
        )

    tick(0)
    with jax.named_scope("x_wait"):
        x_send.wait_recv()
    x_forward.start()
    tick(1)
    with jax.named_scope("x_forward"):
        x_forward.wait_recv()
    norm_block(1 - parity)
    tick(2)
    finish_far(0)

    @pl.when(s < n_sp - 2)
    def _():
        pl.semaphore_wait(known.at[0], 1)


    def project(weight, b):
        return jnp.dot(normed[b], weight[...], preferred_element_type=jnp.float32)

    lat = md.shape[1]
    lat_q = qd.shape[1]
    held = pl.ds(pl.multiple_of(t * lat, lat), lat)
    query_across = remote(lq_all.at[t], lq_all.at[t], part_sem.at[0], part_sem.at[1], partner)
    query_copy = remote(lq_all.at[t], lq_all.at[t], tp_send.at[0], tp_recv.at[0], twin)
    memory_copy = remote(lm_all.at[t], lm_all.at[t], tp_send.at[1], tp_recv.at[1], twin)
    stat_copy = remote(stats, stats_all, tp_send.at[2], tp_recv.at[2], twin)
    gate_across = remote(gate_out, gate_in, part_sem.at[2], part_sem.at[3], partner)

    complete(0)

    @pl.when(even)
    def _():
        for b in range(2):
            lq_all[t, b] = project(qd_all, b).astype(jnp.bfloat16)
        query_across.start()
        query_copy.start()

    @pl.when(odd)
    def _():
        for b in range(2):
            lm_all[t, b] = project(md_all, b).astype(jnp.bfloat16)
        memory_copy.start()

    tick(3)

    def normed_columns(parts, width, gain_at, put):
        @pl.loop(0, rows // 128)
        def _(i):
            at = pl.ds(pl.multiple_of(i * 128, 128), 128)
            pieces = [parts(g, at).astype(jnp.float32) for g in range(n_tp)]
            total = sum(jnp.sum(p * p, axis=-1, keepdims=True) for p in pieces)
            scale = lax.rsqrt(total / (width * n_tp) + epsilon)
            for g in range(n_tp):
                shaped = (pieces[g] * scale * gain_at(g * width, width)).astype(jnp.bfloat16)
                put(g * width, width, at, shaped.astype(jnp.float32).T.astype(jnp.bfloat16))

    pair = pl.ds(2 * couple, 2)
    both = mem_all.at[pair, held, :]
    back = remote(both, both, part_sem.at[4], part_sem.at[5], partner)
    back_forward = remote(both, both, fw_send.at[couples - 1], fw_recv.at[couples - 1], twin)
    onward, forwards = [], []
    for d in range(1, couples):
        group = []
        later = lax.rem(couple + d, couples)
        for e in range(2):
            target = {"sp": 2 * later + e}
            group.append((
                remote(
                    mem_all.at[pair, held, :], mem_all.at[pair, held, :],
                    sp_send.at[d - 1, e, 0], sp_recv.at[d - 1, 0], target,
                ),
                remote(
                    rr_all.at[pair], rr_all.at[pair],
                    sp_send.at[d - 1, e, 1], sp_recv.at[d - 1, 1], target,
                ),
            ))
        onward.append(group)
        earlier = mem_all.at[pl.ds(2 * lax.rem(couple + couples - d, couples), 2), held, :]
        forwards.append(remote(earlier, earlier, fw_send.at[d - 1], fw_recv.at[d - 1], twin))

    @pl.when(odd)
    def _():
        with jax.named_scope("memory_wait"):
            memory_copy.wait_recv()
        for b in (1, 0):
            def put_memory(begin, width, at, piece, b=b):
                mem_all[2 * couple + b, begin : begin + width, at] = piece

            normed_columns(
                lambda g, at, b=b: lm_all[g, b, at, :], lat,
                lambda begin, width: mgain_ref[:, begin : begin + width], put_memory,
            )
        for d in range(1, couples):
            @pl.when(couple + d < couples)
            def _(d=d):
                for e in range(2):
                    for copy in onward[d - 1][e]:
                        copy.start()
        back.start()

    finish_far(1)
    tick(4)
    finish_far(2)

    @pl.when(even)
    def _():
        with jax.named_scope("back_wait"):
            back.wait_recv()
        back_forward.start()

    tick(5)
    finish_far(3)

    @pl.when(odd)
    def _():
        with jax.named_scope("query_across"):
            query_across.wait_recv()
        query_copy.start()


    @pl.when(even)
    def _():
        with jax.named_scope("back_forward"):
            back_forward.wait_recv()

    def expand(j):
        k_t[j] = dot_heads(ku_all[...], mem_all[j])
        v_t[j] = dot_heads(vu_all[...], mem_all[j]).astype(jnp.bfloat16)
        shared = rr_all[j].astype(jnp.float32)
        ropesq[j] = jnp.sum(shared * shared, axis=0, keepdims=True)
        shared = shared * kcol[QK_NOPE:, :]
        front, back_half = shared[:half_rope], shared[half_rope:]
        at = pl.ds(pl.multiple_of(j * rows, rows), rows)
        cosine, sine = cos_ref[:, at], sin_ref[:, at]
        turned[j] = jnp.concatenate(
            [front * cosine - back_half * sine, front * sine + back_half * cosine], axis=0
        )

    pl.loop(2 * couple, n_sp)(expand)
    for d in range(1, couples):
        @pl.when(couple >= d)
        def _(d=d):
            with jax.named_scope(f"behind_{d}"):
                for copy in onward[d - 1][0]:
                    copy.wait_recv()
            forwards[d - 1].start()
    with jax.named_scope("query_wait"):
        query_copy.wait_recv()
    for b in range(2):
        def put_query(begin, width, at, piece, b=b):
            at = pl.ds(pl.multiple_of(b * rows + at.start, 128), at.size)
            qn_t[begin : begin + width, at] = piece

        normed_columns(
            lambda g, at, b=b: lq_all[g, b, at, :], lat_q,
            lambda begin, width: jnp.concatenate(
                [lgain_ref[r : r + 1, :] for r in range(begin // 128, (begin + width) // 128)],
                axis=1,
            ),
            put_query,
        )
    for d in range(1, couples):
        @pl.when(couple >= d)
        def _(d=d):
            with jax.named_scope(f"forward_{d}"):
                forwards[d - 1].wait_recv()
    pl.loop(0, 2 * couple)(expand)
    q_t[...] = dot_heads(qu_all[...], qn_t[...])
    tick(6)
    finish_far(4)
    heads = qu.shape[1] // 2 // QK_DIM
    here = pl.ds(pl.multiple_of(2 * couple * rows, rows), 2 * rows)
    score_scale = QK_DIM ** (-0.5)

    def head(h):
        q = q_t[pl.ds(pl.multiple_of(h * QK_DIM, QK_DIM), QK_DIM), :]
        q = q * lax.rsqrt(jnp.mean(q * q, axis=0, keepdims=True) + epsilon) * qcol[...]
        front, back_half = q[QK_NOPE : QK_NOPE + half_rope], q[QK_NOPE + half_rope :]
        cosine, sine = cos_ref[:, here], sin_ref[:, here]
        q = jnp.concatenate(
            [
                q[:QK_NOPE],
                front * cosine - back_half * sine,
                front * sine + back_half * cosine,
            ],
            axis=0,
        ).astype(jnp.bfloat16)
        krow = pl.ds(pl.multiple_of(h * QK_NOPE, QK_NOPE), QK_NOPE)
        vrow = pl.ds(pl.multiple_of(h * V_DIM, V_DIM), V_DIM)
        top = jnp.full((1, 2 * rows), masked_score, jnp.float32)
        for j in range(n_sp):
            nope = k_t[j, krow, :]
            scale = lax.rsqrt(
                (jnp.sum(nope * nope, axis=0, keepdims=True) + ropesq[j]) / QK_DIM + epsilon
            )
            key = jnp.concatenate(
                [nope * scale * kcol[:QK_NOPE, :], turned[j] * scale], axis=0
            ).astype(jnp.bfloat16)
            block = dot_heads(key, q) + bias[j]
            scores[j] = block
            top = jnp.maximum(top, jnp.max(block, axis=0, keepdims=True))
        total = jnp.zeros((1, 2 * rows), jnp.float32)
        summed = jnp.zeros((V_DIM, 2 * rows), jnp.float32)
        for j in range(n_sp):
            weight = jnp.exp((scores[j] - top) * score_scale)
            total = total + jnp.sum(weight, axis=0, keepdims=True)
            summed = summed + jnp.dot(
                v_t[j, vrow, :], weight.astype(jnp.bfloat16),
                preferred_element_type=jnp.float32,
            )
        att_t[vrow, :] = summed / total

    pl.loop(0, heads // 2)(head)
    finish_far(5)
    for b in range(2):
        acc_v[b] = project(cv_all, b)
    tick(7)
    pl.loop(heads // 2, heads)(head)
    value_rows = heads * V_DIM
    own_rows = pl.ds(pl.multiple_of(parity * value_rows, value_rows), value_rows)
    their_lanes = pl.ds(pl.multiple_of((1 - parity) * rows, rows), rows)
    own_lanes = pl.ds(pl.multiple_of(parity * rows, rows), rows)
    att_across = remote(
        att_out, att_all.at[own_rows, :], part_sem.at[6], part_sem.at[7], partner
    )
    att_out[...] = att_t[:, their_lanes].astype(jnp.bfloat16)
    att_across.start()
    att_all[own_rows, :] = att_t[:, own_lanes].astype(jnp.bfloat16)
    finish_far(6)
    opposite = pl.ds(pl.multiple_of((1 - parity) * wide, 128), wide)
    body_rows, halo = pl.ds(RIM, rows), pl.ds(0, RIM)

    def gate(b):
        gates = project(cg_all, b)
        return (acc_v[b] * jax.nn.sigmoid(gates)).astype(jnp.bfloat16)

    end = slice(rows - RIM, rows)
    later_rim = remote(
        rim_out, rim.at[parity], rim_sem.at[0], rim_sem.at[1 + parity],
        {"sp": 2 * lax.rem(couple + 1, couples)},
    )
    has_later, has_earlier = couple < couples - 1, jnp.logical_and(even, couple > 0)
    lower = gate(0)

    @pl.when(even)
    def _():
        ext[body_rows, side] = lower.astype(jnp.float32)
        ext[halo, :] = jnp.zeros((RIM, ext.shape[1]), jnp.float32)
        gate_out[halo, :] = lower[end]

    @pl.when(odd)
    def _():
        gate_out[halo, :] = jnp.zeros((RIM, wide), jnp.bfloat16)
        gate_out[body_rows, :] = lower
        gate_across.start()
        ext[halo, side] = lower[end].astype(jnp.float32)

    upper = gate(1)
    rim_out[...] = upper[end]

    @pl.when(has_later)
    def _():
        later_rim.start()

    @pl.when(even)
    def _():
        gate_out[body_rows, :] = upper
        gate_across.start()

    @pl.when(odd)
    def _():
        ext[body_rows, side] = upper.astype(jnp.float32)

    tick(8)

    @pl.when(has_earlier)
    def _():
        with jax.named_scope("rim_wait"):
            for g in range(2):
                remote(
                    rim_out, rim.at[g], rim_sem.at[0], rim_sem.at[1 + g], partner
                ).wait_recv()
        for g in range(2):
            ext[halo, g * wide : (g + 1) * wide] = rim[g].astype(jnp.float32)

    tap_count = taps_ref.shape[0]
    block = 64

    lead = RIM - (tap_count - 1)

    def convolve(c):
        cols = pl.ds(pl.multiple_of(c * 128, 128), 128)
        taps = taps_ref[:, cols].astype(jnp.float32)
        for r in range(0, rows, block):
            total = jnp.zeros((block, 128), jnp.float32)
            for shift in range(8):
                height = block + (8 if shift else 0)
                partial = jnp.zeros((height, 128), jnp.float32)
                for offset in range(shift, RIM + 1, 8):
                    if offset >= lead:
                        tap = taps[offset - lead : offset - lead + 1, :]
                        partial = partial + ext[pl.ds(r + offset - shift, height), cols] * tap
                total = total + partial[shift : shift + block]
            sums[pl.ds(r, block), cols] = total

    tiles = wide // 128
    pl.loop(parity * tiles, (parity + 1) * tiles)(convolve)
    pl.when(odd)(lambda: tick(9))
    with jax.named_scope("gate_wait"):
        gate_across.wait_recv()
    ext[body_rows, opposite] = gate_in[body_rows, :].astype(jnp.float32)

    @pl.when(odd)
    def _():
        ext[halo, opposite] = gate_in[halo, :].astype(jnp.float32)

    pl.loop((1 - parity) * tiles, (2 - parity) * tiles)(convolve)
    finish_far(7)

    @pl.loop(0, rows // part)
    def _(i):
        begin = pl.multiple_of(i * part, part)
        values = sums[pl.ds(begin, part), :]
        stats[pl.ds(begin, part), :] = jnp.broadcast_to(
            jnp.sum(values, axis=1, keepdims=True), (part, 128)
        )
        stats[pl.ds(pl.multiple_of(rows + begin, part), part), :] = jnp.broadcast_to(
            jnp.sum(values * values, axis=1, keepdims=True), (part, 128)
        )

    stat_copy.start()
    pl.when(even)(lambda: tick(9))
    with jax.named_scope("att_wait"):
        att_across.wait_recv()
    att = att_all[...].astype(jnp.float32).T.astype(jnp.bfloat16)
    span = ho.shape[1]

    complete(4)

    @pl.loop(0, n_fs)
    def _(i):
        cols = pl.ds(pl.multiple_of(i * span, span), span)
        acc_out[:, cols] = jnp.dot(
            att[:, :first_rows], ho_all[:first_rows, cols], preferred_element_type=jnp.float32
        )

    finish_far(8)
    with jax.named_scope("stat_wait"):
        stat_copy.wait_recv()
    channels = ext.shape[1] * n_tp

    @pl.loop(0, rows // part)
    def _(i):
        begin = pl.multiple_of(i * part, part)
        upper = pl.ds(begin, part)
        lower = pl.ds(pl.multiple_of(rows + begin, part), part)
        total = stats[upper, :] + stats_all[upper, :]
        squares = stats[lower, :] + stats_all[lower, :]
        mean = total[:, :1] / channels
        spread = squares[:, :1] / channels - mean * mean
        shaped = (sums[upper, :] - mean) * lax.rsqrt(spread + epsilon)
        conv_s[upper, :] = jax.nn.silu(
            shaped * cgain_ref[...] + cshift_ref[...]
        ).astype(jnp.bfloat16)

    tick(10)
    outs = []
    for i, owner in enumerate([f, near_x, near_y, far]):
        cols = pl.ds(pl.multiple_of(owner * span, span), span)
        outs.append(remote(
            mine_ref.at[:, cols], other_ref.at[:, cols], out_send.at[i], out_recv.at[i], twin
        ))
        if i == 1:
            complete(7, slice(0, len(sources)))
            complete(8, slice(0, len(sources)))
        if i == n_fs - 1:
            finish_far(9)
            finish_far(last)
            complete(7, slice(len(sources), None))
            complete(8, slice(len(sources), None))
        mine_ref[:, cols] = (
            acc_out[:, cols]
            + jnp.dot(att[:, first_rows:], ho_all[first_rows:, cols], preferred_element_type=jnp.float32)
            + jnp.dot(conv_s[...], co_all[:, cols], preferred_element_type=jnp.float32)
        ).astype(jnp.bfloat16)
        outs[i].start()

    for a in range(last + 1 - slots, last + 1):
        sent(a, 0)
        sent(a, 1)
    for a in lanes:
        sent(a, 2)
    for copy in (x_send, x_forward, query_copy, stat_copy, gate_across, att_across):
        copy.wait_send()

    @pl.when(even)
    def _():
        query_across.wait_send()
        back_forward.wait_send()

    @pl.when(odd)
    def _():
        memory_copy.wait_send()
        back.wait_send()
        for d in range(1, couples):
            @pl.when(couple + d < couples)
            def _(d=d):
                for e in range(2):
                    for copy in onward[d - 1][e]:
                        copy.wait_send()

    for d in range(1, couples):
        @pl.when(couple >= d)
        def _(d=d):
            forwards[d - 1].wait_send()

    @pl.when(has_later)
    def _():
        later_rim.wait_send()

    with jax.named_scope("out_wait"):
        for copy in outs:
            copy.wait()


def fused_call(
    sizes, x, mix_gain, rope_weight, taps, channel_gain, channel_shift,
    latent_gain, memory_gain, query_gain, key_gain,
    qd, md, cv, cg, qu, ku, vu, ho, co,
):
    n_fs, n_sp, n_tp = sizes
    rows, model = x.shape
    bf16, f32 = jnp.bfloat16, jnp.float32
    hbm = pl.BlockSpec(memory_space=pl.ANY)
    cosine, sine = table_rows(n_sp * rows)
    small = [
        mix_gain[None, :], rope_weight.T, taps, channel_gain[None, :], channel_shift[None, :],
        latent_gain.reshape(-1, 128), memory_gain[None, :], query_gain[None, :],
        key_gain[None, :], jnp.asarray(cosine), jnp.asarray(sine),
    ]

    def whole(w, dim=0, parts=1):
        rows_w, cols_w = w.shape[0], w.shape[1] // parts
        return (rows_w * n_fs, cols_w) if dim == 0 else (rows_w, cols_w * n_fs)

    def scratch(*shape, dtype=f32):
        return pltpu.VMEM(shape, dtype)

    dma = pltpu.SemaphoreType.DMA
    channels, lat = cv.shape[1], md.shape[1] * n_tp
    rope = rope_weight.shape[1]
    couples = n_sp // 2
    spare = max(couples - 1, 1)
    count, slots = 11, 3
    return pl.pallas_call(
        functools.partial(fused_kernel, sizes),
        out_shape=[jax.ShapeDtypeStruct((rows, ho.shape[1] * n_fs), bf16)] * 2,
        in_specs=[hbm] * 21,
        out_specs=[pl.BlockSpec(memory_space=pltpu.VMEM)] * 2,
        scratch_shapes=[scratch(*a.shape, dtype=a.dtype) for a in small] + [
            scratch(*whole(qd), dtype=bf16), scratch(*whole(md), dtype=bf16),
            scratch(*whole(ku, 0, 2), dtype=bf16), scratch(*whole(vu, 0, 2), dtype=bf16),
            scratch(*whole(qu, 0, 2), dtype=bf16), scratch(*whole(cv, 0, 2), dtype=bf16),
            scratch(*whole(cg, 0, 2), dtype=bf16), scratch(*whole(ho, 1), dtype=bf16),
            scratch(*whole(co, 1), dtype=bf16),
            scratch(2, rows, model, dtype=bf16), scratch(2, rows, model, dtype=bf16),
            scratch(n_tp, 2, rows, qd.shape[1], dtype=bf16),
            scratch(n_tp, 2, rows, md.shape[1], dtype=bf16),
            scratch(n_sp, lat, rows, dtype=bf16), scratch(n_sp, rope, rows, dtype=bf16),
            scratch(qu.shape[0] * n_fs, 2 * rows, dtype=bf16), scratch(qu.shape[1] // 2, 2 * rows),
            scratch(n_sp, ku.shape[1] // 2, rows),
            scratch(n_sp, vu.shape[1] // 2, rows, dtype=bf16),
            scratch(n_sp, rope, rows), scratch(n_sp, 1, rows),
            scratch(QK_DIM, 2 * rows), scratch(QK_DIM, rows),
            scratch(n_sp, rows, 2 * rows), scratch(n_sp, rows, 2 * rows),
            scratch(vu.shape[1] // 2, 2 * rows), scratch(vu.shape[1] // 2, rows, dtype=bf16),
            scratch(vu.shape[1], rows, dtype=bf16), scratch(rows, channels, dtype=bf16),
            scratch(2, rows, channels // 2),
            scratch(rows, ho.shape[1] * n_fs),
            scratch(rows + RIM, channels // 2, dtype=bf16),
            scratch(rows + RIM, channels // 2, dtype=bf16),
            scratch(rows + RIM, channels), scratch(RIM, channels // 2, dtype=bf16),
            scratch(2, RIM, channels // 2, dtype=bf16), scratch(rows, channels),
            scratch(2 * rows, 128), scratch(2 * rows, 128),
            dma((slots, 2)), dma((count, 2)), dma((slots, 2)), dma((count, 2)),
            dma((slots, 3)), dma((slots, 3)), dma((slots,)), dma((slots,)), dma((3,)),
            dma((5,)), dma((8,)), dma((spare, 2, 2)), dma((spare, 2)),
            dma((couples,)), dma((couples,)), dma((3,)), dma((3,)), dma((n_fs,)), dma((n_fs,)),
            pltpu.SemaphoreType.REGULAR((1,)),
        ],
        compiler_params=pltpu.CompilerParams(
            collective_id=1, has_side_effects=True, vmem_limit_bytes=40 * 1024 * 1024
        ),
    )(*[
        pltpu.with_memory_space_constraint(a, pltpu.HBM)
        for a in (x, *small, qd, md, ku, vu, qu, cv, cg, ho, co)
    ])


def fused_local(
    tokens, mix_gain, query_down, memory_down, rope_weight, query_up, key_up, value_up,
    latent_gain, memory_gain, query_gain, key_gain, conv_value, conv_gate, conv_kernel,
    channel_gain, channel_shift, heads_out, conv_out,
):
    mine, other = fused_call(
        (lax.axis_size("fs"), lax.axis_size("sp"), lax.axis_size("tp")),
        tokens[0], mix_gain, rope_weight, conv_kernel, channel_gain, channel_shift,
        latent_gain, memory_gain, query_gain, key_gain,
        query_down, memory_down, conv_value, conv_gate,
        query_up, key_up, value_up, heads_out, conv_out,
    )
    return (mine.astype(jnp.float32) + other.astype(jnp.float32)).astype(jnp.bfloat16)[None]


def solution(mesh):
    in_specs = (
        P("fs", "sp", None),
        P(),
        P("fs", "tp"),
        P("fs", "tp"),
        P(),
        P("fs", "tp"),
        P("fs", "tp"),
        P("fs", "tp"),
        P(),
        P(),
        P(),
        P(),
        P("fs", "tp"),
        P("fs", "tp"),
        P(None, "tp"),
        P("tp"),
        P("tp"),
        P("tp", "fs"),
        P("tp", "fs"),
    )
    out_specs = P("fs", "sp", None)
    n_fs, n_sp, n_tp = (mesh.shape[axis] for axis in ("fs", "sp", "tp"))
    fits = n_fs == 4 and n_tp == 2 and n_sp in (2, 4)
    body = fused_local if fits else local
    return jax.shard_map(body, mesh=mesh, in_specs=in_specs, out_specs=out_specs, check_vma=False)
```

```python
import functools

import jax
import jax.numpy as jnp
import numpy as np
from jax import lax
from jax.experimental import pallas as pl
from jax.experimental.pallas import tpu as pltpu
from jax.sharding import PartitionSpec as P

MESH_ID = pl.DeviceIdType.MESH

QK_NOPE = 64
QK_ROPE = 32
V_DIM = 64
CONV_W = 1024
SEG = 64
QK_DIM = 96


epsilon = 1e-06
rope_base = 10000.0
masked_score = -1e30


def norm_rows(matrix, scale_vector):
    return (
        matrix
        * lax.rsqrt(jnp.mean(matrix * matrix, axis=-1, keepdims=True) + epsilon)
        * scale_vector
    )


def rope_tables(positions):
    inverse_freq = 1.0 / rope_base ** (jnp.arange(0, QK_ROPE, 2, dtype=jnp.float32) / QK_ROPE)
    angles = positions.astype(jnp.float32)[:, None] * inverse_freq[None, :]
    return (jnp.cos(angles)[:, None, :], jnp.sin(angles)[:, None, :])


def rotate(matrix, cosine_table, sine_table):
    half_width = matrix.shape[-1] // 2
    front_half = matrix[..., :half_width]
    back_half = matrix[..., half_width:]
    return jnp.concatenate(
        [
            front_half * cosine_table - back_half * sine_table,
            front_half * sine_table + back_half * cosine_table,
        ],
        axis=-1,
    )


def heads_query(latent, weight, scale_vector, cosine_table, sine_table):
    row_count = latent.shape[0]
    projected = jnp.dot(latent, weight, preferred_element_type=jnp.float32)
    projected = norm_rows(
        projected.reshape(row_count, weight.shape[1] // QK_DIM, QK_DIM), scale_vector
    )
    turned = rotate(projected[..., QK_NOPE:], cosine_table, sine_table)
    return jnp.concatenate([projected[..., :QK_NOPE], turned], axis=-1).astype(jnp.bfloat16)


def heads_key(latent, rope_rows, weight, scale_vector, cosine_table, sine_table):
    row_count = latent.shape[0]
    head_count = weight.shape[1] // QK_NOPE
    nope_part = jnp.dot(latent, weight, preferred_element_type=jnp.float32).reshape(
        row_count, head_count, QK_NOPE
    )
    shared = jnp.broadcast_to(
        rope_rows.astype(jnp.float32)[:, None, :], (row_count, head_count, QK_ROPE)
    )
    joined = norm_rows(jnp.concatenate([nope_part, shared], axis=-1), scale_vector)
    turned = rotate(joined[..., QK_NOPE:], cosine_table, sine_table)
    return jnp.concatenate([joined[..., :QK_NOPE], turned], axis=-1).astype(jnp.bfloat16)


RIM = 32


def relayed_rows(rows, paired):
    return (rows * 5 // 16) // 16 * 16 if paired else 0


def gather_kernel(
    sizes,
    x_ref, gain_ref, rope_ref, taps_ref, cgain_ref, cshift_ref,
    qd, md, cv, cg, qu, ku, vu, ho, co,
    lq_all, lm_all, rr_all, conv_ref, qu_all, ku_all, vu_all, ho_all, co_all,
    qd_all, md_all, cv_all, cg_all, normed, acc_q, acc_m, acc_v, acc_g, ext, tail, rim,
    sums, stats, stats_all,
    send_d, recv_d, send_r, recv_r, send_z, recv_z, local_sem, rim_sem,
    sp_send, sp_recv, rr_send, rr_recv, tp_send, tp_recv,
):
    n_fs, n_sp, n_tp = sizes
    paired = n_sp % 2 == 0
    f = lax.axis_index("fs")
    s = lax.axis_index("sp")
    t = lax.axis_index("tp")
    parity = lax.rem(s, 2)
    partner = s + 1 - 2 * parity

    barrier = pltpu.get_barrier_semaphore()
    for axis, at, count in (("fs", f, n_fs), ("sp", s, n_sp), ("tp", t, n_tp)):
        for k in range(1, count):
            pl.semaphore_signal(
                barrier, inc=1, device_id={axis: lax.rem(at + k, count)}, device_id_type=MESH_ID
            )
    pl.semaphore_wait(barrier, n_fs + n_sp + n_tp - 3)

    jobs = [
        (qd, qd_all, 0), (md, md_all, 0), (cv, cv_all, 0), (cg, cg_all, 0),
        (qu, qu_all, 0), (ku, ku_all, 0), (vu, vu_all, 0), (ho, ho_all, 1), (co, co_all, 1),
    ]
    last = len(jobs) - 1
    ahead = 4

    def place(whole, shard, dim, owner, start, count):
        rows, cols = shard.shape
        if dim == 0:
            return whole.at[pl.ds(pl.multiple_of(owner * rows + start, 16), count), :]
        return whole.at[
            pl.ds(pl.multiple_of(start, 16), count),
            pl.ds(pl.multiple_of(owner * cols, 128), cols),
        ]

    square = n_fs == 4
    if square:
        near_x = f + 1 - 2 * lax.rem(f, 2)
        near_y = lax.rem(f + 2, 4)
        far = lax.rem(near_x + 2, 4)
        targets = sources = [near_x, near_y]
    else:
        targets = [lax.rem(f + k, n_fs) for k in range(1, n_fs)]
        sources = [lax.rem(f + n_fs - k, n_fs) for k in range(1, n_fs)]

    direct, far_copies, over_sp, own = [], [], [], []
    for a, (shard, whole, dim) in enumerate(jobs):
        rows = shard.shape[0]
        less = 0 if a == last else relayed_rows(rows, paired)
        start = parity * less
        count = rows - less
        direct.append([
            pltpu.make_async_remote_copy(
                src_ref=shard.at[pl.ds(pl.multiple_of(start, 16), count), :],
                dst_ref=place(whole, shard, dim, f, start, count),
                send_sem=send_d.at[a, k], recv_sem=recv_d.at[a, k],
                device_id={"fs": target}, device_id_type=MESH_ID,
            )
            for k, target in enumerate(targets)
        ])
        halves = []
        if square:
            half = (count // 2 + 15) // 16 * 16
            for k, (owner, target, begin, size) in enumerate((
                (near_y, near_x, start, half), (near_x, near_y, start + half, count - half)
            )):
                piece = place(whole, shard, dim, owner, begin, size)
                halves.append(pltpu.make_async_remote_copy(
                    src_ref=piece, dst_ref=piece,
                    send_sem=send_r.at[a, k], recv_sem=recv_r.at[a, k],
                    device_id={"fs": target}, device_id_type=MESH_ID,
                ))
        far_copies.append(halves)
        across = []
        if less:
            lack = parity * (rows - less)
            for k, owner in enumerate(sources + ([far] if square else [])):
                piece = place(whole, shard, dim, owner, lack, less)
                across.append(pltpu.make_async_remote_copy(
                    src_ref=piece, dst_ref=piece,
                    send_sem=send_z.at[a, k], recv_sem=recv_z.at[a, k],
                    device_id={"sp": partner}, device_id_type=MESH_ID,
                ))
        over_sp.append(across)
        own.append(pltpu.make_async_copy(
            shard, place(whole, shard, dim, f, 0, rows), local_sem.at[a]
        ))

    def begin_array(a):
        if a <= last:
            for copy in direct[a]:
                copy.start()

    def finish_far(a):
        for copy in far_copies[a]:
            copy.wait_recv()
        for copy in over_sp[a][len(sources):]:
            copy.start()

    def tick(a):
        for copy in direct[a]:
            copy.wait_recv()
        for copy in far_copies[a]:
            copy.start()
        begin_array(a + ahead)
        for copy in over_sp[a][: len(sources)]:
            copy.start()
        if a >= 1:
            finish_far(a - 1)

    def complete(a):
        own[a].wait()
        for copy in over_sp[a]:
            copy.wait_recv()

    for a in range(ahead):
        begin_array(a)
    for copy in own:
        copy.start()

    rows = x_ref.shape[0]
    part = 32

    @pl.loop(0, rows // part)
    def _(i):
        at = pl.ds(pl.multiple_of(i * part, part), part)
        x = x_ref[at, :].astype(jnp.float32)
        scale = lax.rsqrt(jnp.mean(x * x, axis=-1, keepdims=True) + epsilon)
        normed[at, :] = (x * scale * gain_ref[...]).astype(jnp.bfloat16)

    depth = qd.shape[0]

    def project(weight, acc):
        acc[...] = jnp.zeros_like(acc)

        @pl.loop(0, n_fs)
        def _(i):
            at = pl.ds(pl.multiple_of(i * depth, depth), depth)
            acc[...] += jnp.dot(
                normed[:, at], weight[at, :], preferred_element_type=jnp.float32
            )

    mine = pl.ds(pl.multiple_of(s * rows, 16), rows)
    rr_all[mine, :] = jnp.dot(
        normed[...], rope_ref[...], preferred_element_type=jnp.float32
    ).astype(jnp.bfloat16)
    tick(0)
    tick(1)
    tick(2)
    complete(0)
    project(qd_all, acc_q)
    lq_all[t, :, :] = acc_q[...].astype(jnp.bfloat16)
    tick(3)
    complete(1)
    project(md_all, acc_m)
    lm_all[t, mine, :] = acc_m[...].astype(jnp.bfloat16)
    tick(4)
    complete(2)
    project(cv_all, acc_v)

    exchanges, passes = [], []
    for k in range(1, n_sp):
        peer = {"sp": lax.rem(s + k, n_sp)}
        exchanges.append(pltpu.make_async_remote_copy(
            src_ref=lm_all.at[t, mine, :], dst_ref=lm_all.at[t, mine, :],
            send_sem=sp_send.at[k - 1], recv_sem=sp_recv.at[k - 1],
            device_id=peer, device_id_type=MESH_ID,
        ))
        exchanges.append(pltpu.make_async_remote_copy(
            src_ref=rr_all.at[mine, :], dst_ref=rr_all.at[mine, :],
            send_sem=rr_send.at[k - 1], recv_sem=rr_recv.at[k - 1],
            device_id=peer, device_id_type=MESH_ID,
        ))
    tp_peers = [{"tp": lax.rem(t + k, n_tp)} for k in range(1, n_tp)]

    def to_tp(kind, source, landing):
        return [
            pltpu.make_async_remote_copy(
                src_ref=source, dst_ref=landing(k),
                send_sem=tp_send.at[kind, k], recv_sem=tp_recv.at[kind, k],
                device_id=peer, device_id_type=MESH_ID,
            )
            for k, peer in enumerate(tp_peers)
        ]

    query_copies = to_tp(0, lq_all.at[t], lambda k: lq_all.at[t])
    memory_copies = to_tp(1, lm_all.at[t], lambda k: lm_all.at[t])
    stat_copies = to_tp(2, stats, lambda k: stats_all.at[k])
    for copy in exchanges + query_copies:
        copy.start()
    tick(5)
    complete(3)
    project(cg_all, acc_g)

    @pl.loop(0, rows // part)
    def _(i):
        at = pl.ds(pl.multiple_of(i * part, part), part)
        gated = (acc_v[at, :] * jax.nn.sigmoid(acc_g[at, :])).astype(jnp.bfloat16)
        ext[pl.ds(pl.multiple_of(RIM + i * part, part), part), :] = gated.astype(jnp.float32)

    tail[...] = ext[pl.ds(rows, RIM), :].astype(jnp.bfloat16)
    rim_copy = pltpu.make_async_remote_copy(
        src_ref=tail, dst_ref=rim, send_sem=rim_sem.at[0], recv_sem=rim_sem.at[1],
        device_id={"sp": lax.rem(s + 1, n_sp)}, device_id_type=MESH_ID,
    )
    tick(6)

    @pl.when(s < n_sp - 1)
    def _():
        rim_copy.start()

    for copy in exchanges:
        copy.wait_recv()
    for copy in memory_copies:
        copy.start()

    @pl.when(s > 0)
    def _():
        rim_copy.wait_recv()
        ext[pl.ds(0, RIM), :] = rim[...].astype(jnp.float32)

    @pl.when(s == 0)
    def _():
        ext[pl.ds(0, RIM), :] = jnp.zeros((RIM, ext.shape[1]), jnp.float32)

    tap_count = taps_ref.shape[0]
    block = 64

    def convolve(c):
        cols = pl.ds(pl.multiple_of(c * 128, 128), 128)
        taps = taps_ref[:, cols].astype(jnp.float32)
        for r in range(0, rows, block):
            total = jnp.zeros((block, 128), jnp.float32)
            for j in range(tap_count):
                total = total + ext[
                    pl.ds(r + RIM - (tap_count - 1) + j, block), cols
                ] * taps[j : j + 1, :]
            sums[pl.ds(r, block), cols] = total

    tiles = ext.shape[1] // 128
    pl.loop(0, tiles // 2)(convolve)
    tick(7)
    pl.loop(tiles // 2, tiles)(convolve)

    @pl.loop(0, rows // part)
    def _(i):
        begin = pl.multiple_of(i * part, part)
        values = sums[pl.ds(begin, part), :]
        stats[pl.ds(begin, part), :] = jnp.broadcast_to(
            jnp.sum(values, axis=1, keepdims=True), (part, 128)
        )
        stats[pl.ds(pl.multiple_of(rows + begin, part), part), :] = jnp.broadcast_to(
            jnp.sum(values * values, axis=1, keepdims=True), (part, 128)
        )

    tick(8)
    for copy in stat_copies:
        copy.start()
    for copy in stat_copies:
        copy.wait_recv()

    channels = ext.shape[1] * n_tp

    @pl.loop(0, rows // part)
    def _(i):
        begin = pl.multiple_of(i * part, part)
        upper = pl.ds(begin, part)
        lower = pl.ds(pl.multiple_of(rows + begin, part), part)
        total, squares = stats[upper, :], stats[lower, :]
        for k in range(n_tp - 1):
            total = total + stats_all[k, upper, :]
            squares = squares + stats_all[k, lower, :]
        mean = total[:, :1] / channels
        spread = squares[:, :1] / channels - mean * mean
        shaped = (sums[upper, :] - mean) * lax.rsqrt(spread + epsilon)
        conv_ref[upper, :] = jax.nn.silu(
            shaped * cgain_ref[...] + cshift_ref[...]
        ).astype(jnp.bfloat16)

    finish_far(last)
    for a in range(4, last + 1):
        complete(a)
    for copy in query_copies + memory_copies:
        copy.wait_recv()
    for group in direct + far_copies + over_sp:
        for copy in group:
            copy.wait_send()
    for copy in exchanges + query_copies + memory_copies + stat_copies:
        copy.wait_send()

    @pl.when(s < n_sp - 1)
    def _():
        rim_copy.wait_send()


def gather_and_project(
    sizes, x, mix_gain, rope_weight, taps, channel_gain, channel_shift,
    qd, md, cv, cg, qu, ku, vu, ho, co,
):
    n_fs, n_sp, n_tp = sizes
    rows = x.shape[0]
    bf16, f32 = jnp.bfloat16, jnp.float32
    vmem = pl.BlockSpec(memory_space=pltpu.VMEM)
    hbm = pl.BlockSpec(memory_space=pl.ANY)

    def whole(w, dim=0):
        return (w.shape[0] * n_fs, w.shape[1]) if dim == 0 else (w.shape[0], w.shape[1] * n_fs)

    out_shapes = [
        ((n_tp, rows, qd.shape[1]), bf16), ((n_tp, n_sp * rows, md.shape[1]), bf16),
        ((n_sp * rows, rope_weight.shape[1]), bf16), ((rows, cv.shape[1]), bf16),
        (whole(qu), bf16), (whole(ku), bf16), (whole(vu), bf16),
        (whole(ho, 1), bf16), (whole(co, 1), bf16),
    ]
    dma = pltpu.SemaphoreType.DMA
    tp_others = max(n_tp - 1, 1)
    sp_others = max(n_sp - 1, 1)
    return pl.pallas_call(
        functools.partial(gather_kernel, sizes),
        out_shape=[jax.ShapeDtypeStruct(*o) for o in out_shapes],
        in_specs=[vmem] * 6 + [hbm] * 9,
        out_specs=[vmem] * 9,
        scratch_shapes=[
            pltpu.VMEM(whole(qd), bf16), pltpu.VMEM(whole(md), bf16),
            pltpu.VMEM(whole(cv), bf16), pltpu.VMEM(whole(cg), bf16),
            pltpu.VMEM(x.shape, bf16), pltpu.VMEM((rows, qd.shape[1]), f32),
            pltpu.VMEM((rows, md.shape[1]), f32),
            pltpu.VMEM((rows, cv.shape[1]), f32), pltpu.VMEM((rows, cv.shape[1]), f32),
            pltpu.VMEM((rows + RIM, cv.shape[1]), f32),
            pltpu.VMEM((RIM, cv.shape[1]), bf16), pltpu.VMEM((RIM, cv.shape[1]), bf16),
            pltpu.VMEM((rows, cv.shape[1]), f32), pltpu.VMEM((2 * rows, 128), f32),
            pltpu.VMEM((tp_others, 2 * rows, 128), f32),
            dma((9, n_fs - 1)), dma((9, n_fs - 1)), dma((9, 2)), dma((9, 2)),
            dma((9, n_fs - 1)), dma((9, n_fs - 1)), dma((9,)), dma((2,)),
            dma((sp_others,)), dma((sp_others,)), dma((sp_others,)), dma((sp_others,)),
            dma((3, tp_others)), dma((3, tp_others)),
        ],
        compiler_params=pltpu.CompilerParams(
            collective_id=0, has_side_effects=True, vmem_limit_bytes=56 * 1024 * 1024
        ),
    )(
        x, mix_gain[None, :], rope_weight, taps, channel_gain[None, :], channel_shift[None, :],
        qd, md, cv, cg, qu, ku, vu, ho, co,
    )


def key_block(key_count):
    block_size = key_count
    while block_size > 2048 and block_size % 2 == 0:
        block_size = block_size // 2
    return block_size


def sum_groups(partial):
    count = lax.axis_size("tp")
    if count != 2:
        return lax.psum(partial, "tp")
    other = lax.ppermute(partial, "tp", [(0, 1), (1, 0)])
    return (partial.astype(jnp.float32) + other.astype(jnp.float32)).astype(jnp.bfloat16)


def local(
    tokens,
    mix_gain,
    query_down,
    memory_down,
    rope_weight,
    query_up,
    key_up,
    value_up,
    latent_gain,
    memory_gain,
    query_gain,
    key_gain,
    conv_value,
    conv_gate,
    conv_kernel,
    channel_gain,
    channel_shift,
    heads_out,
    conv_out,
):
    own_rows = tokens[0]
    (
        query_parts, memory_parts, rope_piece, conv_result,
        up_query, up_keys, up_values, out_heads, out_conv,
    ) = gather_and_project(
        (lax.axis_size("fs"), lax.axis_size("sp"), lax.axis_size("tp")),
        own_rows, mix_gain, rope_weight, conv_kernel, channel_gain, channel_shift,
        query_down, memory_down, conv_value, conv_gate,
        query_up, key_up, value_up, heads_out, conv_out,
    )
    row_count = own_rows.shape[0]
    whole_query = jnp.concatenate(list(query_parts), axis=1)
    whole_memory = jnp.concatenate(list(memory_parts), axis=1)
    query_normed = norm_rows(whole_query.astype(jnp.float32), latent_gain).astype(jnp.bfloat16)
    memory_piece = norm_rows(whole_memory.astype(jnp.float32), memory_gain).astype(jnp.bfloat16)
    positions = lax.axis_index("sp") * row_count + jnp.arange(row_count, dtype=jnp.int32)
    cosine_table, sine_table = rope_tables(positions)
    queries = heads_query(query_normed, up_query, query_gain, cosine_table, sine_table)
    head_count = queries.shape[1]
    query_segment = positions // SEG
    score_scale = QK_DIM ** (-0.5)
    def attend(state_carry, key_rows, value_rows, key_pos):
        running_max, row_total, weighted = state_carry
        scores = (
            jnp.einsum("qhd,khd->qhk", queries, key_rows, preferred_element_type=jnp.float32)
            * score_scale
        )
        allowed = ((key_pos // SEG)[None, :] <= query_segment[:, None])[:, None, :]
        scores = jnp.where(allowed, scores, masked_score)
        new_max = jnp.maximum(running_max, jnp.max(scores, axis=2))
        weights = jnp.where(allowed, jnp.exp(scores - new_max[:, :, None]), 0.0)
        factor = jnp.exp(running_max - new_max)
        row_total = row_total * factor + jnp.sum(weights, axis=2)
        weighted = weighted * factor[:, :, None] + jnp.einsum(
            "qhk,khd->qhd",
            weights.astype(jnp.bfloat16),
            value_rows,
            preferred_element_type=jnp.float32,
        )
        return (new_max, row_total, weighted)

    initial = (
        jnp.full((row_count, head_count), masked_score, jnp.float32),
        jnp.zeros((row_count, head_count), jnp.float32),
        jnp.zeros((row_count, head_count, V_DIM), jnp.float32),
    )
    def block_keys(block_start, block_size):
        memory_block = lax.dynamic_slice_in_dim(memory_piece, block_start, block_size, 0)
        rope_block = lax.dynamic_slice_in_dim(rope_piece, block_start, block_size, 0)
        key_pos = block_start + jnp.arange(block_size, dtype=jnp.int32)
        cosine_keys, sine_keys = rope_tables(key_pos)
        key_rows = heads_key(memory_block, rope_block, up_keys, key_gain, cosine_keys, sine_keys)
        value_rows = (
            jnp.dot(memory_block, up_values, preferred_element_type=jnp.float32)
            .astype(jnp.bfloat16)
            .reshape(block_size, head_count, V_DIM)
        )
        return (key_rows, value_rows, key_pos)

    key_count = memory_piece.shape[0]
    block_size = key_block(key_count)

    def step(block_index, running):
        key_rows, value_rows, key_pos = block_keys(block_index * block_size, block_size)
        return attend(running, key_rows, value_rows, key_pos)

    final_state = lax.fori_loop(0, key_count // block_size, step, initial)
    running_max, row_total, weighted = final_state
    attention = (
        (weighted / row_total[:, :, None])
        .astype(jnp.bfloat16)
        .reshape(row_count, head_count * V_DIM)
    )
    mixer_rows = jnp.concatenate([attention, conv_result], axis=1)
    out_weight = jnp.concatenate([out_heads, out_conv], axis=0)
    partial_sum = jnp.dot(mixer_rows, out_weight, preferred_element_type=jnp.float32)
    mixed = sum_groups(partial_sum.astype(jnp.bfloat16))
    return mixed[None]


def table_rows(count):
    inverse_freq = 1.0 / np.float32(rope_base) ** (
        np.arange(0, QK_ROPE, 2, dtype=np.float32) / np.float32(QK_ROPE)
    )
    angles = inverse_freq[:, None] * np.arange(count, dtype=np.float32)[None, :]
    angles = angles.astype(np.float64)
    return np.cos(angles).astype(np.float32), np.sin(angles).astype(np.float32)


def dot_heads(left, right):
    return lax.dot_general(
        left, right, (((0,), (0,)), ((), ())), preferred_element_type=jnp.float32
    )


def swapped_rows(count, part):
    return (count * part // 16) // 16 * 16


def fused_kernel(
    sizes,
    x_hbm, gain_hbm, rope_hbm, taps_hbm, cgain_hbm, cshift_hbm,
    lgain_hbm, mgain_hbm, qgain_hbm, kgain_hbm, cos_hbm, sin_hbm,
    qd, md, ku, vu, qu, cv, cg, ho, co,
    mine_ref, other_ref,
    gain_ref, rope_ref, taps_ref, cgain_ref, cshift_ref,
    lgain_ref, mgain_ref, qgain_ref, kgain_ref, cos_ref, sin_ref,
    qd_all, md_all, ku_all, vu_all, qu_all, cv_all, cg_all, ho_all, co_all,
    x_all, normed, lq_all, lm_all, mem_all, rr_all, qn_t, q_t, k_t, v_t,
    turned, ropesq, qcol, kcol, bias, scores,
    att_t, att_out, att_all, conv_s, acc_v, acc_out, gate_out, gate_in, ext, rim_out, rim, sums, stats, stats_all,
    send_d, recv_d, send_r, recv_r, send_z, recv_z, local_sem, small_sem, rim_sem, x_sem,
    part_sem, sp_send, sp_recv, fw_send, fw_recv, tp_send, tp_recv, out_send, out_recv, known,
):
    n_fs, n_sp, n_tp = sizes
    f = lax.axis_index("fs")
    s = lax.axis_index("sp")
    t = lax.axis_index("tp")
    parity = lax.rem(s, 2)
    couple = lax.div(s, 2)
    couples = n_sp // 2
    partner = {"sp": s + 1 - 2 * parity}
    twin = {"tp": 1 - t}
    even, odd = parity == 0, parity == 1

    near_x = f + 1 - 2 * lax.rem(f, 2)
    near_y = lax.rem(f + 2, 4)
    far = lax.rem(near_x + 2, 4)
    sources = [near_x, near_y]
    has_below, has_above = s > 0, s < n_sp - 1

    barrier = pltpu.get_barrier_semaphore()

    def greet(device):
        pl.semaphore_signal(barrier, inc=1, device_id=device, device_id_type=MESH_ID)

    for device in (twin, {"fs": near_x}, {"fs": near_y}):
        greet(device)
    pl.when(has_below)(lambda: greet({"sp": s - 1}))
    pl.when(has_above)(lambda: greet({"sp": s + 1}))

    slots = 3
    rows = x_hbm.shape[0]
    x_own = pltpu.make_async_copy(x_hbm, x_all.at[parity], x_sem.at[0])
    x_own.start()
    small = [
        pltpu.make_async_copy(source, landing, small_sem.at[i % slots])
        for i, (source, landing) in enumerate((
            (gain_hbm, gain_ref), (rope_hbm, rope_ref), (taps_hbm, taps_ref),
            (cgain_hbm, cgain_ref), (cshift_hbm, cshift_ref), (lgain_hbm, lgain_ref),
            (mgain_hbm, mgain_ref), (qgain_hbm, qgain_ref), (kgain_hbm, kgain_ref),
            (cos_hbm, cos_ref), (sin_hbm, sin_ref),
        ))
    ]
    for copy in small[:slots]:
        copy.start()

    def remote(source, landing, send, recv, device):
        return pltpu.make_async_remote_copy(
            src_ref=source, dst_ref=landing, send_sem=send, recv_sem=recv,
            device_id=device, device_id_type=MESH_ID,
        )

    share = rows // n_tp
    slab = pl.ds(pl.multiple_of(t * share, 16), share)
    x_send = remote(
        x_hbm.at[slab, :], x_all.at[parity, slab, :], x_sem.at[1], x_sem.at[2], partner
    )
    theirs = x_all.at[1 - parity, slab, :]
    x_forward = remote(theirs, theirs, x_sem.at[3], x_sem.at[4], twin)

    def job(a, shard, whole, swap=None, dim=0, first=0, count=None):
        depth, cols = shard.shape
        count = depth if count is None else count
        lane, mine, lacking, giving = swap or (0, 0, 0, 0)
        lack, give = swapped_rows(count, lacking), swapped_rows(count, giving)
        kept = count - lack

        def place(owner, start, size):
            if dim == 0:
                return whole.at[pl.ds(pl.multiple_of(owner * depth + start, 16), size), :]
            return whole.at[
                pl.ds(pl.multiple_of(start, 16), size),
                pl.ds(pl.multiple_of(owner * cols, 128), cols),
            ]

        start = first + mine * lack
        direct = [
            remote(
                shard.at[pl.ds(start, kept), :], place(f, start, kept),
                send_d.at[a % slots, k], recv_d.at[a, k], {"fs": target},
            )
            for k, target in enumerate(sources)
        ]
        half = (kept // 2 + 15) // 16 * 16
        relays = []
        for k, (owner, target, begin, size) in enumerate((
            (near_y, near_x, start, half), (near_x, near_y, start + half, kept - half)
        )):
            piece = place(owner, begin, size)
            relays.append(remote(
                piece, piece, send_r.at[a % slots, k], recv_r.at[a, k], {"fs": target}
            ))
        gives, lacks = [], []
        if swap:
            for k, owner in enumerate(sources + [far]):
                sems = (send_z.at[lane, k], recv_z.at[lane, k], partner)
                if give:
                    piece = place(owner, first + mine * (count - give), give)
                    gives.append(remote(piece, piece, *sems))
                if lack:
                    piece = place(owner, first + (1 - mine) * kept, lack)
                    lacks.append(remote(piece, piece, *sems))
        own = pltpu.make_async_copy(
            shard.at[pl.ds(first, count), :], place(f, first, count), local_sem.at[a % slots]
        )
        return direct, relays, gives, own, lacks

    def half_columns(shard):
        width = shard.shape[1] // 2
        return shard.at[:, pl.ds(pl.multiple_of(parity * width, 128), width)]

    wide = cv.shape[1] // 2
    side = pl.ds(pl.multiple_of(parity * wide, 128), wide)
    half_rows = ho.shape[0] // 2
    last_rows = half_rows // 4
    first_rows = half_rows * 14 // 8

    def swapping(lane, even_lacks, odd_lacks, *rest):
        shard, whole, *rest = rest
        return [
            (even, shard, whole, (lane, 0, even_lacks, odd_lacks), *rest),
            (odd, shard, whole, (lane, 1, odd_lacks, even_lacks), *rest),
        ]

    plan = [
        [(even, qd, qd_all), (odd, md, md_all)],
        [(None, half_columns(ku), ku_all)], [(None, half_columns(vu), vu_all)],
        swapping(0, 8, 8, ho, ho_all, 1, 0, first_rows),
        [(None, half_columns(qu), qu_all)],
        [(None, half_columns(cv), cv_all)], [(None, half_columns(cg), cg_all)],
        swapping(1, 8, 4, ho, ho_all, 1, first_rows, 2 * half_rows - first_rows),
        swapping(2, 8, 2, co, co_all, 1, 0, half_rows),
        [(None, co, co_all, None, 1, half_rows, half_rows - last_rows)],
        [(None, co, co_all, None, 1, 2 * half_rows - last_rows, last_rows)],
    ]
    jobs = [[(who[0], job(a, *who[1:])) for who in group] for a, group in enumerate(plan)]
    last = len(jobs) - 1
    lanes = [a for a, group in enumerate(plan) if len(group[0]) > 3 and group[0][3]]

    def each(a, action):
        for condition, parts in jobs[a]:
            if condition is None:
                action(parts)
            else:
                pl.when(condition)(functools.partial(action, parts))

    def sent(a, kind):
        def go(parts):
            for copy in parts[kind]:
                copy.wait_send()

        if a >= 0:
            each(a, go)

    def begin_array(a):
        def start(parts):
            for copy in parts[0]:
                copy.start()
            parts[3].start()

        if a <= last:
            sent(a - slots, 0)
            each(a, start)

    def finish_far(a):
        def go(parts):
            with jax.named_scope(f"far_{a}"):
                for copy in parts[1]:
                    copy.wait_recv()
            for copy in parts[2][len(sources):]:
                copy.start()

        each(a, go)

    def swap_near(a):
        def swap(parts):
            for copy in parts[2][: len(sources)]:
                copy.start()

        if a in lanes:
            each(a, swap)

    begins = {0: [3], 1: [4], 2: [5], 3: [6], 5: [7], 6: [8], 7: [9], 8: [10]}

    def tick(a):
        def go(parts):
            with jax.named_scope(f"direct_{a}"):
                for copy in parts[0]:
                    copy.wait_recv()
                parts[3].wait()
            for copy in parts[1]:
                copy.start()

        sent(a - slots, 1)
        each(a, go)
        for later in begins.get(a, ()):
            begin_array(later)
        swap_near(a)

    def complete(a, which=slice(None)):
        def go(parts):
            with jax.named_scope(f"across_{a}"):
                for copy in parts[4][which]:
                    copy.wait_recv()

        each(a, go)

    with jax.named_scope("entry"):
        pl.semaphore_wait(
            barrier, 3 + has_below.astype(jnp.int32) + has_above.astype(jnp.int32)
        )
    x_send.start()
    for a in range(slots):
        begin_array(a)

    @pl.when(jnp.logical_and(has_below, has_above))
    def _():
        pl.semaphore_signal(
            known.at[0], inc=1, device_id={"sp": s - 1}, device_id_type=MESH_ID
        )

    with jax.named_scope("small_wait"):
        for r in range(0, len(small), slots):
            if r:
                for copy in small[r : r + slots]:
                    copy.start()
            for copy in small[r : r + slots]:
                copy.wait()
        x_own.wait()

    part = 32

    def norm_block(b):
        @pl.loop(0, rows // part)
        def _(i):
            at = pl.ds(pl.multiple_of(i * part, part), part)
            x = x_all[b, at, :].astype(jnp.float32)
            scale = lax.rsqrt(jnp.mean(x * x, axis=-1, keepdims=True) + epsilon)
            normed[b, at, :] = (x * scale * gain_ref[...]).astype(jnp.bfloat16)

        rr_all[2 * couple + b] = lax.dot_general(
            rope_ref[...], normed[b], (((1,), (1,)), ((), ())), preferred_element_type=jnp.float32
        ).astype(jnp.bfloat16)

    norm_block(parity)
    half_rope = QK_ROPE // 2

    def column(row_ref, col_ref):
        shape = (QK_DIM, QK_DIM)
        here = lax.broadcasted_iota(jnp.int32, shape, 0) == lax.broadcasted_iota(jnp.int32, shape, 1)
        spread_row = jnp.broadcast_to(row_ref[...], shape)
        picked = jnp.sum(jnp.where(here, spread_row, 0.0), axis=1, keepdims=True)
        col_ref[...] = jnp.broadcast_to(picked, col_ref.shape)

    column(qgain_ref, qcol)
    column(kgain_ref, kcol)

    @pl.loop(2 * couple + 2, n_sp)
    def _(j):
        mem_all[j] = jnp.zeros(mem_all.shape[1:], jnp.bfloat16)
        rr_all[j] = jnp.zeros(rr_all.shape[1:], jnp.bfloat16)

    @pl.loop(0, n_sp)
    def _(j):
        shape = (rows, 2 * rows)
        key_at = j * rows + lax.broadcasted_iota(jnp.int32, shape, 0)
        query_at = 2 * couple * rows + lax.broadcasted_iota(jnp.int32, shape, 1)
        bias[j] = jnp.where(
            lax.div(key_at, SEG) <= lax.div(query_at, SEG), 0.0, masked_score
        )

    tick(0)
    with jax.named_scope("x_wait"):
        x_send.wait_recv()
    x_forward.start()
    tick(1)
    with jax.named_scope("x_forward"):
        x_forward.wait_recv()
    norm_block(1 - parity)
    tick(2)
    finish_far(0)

    @pl.when(s < n_sp - 2)
    def _():
        pl.semaphore_wait(known.at[0], 1)


    def project(weight, b):
        return jnp.dot(normed[b], weight[...], preferred_element_type=jnp.float32)

    lat = md.shape[1]
    lat_q = qd.shape[1]
    held = pl.ds(pl.multiple_of(t * lat, lat), lat)
    query_across = remote(lq_all.at[t], lq_all.at[t], part_sem.at[0], part_sem.at[1], partner)
    query_copy = remote(lq_all.at[t], lq_all.at[t], tp_send.at[0], tp_recv.at[0], twin)
    memory_copy = remote(lm_all.at[t], lm_all.at[t], tp_send.at[1], tp_recv.at[1], twin)
    stat_copy = remote(stats, stats_all, tp_send.at[2], tp_recv.at[2], twin)
    gate_across = remote(gate_out, gate_in, part_sem.at[2], part_sem.at[3], partner)

    complete(0)

    @pl.when(even)
    def _():
        for b in range(2):
            lq_all[t, b] = project(qd_all, b).astype(jnp.bfloat16)
        query_across.start()
        query_copy.start()

    @pl.when(odd)
    def _():
        for b in range(2):
            lm_all[t, b] = project(md_all, b).astype(jnp.bfloat16)
        memory_copy.start()

    tick(3)

    def normed_columns(parts, width, gain_at, put):
        @pl.loop(0, rows // 128)
        def _(i):
            at = pl.ds(pl.multiple_of(i * 128, 128), 128)
            pieces = [parts(g, at).astype(jnp.float32) for g in range(n_tp)]
            total = sum(jnp.sum(p * p, axis=-1, keepdims=True) for p in pieces)
            scale = lax.rsqrt(total / (width * n_tp) + epsilon)
            for g in range(n_tp):
                shaped = (pieces[g] * scale * gain_at(g * width, width)).astype(jnp.bfloat16)
                put(g * width, width, at, shaped.astype(jnp.float32).T.astype(jnp.bfloat16))

    pair = pl.ds(2 * couple, 2)
    both = mem_all.at[pair, held, :]
    back = remote(both, both, part_sem.at[4], part_sem.at[5], partner)
    back_forward = remote(both, both, fw_send.at[couples - 1], fw_recv.at[couples - 1], twin)
    onward, forwards = [], []
    for d in range(1, couples):
        group = []
        later = lax.rem(couple + d, couples)
        for e in range(2):
            target = {"sp": 2 * later + e}
            group.append((
                remote(
                    mem_all.at[pair, held, :], mem_all.at[pair, held, :],
                    sp_send.at[d - 1, e, 0], sp_recv.at[d - 1, 0], target,
                ),
                remote(
                    rr_all.at[pair], rr_all.at[pair],
                    sp_send.at[d - 1, e, 1], sp_recv.at[d - 1, 1], target,
                ),
            ))
        onward.append(group)
        earlier = mem_all.at[pl.ds(2 * lax.rem(couple + couples - d, couples), 2), held, :]
        forwards.append(remote(earlier, earlier, fw_send.at[d - 1], fw_recv.at[d - 1], twin))

    @pl.when(odd)
    def _():
        with jax.named_scope("memory_wait"):
            memory_copy.wait_recv()
        for b in (1, 0):
            def put_memory(begin, width, at, piece, b=b):
                mem_all[2 * couple + b, begin : begin + width, at] = piece

            normed_columns(
                lambda g, at, b=b: lm_all[g, b, at, :], lat,
                lambda begin, width: mgain_ref[:, begin : begin + width], put_memory,
            )
        for d in range(1, couples):
            @pl.when(couple + d < couples)
            def _(d=d):
                for e in range(2):
                    for copy in onward[d - 1][e]:
                        copy.start()
        back.start()

    finish_far(1)
    tick(4)
    finish_far(2)

    @pl.when(even)
    def _():
        with jax.named_scope("back_wait"):
            back.wait_recv()
        back_forward.start()

    tick(5)
    finish_far(3)

    @pl.when(odd)
    def _():
        with jax.named_scope("query_across"):
            query_across.wait_recv()
        query_copy.start()


    @pl.when(even)
    def _():
        with jax.named_scope("back_forward"):
            back_forward.wait_recv()

    def expand(j):
        k_t[j] = dot_heads(ku_all[...], mem_all[j])
        v_t[j] = dot_heads(vu_all[...], mem_all[j]).astype(jnp.bfloat16)
        shared = rr_all[j].astype(jnp.float32)
        ropesq[j] = jnp.sum(shared * shared, axis=0, keepdims=True)
        shared = shared * kcol[QK_NOPE:, :]
        front, back_half = shared[:half_rope], shared[half_rope:]
        at = pl.ds(pl.multiple_of(j * rows, rows), rows)
        cosine, sine = cos_ref[:, at], sin_ref[:, at]
        turned[j] = jnp.concatenate(
            [front * cosine - back_half * sine, front * sine + back_half * cosine], axis=0
        )

    pl.loop(2 * couple, n_sp)(expand)
    for d in range(1, couples):
        @pl.when(couple >= d)
        def _(d=d):
            with jax.named_scope(f"behind_{d}"):
                for copy in onward[d - 1][0]:
                    copy.wait_recv()
            forwards[d - 1].start()
    with jax.named_scope("query_wait"):
        query_copy.wait_recv()
    for b in range(2):
        def put_query(begin, width, at, piece, b=b):
            at = pl.ds(pl.multiple_of(b * rows + at.start, 128), at.size)
            qn_t[begin : begin + width, at] = piece

        normed_columns(
            lambda g, at, b=b: lq_all[g, b, at, :], lat_q,
            lambda begin, width: jnp.concatenate(
                [lgain_ref[r : r + 1, :] for r in range(begin // 128, (begin + width) // 128)],
                axis=1,
            ),
            put_query,
        )
    for d in range(1, couples):
        @pl.when(couple >= d)
        def _(d=d):
            with jax.named_scope(f"forward_{d}"):
                forwards[d - 1].wait_recv()
    pl.loop(0, 2 * couple)(expand)
    tick(6)
    finish_far(4)
    q_t[...] = dot_heads(qu_all[...], qn_t[...])
    heads = qu.shape[1] // 2 // QK_DIM
    here = pl.ds(pl.multiple_of(2 * couple * rows, rows), 2 * rows)
    score_scale = QK_DIM ** (-0.5)

    def head(h):
        q = q_t[pl.ds(pl.multiple_of(h * QK_DIM, QK_DIM), QK_DIM), :]
        q = q * lax.rsqrt(jnp.mean(q * q, axis=0, keepdims=True) + epsilon) * qcol[...]
        front, back_half = q[QK_NOPE : QK_NOPE + half_rope], q[QK_NOPE + half_rope :]
        cosine, sine = cos_ref[:, here], sin_ref[:, here]
        q = jnp.concatenate(
            [
                q[:QK_NOPE],
                front * cosine - back_half * sine,
                front * sine + back_half * cosine,
            ],
            axis=0,
        ).astype(jnp.bfloat16)
        krow = pl.ds(pl.multiple_of(h * QK_NOPE, QK_NOPE), QK_NOPE)
        vrow = pl.ds(pl.multiple_of(h * V_DIM, V_DIM), V_DIM)
        top = jnp.full((1, 2 * rows), masked_score, jnp.float32)
        for j in range(n_sp):
            nope = k_t[j, krow, :]
            scale = lax.rsqrt(
                (jnp.sum(nope * nope, axis=0, keepdims=True) + ropesq[j]) / QK_DIM + epsilon
            )
            key = jnp.concatenate(
                [nope * scale * kcol[:QK_NOPE, :], turned[j] * scale], axis=0
            ).astype(jnp.bfloat16)
            block = dot_heads(key, q) + bias[j]
            scores[j] = block
            top = jnp.maximum(top, jnp.max(block, axis=0, keepdims=True))
        total = jnp.zeros((1, 2 * rows), jnp.float32)
        summed = jnp.zeros((V_DIM, 2 * rows), jnp.float32)
        for j in range(n_sp):
            weight = jnp.exp((scores[j] - top) * score_scale)
            total = total + jnp.sum(weight, axis=0, keepdims=True)
            summed = summed + jnp.dot(
                v_t[j, vrow, :], weight.astype(jnp.bfloat16),
                preferred_element_type=jnp.float32,
            )
        att_t[vrow, :] = summed / total

    pl.loop(0, heads // 2)(head)
    finish_far(5)
    for b in range(2):
        acc_v[b] = project(cv_all, b)
    tick(7)
    pl.loop(heads // 2, heads)(head)
    value_rows = heads * V_DIM
    own_rows = pl.ds(pl.multiple_of(parity * value_rows, value_rows), value_rows)
    their_lanes = pl.ds(pl.multiple_of((1 - parity) * rows, rows), rows)
    own_lanes = pl.ds(pl.multiple_of(parity * rows, rows), rows)
    att_across = remote(
        att_out, att_all.at[own_rows, :], part_sem.at[6], part_sem.at[7], partner
    )
    att_out[...] = att_t[:, their_lanes].astype(jnp.bfloat16)
    att_across.start()
    att_all[own_rows, :] = att_t[:, own_lanes].astype(jnp.bfloat16)
    finish_far(6)
    opposite = pl.ds(pl.multiple_of((1 - parity) * wide, 128), wide)
    body_rows, halo = pl.ds(RIM, rows), pl.ds(0, RIM)

    def gate(b):
        gates = project(cg_all, b)
        return (acc_v[b] * jax.nn.sigmoid(gates)).astype(jnp.bfloat16)

    end = slice(rows - RIM, rows)
    later_rim = remote(
        rim_out, rim.at[parity], rim_sem.at[0], rim_sem.at[1 + parity],
        {"sp": 2 * lax.rem(couple + 1, couples)},
    )
    has_later, has_earlier = couple < couples - 1, jnp.logical_and(even, couple > 0)
    lower = gate(0)

    @pl.when(even)
    def _():
        ext[body_rows, side] = lower.astype(jnp.float32)
        ext[halo, :] = jnp.zeros((RIM, ext.shape[1]), jnp.float32)
        gate_out[halo, :] = lower[end]

    @pl.when(odd)
    def _():
        gate_out[halo, :] = jnp.zeros((RIM, wide), jnp.bfloat16)
        gate_out[body_rows, :] = lower
        gate_across.start()
        ext[halo, side] = lower[end].astype(jnp.float32)

    upper = gate(1)
    rim_out[...] = upper[end]

    @pl.when(has_later)
    def _():
        later_rim.start()

    @pl.when(even)
    def _():
        gate_out[body_rows, :] = upper
        gate_across.start()

    @pl.when(odd)
    def _():
        ext[body_rows, side] = upper.astype(jnp.float32)

    tick(8)

    @pl.when(has_earlier)
    def _():
        with jax.named_scope("rim_wait"):
            for g in range(2):
                remote(
                    rim_out, rim.at[g], rim_sem.at[0], rim_sem.at[1 + g], partner
                ).wait_recv()
        for g in range(2):
            ext[halo, g * wide : (g + 1) * wide] = rim[g].astype(jnp.float32)

    tap_count = taps_ref.shape[0]
    block = 64

    lead = RIM - (tap_count - 1)

    def convolve(c):
        cols = pl.ds(pl.multiple_of(c * 128, 128), 128)
        taps = taps_ref[:, cols].astype(jnp.float32)
        for r in range(0, rows, block):
            total = jnp.zeros((block, 128), jnp.float32)
            for shift in range(8):
                height = block + (8 if shift else 0)
                partial = jnp.zeros((height, 128), jnp.float32)
                for offset in range(shift, RIM + 1, 8):
                    if offset >= lead:
                        tap = taps[offset - lead : offset - lead + 1, :]
                        partial = partial + ext[pl.ds(r + offset - shift, height), cols] * tap
                total = total + partial[shift : shift + block]
            sums[pl.ds(r, block), cols] = total

    tiles = wide // 128
    pl.loop(parity * tiles, (parity + 1) * tiles)(convolve)
    pl.when(odd)(lambda: tick(9))
    with jax.named_scope("gate_wait"):
        gate_across.wait_recv()
    ext[body_rows, opposite] = gate_in[body_rows, :].astype(jnp.float32)

    @pl.when(odd)
    def _():
        ext[halo, opposite] = gate_in[halo, :].astype(jnp.float32)

    pl.loop((1 - parity) * tiles, (2 - parity) * tiles)(convolve)
    finish_far(7)

    @pl.loop(0, rows // part)
    def _(i):
        begin = pl.multiple_of(i * part, part)
        values = sums[pl.ds(begin, part), :]
        stats[pl.ds(begin, part), :] = jnp.broadcast_to(
            jnp.sum(values, axis=1, keepdims=True), (part, 128)
        )
        stats[pl.ds(pl.multiple_of(rows + begin, part), part), :] = jnp.broadcast_to(
            jnp.sum(values * values, axis=1, keepdims=True), (part, 128)
        )

    stat_copy.start()
    pl.when(even)(lambda: tick(9))
    with jax.named_scope("att_wait"):
        att_across.wait_recv()
    att = att_all[...].astype(jnp.float32).T.astype(jnp.bfloat16)
    span = ho.shape[1]

    complete(3)

    @pl.loop(0, n_fs)
    def _(i):
        cols = pl.ds(pl.multiple_of(i * span, span), span)
        acc_out[:, cols] = jnp.dot(
            att[:, :first_rows], ho_all[:first_rows, cols], preferred_element_type=jnp.float32
        )

    finish_far(8)
    with jax.named_scope("stat_wait"):
        stat_copy.wait_recv()
    channels = ext.shape[1] * n_tp

    @pl.loop(0, rows // part)
    def _(i):
        begin = pl.multiple_of(i * part, part)
        upper = pl.ds(begin, part)
        lower = pl.ds(pl.multiple_of(rows + begin, part), part)
        total = stats[upper, :] + stats_all[upper, :]
        squares = stats[lower, :] + stats_all[lower, :]
        mean = total[:, :1] / channels
        spread = squares[:, :1] / channels - mean * mean
        shaped = (sums[upper, :] - mean) * lax.rsqrt(spread + epsilon)
        conv_s[upper, :] = jax.nn.silu(
            shaped * cgain_ref[...] + cshift_ref[...]
        ).astype(jnp.bfloat16)

    tick(10)
    outs = []
    for i, owner in enumerate([f, near_x, near_y, far]):
        cols = pl.ds(pl.multiple_of(owner * span, span), span)
        outs.append(remote(
            mine_ref.at[:, cols], other_ref.at[:, cols], out_send.at[i], out_recv.at[i], twin
        ))
        if i == 1:
            complete(7, slice(0, len(sources)))
            complete(8, slice(0, len(sources)))
        if i == n_fs - 1:
            finish_far(9)
            finish_far(last)
            complete(7, slice(len(sources), None))
            complete(8, slice(len(sources), None))
        mine_ref[:, cols] = (
            acc_out[:, cols]
            + jnp.dot(att[:, first_rows:], ho_all[first_rows:, cols], preferred_element_type=jnp.float32)
            + jnp.dot(conv_s[...], co_all[:, cols], preferred_element_type=jnp.float32)
        ).astype(jnp.bfloat16)
        outs[i].start()

    for a in range(last + 1 - slots, last + 1):
        sent(a, 0)
        sent(a, 1)
    for a in lanes:
        sent(a, 2)
    for copy in (x_send, x_forward, query_copy, stat_copy, gate_across, att_across):
        copy.wait_send()

    @pl.when(even)
    def _():
        query_across.wait_send()
        back_forward.wait_send()

    @pl.when(odd)
    def _():
        memory_copy.wait_send()
        back.wait_send()
        for d in range(1, couples):
            @pl.when(couple + d < couples)
            def _(d=d):
                for e in range(2):
                    for copy in onward[d - 1][e]:
                        copy.wait_send()

    for d in range(1, couples):
        @pl.when(couple >= d)
        def _(d=d):
            forwards[d - 1].wait_send()

    @pl.when(has_later)
    def _():
        later_rim.wait_send()

    with jax.named_scope("out_wait"):
        for copy in outs:
            copy.wait()


def fused_call(
    sizes, x, mix_gain, rope_weight, taps, channel_gain, channel_shift,
    latent_gain, memory_gain, query_gain, key_gain,
    qd, md, cv, cg, qu, ku, vu, ho, co,
):
    n_fs, n_sp, n_tp = sizes
    rows, model = x.shape
    bf16, f32 = jnp.bfloat16, jnp.float32
    hbm = pl.BlockSpec(memory_space=pl.ANY)
    cosine, sine = table_rows(n_sp * rows)
    small = [
        mix_gain[None, :], rope_weight.T, taps, channel_gain[None, :], channel_shift[None, :],
        latent_gain.reshape(-1, 128), memory_gain[None, :], query_gain[None, :],
        key_gain[None, :], jnp.asarray(cosine), jnp.asarray(sine),
    ]

    def whole(w, dim=0, parts=1):
        rows_w, cols_w = w.shape[0], w.shape[1] // parts
        return (rows_w * n_fs, cols_w) if dim == 0 else (rows_w, cols_w * n_fs)

    def scratch(*shape, dtype=f32):
        return pltpu.VMEM(shape, dtype)

    dma = pltpu.SemaphoreType.DMA
    channels, lat = cv.shape[1], md.shape[1] * n_tp
    rope = rope_weight.shape[1]
    couples = n_sp // 2
    spare = max(couples - 1, 1)
    count, slots = 11, 3
    return pl.pallas_call(
        functools.partial(fused_kernel, sizes),
        out_shape=[jax.ShapeDtypeStruct((rows, ho.shape[1] * n_fs), bf16)] * 2,
        in_specs=[hbm] * 21,
        out_specs=[pl.BlockSpec(memory_space=pltpu.VMEM)] * 2,
        scratch_shapes=[scratch(*a.shape, dtype=a.dtype) for a in small] + [
            scratch(*whole(qd), dtype=bf16), scratch(*whole(md), dtype=bf16),
            scratch(*whole(ku, 0, 2), dtype=bf16), scratch(*whole(vu, 0, 2), dtype=bf16),
            scratch(*whole(qu, 0, 2), dtype=bf16), scratch(*whole(cv, 0, 2), dtype=bf16),
            scratch(*whole(cg, 0, 2), dtype=bf16), scratch(*whole(ho, 1), dtype=bf16),
            scratch(*whole(co, 1), dtype=bf16),
            scratch(2, rows, model, dtype=bf16), scratch(2, rows, model, dtype=bf16),
            scratch(n_tp, 2, rows, qd.shape[1], dtype=bf16),
            scratch(n_tp, 2, rows, md.shape[1], dtype=bf16),
            scratch(n_sp, lat, rows, dtype=bf16), scratch(n_sp, rope, rows, dtype=bf16),
            scratch(qu.shape[0] * n_fs, 2 * rows, dtype=bf16), scratch(qu.shape[1] // 2, 2 * rows),
            scratch(n_sp, ku.shape[1] // 2, rows),
            scratch(n_sp, vu.shape[1] // 2, rows, dtype=bf16),
            scratch(n_sp, rope, rows), scratch(n_sp, 1, rows),
            scratch(QK_DIM, 2 * rows), scratch(QK_DIM, rows),
            scratch(n_sp, rows, 2 * rows), scratch(n_sp, rows, 2 * rows),
            scratch(vu.shape[1] // 2, 2 * rows), scratch(vu.shape[1] // 2, rows, dtype=bf16),
            scratch(vu.shape[1], rows, dtype=bf16), scratch(rows, channels, dtype=bf16),
            scratch(2, rows, channels // 2),
            scratch(rows, ho.shape[1] * n_fs),
            scratch(rows + RIM, channels // 2, dtype=bf16),
            scratch(rows + RIM, channels // 2, dtype=bf16),
            scratch(rows + RIM, channels), scratch(RIM, channels // 2, dtype=bf16),
            scratch(2, RIM, channels // 2, dtype=bf16), scratch(rows, channels),
            scratch(2 * rows, 128), scratch(2 * rows, 128),
            dma((slots, 2)), dma((count, 2)), dma((slots, 2)), dma((count, 2)),
            dma((slots, 3)), dma((slots, 3)), dma((slots,)), dma((slots,)), dma((3,)),
            dma((5,)), dma((8,)), dma((spare, 2, 2)), dma((spare, 2)),
            dma((couples,)), dma((couples,)), dma((3,)), dma((3,)), dma((n_fs,)), dma((n_fs,)),
            pltpu.SemaphoreType.REGULAR((1,)),
        ],
        compiler_params=pltpu.CompilerParams(
            collective_id=1, has_side_effects=True, vmem_limit_bytes=40 * 1024 * 1024
        ),
    )(*[
        pltpu.with_memory_space_constraint(a, pltpu.HBM)
        for a in (x, *small, qd, md, ku, vu, qu, cv, cg, ho, co)
    ])


def fused_local(
    tokens, mix_gain, query_down, memory_down, rope_weight, query_up, key_up, value_up,
    latent_gain, memory_gain, query_gain, key_gain, conv_value, conv_gate, conv_kernel,
    channel_gain, channel_shift, heads_out, conv_out,
):
    mine, other = fused_call(
        (lax.axis_size("fs"), lax.axis_size("sp"), lax.axis_size("tp")),
        tokens[0], mix_gain, rope_weight, conv_kernel, channel_gain, channel_shift,
        latent_gain, memory_gain, query_gain, key_gain,
        query_down, memory_down, conv_value, conv_gate,
        query_up, key_up, value_up, heads_out, conv_out,
    )
    return (mine.astype(jnp.float32) + other.astype(jnp.float32)).astype(jnp.bfloat16)[None]


def solution(mesh):
    in_specs = (
        P("fs", "sp", None),
        P(),
        P("fs", "tp"),
        P("fs", "tp"),
        P(),
        P("fs", "tp"),
        P("fs", "tp"),
        P("fs", "tp"),
        P(),
        P(),
        P(),
        P(),
        P("fs", "tp"),
        P("fs", "tp"),
        P(None, "tp"),
        P("tp"),
        P("tp"),
        P("tp", "fs"),
        P("tp", "fs"),
    )
    out_specs = P("fs", "sp", None)
    n_fs, n_sp, n_tp = (mesh.shape[axis] for axis in ("fs", "sp", "tp"))
    fits = n_fs == 4 and n_tp == 2 and n_sp in (2, 4)
    body = fused_local if fits else local
    return jax.shard_map(body, mesh=mesh, in_specs=in_specs, out_specs=out_specs, check_vma=False)
```

```python
import functools

import jax
import jax.numpy as jnp
import numpy as np
from jax import lax
from jax.experimental import pallas as pl
from jax.experimental.pallas import tpu as pltpu
from jax.sharding import PartitionSpec as P

MESH_ID = pl.DeviceIdType.MESH

QK_NOPE = 64
QK_ROPE = 32
V_DIM = 64
CONV_W = 1024
SEG = 64
QK_DIM = 96


epsilon = 1e-06
rope_base = 10000.0
masked_score = -1e30


def norm_rows(matrix, scale_vector):
    return (
        matrix
        * lax.rsqrt(jnp.mean(matrix * matrix, axis=-1, keepdims=True) + epsilon)
        * scale_vector
    )


def rope_tables(positions):
    inverse_freq = 1.0 / rope_base ** (jnp.arange(0, QK_ROPE, 2, dtype=jnp.float32) / QK_ROPE)
    angles = positions.astype(jnp.float32)[:, None] * inverse_freq[None, :]
    return (jnp.cos(angles)[:, None, :], jnp.sin(angles)[:, None, :])


def rotate(matrix, cosine_table, sine_table):
    half_width = matrix.shape[-1] // 2
    front_half = matrix[..., :half_width]
    back_half = matrix[..., half_width:]
    return jnp.concatenate(
        [
            front_half * cosine_table - back_half * sine_table,
            front_half * sine_table + back_half * cosine_table,
        ],
        axis=-1,
    )


def heads_query(latent, weight, scale_vector, cosine_table, sine_table):
    row_count = latent.shape[0]
    projected = jnp.dot(latent, weight, preferred_element_type=jnp.float32)
    projected = norm_rows(
        projected.reshape(row_count, weight.shape[1] // QK_DIM, QK_DIM), scale_vector
    )
    turned = rotate(projected[..., QK_NOPE:], cosine_table, sine_table)
    return jnp.concatenate([projected[..., :QK_NOPE], turned], axis=-1).astype(jnp.bfloat16)


def heads_key(latent, rope_rows, weight, scale_vector, cosine_table, sine_table):
    row_count = latent.shape[0]
    head_count = weight.shape[1] // QK_NOPE
    nope_part = jnp.dot(latent, weight, preferred_element_type=jnp.float32).reshape(
        row_count, head_count, QK_NOPE
    )
    shared = jnp.broadcast_to(
        rope_rows.astype(jnp.float32)[:, None, :], (row_count, head_count, QK_ROPE)
    )
    joined = norm_rows(jnp.concatenate([nope_part, shared], axis=-1), scale_vector)
    turned = rotate(joined[..., QK_NOPE:], cosine_table, sine_table)
    return jnp.concatenate([joined[..., :QK_NOPE], turned], axis=-1).astype(jnp.bfloat16)


RIM = 32


def relayed_rows(rows, paired):
    return (rows * 5 // 16) // 16 * 16 if paired else 0


def gather_kernel(
    sizes,
    x_ref, gain_ref, rope_ref, taps_ref, cgain_ref, cshift_ref,
    qd, md, cv, cg, qu, ku, vu, ho, co,
    lq_all, lm_all, rr_all, conv_ref, qu_all, ku_all, vu_all, ho_all, co_all,
    qd_all, md_all, cv_all, cg_all, normed, acc_q, acc_m, acc_v, acc_g, ext, tail, rim,
    sums, stats, stats_all,
    send_d, recv_d, send_r, recv_r, send_z, recv_z, local_sem, rim_sem,
    sp_send, sp_recv, rr_send, rr_recv, tp_send, tp_recv,
):
    n_fs, n_sp, n_tp = sizes
    paired = n_sp % 2 == 0
    f = lax.axis_index("fs")
    s = lax.axis_index("sp")
    t = lax.axis_index("tp")
    parity = lax.rem(s, 2)
    partner = s + 1 - 2 * parity

    barrier = pltpu.get_barrier_semaphore()
    for axis, at, count in (("fs", f, n_fs), ("sp", s, n_sp), ("tp", t, n_tp)):
        for k in range(1, count):
            pl.semaphore_signal(
                barrier, inc=1, device_id={axis: lax.rem(at + k, count)}, device_id_type=MESH_ID
            )
    pl.semaphore_wait(barrier, n_fs + n_sp + n_tp - 3)

    jobs = [
        (qd, qd_all, 0), (md, md_all, 0), (cv, cv_all, 0), (cg, cg_all, 0),
        (qu, qu_all, 0), (ku, ku_all, 0), (vu, vu_all, 0), (ho, ho_all, 1), (co, co_all, 1),
    ]
    last = len(jobs) - 1
    ahead = 4

    def place(whole, shard, dim, owner, start, count):
        rows, cols = shard.shape
        if dim == 0:
            return whole.at[pl.ds(pl.multiple_of(owner * rows + start, 16), count), :]
        return whole.at[
            pl.ds(pl.multiple_of(start, 16), count),
            pl.ds(pl.multiple_of(owner * cols, 128), cols),
        ]

    square = n_fs == 4
    if square:
        near_x = f + 1 - 2 * lax.rem(f, 2)
        near_y = lax.rem(f + 2, 4)
        far = lax.rem(near_x + 2, 4)
        targets = sources = [near_x, near_y]
    else:
        targets = [lax.rem(f + k, n_fs) for k in range(1, n_fs)]
        sources = [lax.rem(f + n_fs - k, n_fs) for k in range(1, n_fs)]

    direct, far_copies, over_sp, own = [], [], [], []
    for a, (shard, whole, dim) in enumerate(jobs):
        rows = shard.shape[0]
        less = 0 if a == last else relayed_rows(rows, paired)
        start = parity * less
        count = rows - less
        direct.append([
            pltpu.make_async_remote_copy(
                src_ref=shard.at[pl.ds(pl.multiple_of(start, 16), count), :],
                dst_ref=place(whole, shard, dim, f, start, count),
                send_sem=send_d.at[a, k], recv_sem=recv_d.at[a, k],
                device_id={"fs": target}, device_id_type=MESH_ID,
            )
            for k, target in enumerate(targets)
        ])
        halves = []
        if square:
            half = (count // 2 + 15) // 16 * 16
            for k, (owner, target, begin, size) in enumerate((
                (near_y, near_x, start, half), (near_x, near_y, start + half, count - half)
            )):
                piece = place(whole, shard, dim, owner, begin, size)
                halves.append(pltpu.make_async_remote_copy(
                    src_ref=piece, dst_ref=piece,
                    send_sem=send_r.at[a, k], recv_sem=recv_r.at[a, k],
                    device_id={"fs": target}, device_id_type=MESH_ID,
                ))
        far_copies.append(halves)
        across = []
        if less:
            lack = parity * (rows - less)
            for k, owner in enumerate(sources + ([far] if square else [])):
                piece = place(whole, shard, dim, owner, lack, less)
                across.append(pltpu.make_async_remote_copy(
                    src_ref=piece, dst_ref=piece,
                    send_sem=send_z.at[a, k], recv_sem=recv_z.at[a, k],
                    device_id={"sp": partner}, device_id_type=MESH_ID,
                ))
        over_sp.append(across)
        own.append(pltpu.make_async_copy(
            shard, place(whole, shard, dim, f, 0, rows), local_sem.at[a]
        ))

    def begin_array(a):
        if a <= last:
            for copy in direct[a]:
                copy.start()

    def finish_far(a):
        for copy in far_copies[a]:
            copy.wait_recv()
        for copy in over_sp[a][len(sources):]:
            copy.start()

    def tick(a):
        for copy in direct[a]:
            copy.wait_recv()
        for copy in far_copies[a]:
            copy.start()
        begin_array(a + ahead)
        for copy in over_sp[a][: len(sources)]:
            copy.start()
        if a >= 1:
            finish_far(a - 1)

    def complete(a):
        own[a].wait()
        for copy in over_sp[a]:
            copy.wait_recv()

    for a in range(ahead):
        begin_array(a)
    for copy in own:
        copy.start()

    rows = x_ref.shape[0]
    part = 32

    @pl.loop(0, rows // part)
    def _(i):
        at = pl.ds(pl.multiple_of(i * part, part), part)
        x = x_ref[at, :].astype(jnp.float32)
        scale = lax.rsqrt(jnp.mean(x * x, axis=-1, keepdims=True) + epsilon)
        normed[at, :] = (x * scale * gain_ref[...]).astype(jnp.bfloat16)

    depth = qd.shape[0]

    def project(weight, acc):
        acc[...] = jnp.zeros_like(acc)

        @pl.loop(0, n_fs)
        def _(i):
            at = pl.ds(pl.multiple_of(i * depth, depth), depth)
            acc[...] += jnp.dot(
                normed[:, at], weight[at, :], preferred_element_type=jnp.float32
            )

    mine = pl.ds(pl.multiple_of(s * rows, 16), rows)
    rr_all[mine, :] = jnp.dot(
        normed[...], rope_ref[...], preferred_element_type=jnp.float32
    ).astype(jnp.bfloat16)
    tick(0)
    tick(1)
    tick(2)
    complete(0)
    project(qd_all, acc_q)
    lq_all[t, :, :] = acc_q[...].astype(jnp.bfloat16)
    tick(3)
    complete(1)
    project(md_all, acc_m)
    lm_all[t, mine, :] = acc_m[...].astype(jnp.bfloat16)
    tick(4)
    complete(2)
    project(cv_all, acc_v)

    exchanges, passes = [], []
    for k in range(1, n_sp):
        peer = {"sp": lax.rem(s + k, n_sp)}
        exchanges.append(pltpu.make_async_remote_copy(
            src_ref=lm_all.at[t, mine, :], dst_ref=lm_all.at[t, mine, :],
            send_sem=sp_send.at[k - 1], recv_sem=sp_recv.at[k - 1],
            device_id=peer, device_id_type=MESH_ID,
        ))
        exchanges.append(pltpu.make_async_remote_copy(
            src_ref=rr_all.at[mine, :], dst_ref=rr_all.at[mine, :],
            send_sem=rr_send.at[k - 1], recv_sem=rr_recv.at[k - 1],
            device_id=peer, device_id_type=MESH_ID,
        ))
    tp_peers = [{"tp": lax.rem(t + k, n_tp)} for k in range(1, n_tp)]

    def to_tp(kind, source, landing):
        return [
            pltpu.make_async_remote_copy(
                src_ref=source, dst_ref=landing(k),
                send_sem=tp_send.at[kind, k], recv_sem=tp_recv.at[kind, k],
                device_id=peer, device_id_type=MESH_ID,
            )
            for k, peer in enumerate(tp_peers)
        ]

    query_copies = to_tp(0, lq_all.at[t], lambda k: lq_all.at[t])
    memory_copies = to_tp(1, lm_all.at[t], lambda k: lm_all.at[t])
    stat_copies = to_tp(2, stats, lambda k: stats_all.at[k])
    for copy in exchanges + query_copies:
        copy.start()
    tick(5)
    complete(3)
    project(cg_all, acc_g)

    @pl.loop(0, rows // part)
    def _(i):
        at = pl.ds(pl.multiple_of(i * part, part), part)
        gated = (acc_v[at, :] * jax.nn.sigmoid(acc_g[at, :])).astype(jnp.bfloat16)
        ext[pl.ds(pl.multiple_of(RIM + i * part, part), part), :] = gated.astype(jnp.float32)

    tail[...] = ext[pl.ds(rows, RIM), :].astype(jnp.bfloat16)
    rim_copy = pltpu.make_async_remote_copy(
        src_ref=tail, dst_ref=rim, send_sem=rim_sem.at[0], recv_sem=rim_sem.at[1],
        device_id={"sp": lax.rem(s + 1, n_sp)}, device_id_type=MESH_ID,
    )
    tick(6)

    @pl.when(s < n_sp - 1)
    def _():
        rim_copy.start()

    for copy in exchanges:
        copy.wait_recv()
    for copy in memory_copies:
        copy.start()

    @pl.when(s > 0)
    def _():
        rim_copy.wait_recv()
        ext[pl.ds(0, RIM), :] = rim[...].astype(jnp.float32)

    @pl.when(s == 0)
    def _():
        ext[pl.ds(0, RIM), :] = jnp.zeros((RIM, ext.shape[1]), jnp.float32)

    tap_count = taps_ref.shape[0]
    block = 64

    def convolve(c):
        cols = pl.ds(pl.multiple_of(c * 128, 128), 128)
        taps = taps_ref[:, cols].astype(jnp.float32)
        for r in range(0, rows, block):
            total = jnp.zeros((block, 128), jnp.float32)
            for j in range(tap_count):
                total = total + ext[
                    pl.ds(r + RIM - (tap_count - 1) + j, block), cols
                ] * taps[j : j + 1, :]
            sums[pl.ds(r, block), cols] = total

    tiles = ext.shape[1] // 128
    pl.loop(0, tiles // 2)(convolve)
    tick(7)
    pl.loop(tiles // 2, tiles)(convolve)

    @pl.loop(0, rows // part)
    def _(i):
        begin = pl.multiple_of(i * part, part)
        values = sums[pl.ds(begin, part), :]
        stats[pl.ds(begin, part), :] = jnp.broadcast_to(
            jnp.sum(values, axis=1, keepdims=True), (part, 128)
        )
        stats[pl.ds(pl.multiple_of(rows + begin, part), part), :] = jnp.broadcast_to(
            jnp.sum(values * values, axis=1, keepdims=True), (part, 128)
        )

    tick(8)
    for copy in stat_copies:
        copy.start()
    for copy in stat_copies:
        copy.wait_recv()

    channels = ext.shape[1] * n_tp

    @pl.loop(0, rows // part)
    def _(i):
        begin = pl.multiple_of(i * part, part)
        upper = pl.ds(begin, part)
        lower = pl.ds(pl.multiple_of(rows + begin, part), part)
        total, squares = stats[upper, :], stats[lower, :]
        for k in range(n_tp - 1):
            total = total + stats_all[k, upper, :]
            squares = squares + stats_all[k, lower, :]
        mean = total[:, :1] / channels
        spread = squares[:, :1] / channels - mean * mean
        shaped = (sums[upper, :] - mean) * lax.rsqrt(spread + epsilon)
        conv_ref[upper, :] = jax.nn.silu(
            shaped * cgain_ref[...] + cshift_ref[...]
        ).astype(jnp.bfloat16)

    finish_far(last)
    for a in range(4, last + 1):
        complete(a)
    for copy in query_copies + memory_copies:
        copy.wait_recv()
    for group in direct + far_copies + over_sp:
        for copy in group:
            copy.wait_send()
    for copy in exchanges + query_copies + memory_copies + stat_copies:
        copy.wait_send()

    @pl.when(s < n_sp - 1)
    def _():
        rim_copy.wait_send()


def gather_and_project(
    sizes, x, mix_gain, rope_weight, taps, channel_gain, channel_shift,
    qd, md, cv, cg, qu, ku, vu, ho, co,
):
    n_fs, n_sp, n_tp = sizes
    rows = x.shape[0]
    bf16, f32 = jnp.bfloat16, jnp.float32
    vmem = pl.BlockSpec(memory_space=pltpu.VMEM)
    hbm = pl.BlockSpec(memory_space=pl.ANY)

    def whole(w, dim=0):
        return (w.shape[0] * n_fs, w.shape[1]) if dim == 0 else (w.shape[0], w.shape[1] * n_fs)

    out_shapes = [
        ((n_tp, rows, qd.shape[1]), bf16), ((n_tp, n_sp * rows, md.shape[1]), bf16),
        ((n_sp * rows, rope_weight.shape[1]), bf16), ((rows, cv.shape[1]), bf16),
        (whole(qu), bf16), (whole(ku), bf16), (whole(vu), bf16),
        (whole(ho, 1), bf16), (whole(co, 1), bf16),
    ]
    dma = pltpu.SemaphoreType.DMA
    tp_others = max(n_tp - 1, 1)
    sp_others = max(n_sp - 1, 1)
    return pl.pallas_call(
        functools.partial(gather_kernel, sizes),
        out_shape=[jax.ShapeDtypeStruct(*o) for o in out_shapes],
        in_specs=[vmem] * 6 + [hbm] * 9,
        out_specs=[vmem] * 9,
        scratch_shapes=[
            pltpu.VMEM(whole(qd), bf16), pltpu.VMEM(whole(md), bf16),
            pltpu.VMEM(whole(cv), bf16), pltpu.VMEM(whole(cg), bf16),
            pltpu.VMEM(x.shape, bf16), pltpu.VMEM((rows, qd.shape[1]), f32),
            pltpu.VMEM((rows, md.shape[1]), f32),
            pltpu.VMEM((rows, cv.shape[1]), f32), pltpu.VMEM((rows, cv.shape[1]), f32),
            pltpu.VMEM((rows + RIM, cv.shape[1]), f32),
            pltpu.VMEM((RIM, cv.shape[1]), bf16), pltpu.VMEM((RIM, cv.shape[1]), bf16),
            pltpu.VMEM((rows, cv.shape[1]), f32), pltpu.VMEM((2 * rows, 128), f32),
            pltpu.VMEM((tp_others, 2 * rows, 128), f32),
            dma((9, n_fs - 1)), dma((9, n_fs - 1)), dma((9, 2)), dma((9, 2)),
            dma((9, n_fs - 1)), dma((9, n_fs - 1)), dma((9,)), dma((2,)),
            dma((sp_others,)), dma((sp_others,)), dma((sp_others,)), dma((sp_others,)),
            dma((3, tp_others)), dma((3, tp_others)),
        ],
        compiler_params=pltpu.CompilerParams(
            collective_id=0, has_side_effects=True, vmem_limit_bytes=56 * 1024 * 1024
        ),
    )(
        x, mix_gain[None, :], rope_weight, taps, channel_gain[None, :], channel_shift[None, :],
        qd, md, cv, cg, qu, ku, vu, ho, co,
    )


def key_block(key_count):
    block_size = key_count
    while block_size > 2048 and block_size % 2 == 0:
        block_size = block_size // 2
    return block_size


def sum_groups(partial):
    count = lax.axis_size("tp")
    if count != 2:
        return lax.psum(partial, "tp")
    other = lax.ppermute(partial, "tp", [(0, 1), (1, 0)])
    return (partial.astype(jnp.float32) + other.astype(jnp.float32)).astype(jnp.bfloat16)


def local(
    tokens,
    mix_gain,
    query_down,
    memory_down,
    rope_weight,
    query_up,
    key_up,
    value_up,
    latent_gain,
    memory_gain,
    query_gain,
    key_gain,
    conv_value,
    conv_gate,
    conv_kernel,
    channel_gain,
    channel_shift,
    heads_out,
    conv_out,
):
    own_rows = tokens[0]
    (
        query_parts, memory_parts, rope_piece, conv_result,
        up_query, up_keys, up_values, out_heads, out_conv,
    ) = gather_and_project(
        (lax.axis_size("fs"), lax.axis_size("sp"), lax.axis_size("tp")),
        own_rows, mix_gain, rope_weight, conv_kernel, channel_gain, channel_shift,
        query_down, memory_down, conv_value, conv_gate,
        query_up, key_up, value_up, heads_out, conv_out,
    )
    row_count = own_rows.shape[0]
    whole_query = jnp.concatenate(list(query_parts), axis=1)
    whole_memory = jnp.concatenate(list(memory_parts), axis=1)
    query_normed = norm_rows(whole_query.astype(jnp.float32), latent_gain).astype(jnp.bfloat16)
    memory_piece = norm_rows(whole_memory.astype(jnp.float32), memory_gain).astype(jnp.bfloat16)
    positions = lax.axis_index("sp") * row_count + jnp.arange(row_count, dtype=jnp.int32)
    cosine_table, sine_table = rope_tables(positions)
    queries = heads_query(query_normed, up_query, query_gain, cosine_table, sine_table)
    head_count = queries.shape[1]
    query_segment = positions // SEG
    score_scale = QK_DIM ** (-0.5)
    def attend(state_carry, key_rows, value_rows, key_pos):
        running_max, row_total, weighted = state_carry
        scores = (
            jnp.einsum("qhd,khd->qhk", queries, key_rows, preferred_element_type=jnp.float32)
            * score_scale
        )
        allowed = ((key_pos // SEG)[None, :] <= query_segment[:, None])[:, None, :]
        scores = jnp.where(allowed, scores, masked_score)
        new_max = jnp.maximum(running_max, jnp.max(scores, axis=2))
        weights = jnp.where(allowed, jnp.exp(scores - new_max[:, :, None]), 0.0)
        factor = jnp.exp(running_max - new_max)
        row_total = row_total * factor + jnp.sum(weights, axis=2)
        weighted = weighted * factor[:, :, None] + jnp.einsum(
            "qhk,khd->qhd",
            weights.astype(jnp.bfloat16),
            value_rows,
            preferred_element_type=jnp.float32,
        )
        return (new_max, row_total, weighted)

    initial = (
        jnp.full((row_count, head_count), masked_score, jnp.float32),
        jnp.zeros((row_count, head_count), jnp.float32),
        jnp.zeros((row_count, head_count, V_DIM), jnp.float32),
    )
    def block_keys(block_start, block_size):
        memory_block = lax.dynamic_slice_in_dim(memory_piece, block_start, block_size, 0)
        rope_block = lax.dynamic_slice_in_dim(rope_piece, block_start, block_size, 0)
        key_pos = block_start + jnp.arange(block_size, dtype=jnp.int32)
        cosine_keys, sine_keys = rope_tables(key_pos)
        key_rows = heads_key(memory_block, rope_block, up_keys, key_gain, cosine_keys, sine_keys)
        value_rows = (
            jnp.dot(memory_block, up_values, preferred_element_type=jnp.float32)
            .astype(jnp.bfloat16)
            .reshape(block_size, head_count, V_DIM)
        )
        return (key_rows, value_rows, key_pos)

    key_count = memory_piece.shape[0]
    block_size = key_block(key_count)

    def step(block_index, running):
        key_rows, value_rows, key_pos = block_keys(block_index * block_size, block_size)
        return attend(running, key_rows, value_rows, key_pos)

    final_state = lax.fori_loop(0, key_count // block_size, step, initial)
    running_max, row_total, weighted = final_state
    attention = (
        (weighted / row_total[:, :, None])
        .astype(jnp.bfloat16)
        .reshape(row_count, head_count * V_DIM)
    )
    mixer_rows = jnp.concatenate([attention, conv_result], axis=1)
    out_weight = jnp.concatenate([out_heads, out_conv], axis=0)
    partial_sum = jnp.dot(mixer_rows, out_weight, preferred_element_type=jnp.float32)
    mixed = sum_groups(partial_sum.astype(jnp.bfloat16))
    return mixed[None]


def table_rows(count):
    inverse_freq = 1.0 / np.float32(rope_base) ** (
        np.arange(0, QK_ROPE, 2, dtype=np.float32) / np.float32(QK_ROPE)
    )
    angles = inverse_freq[:, None] * np.arange(count, dtype=np.float32)[None, :]
    angles = angles.astype(np.float64)
    return np.cos(angles).astype(np.float32), np.sin(angles).astype(np.float32)


def dot_heads(left, right):
    return lax.dot_general(
        left, right, (((0,), (0,)), ((), ())), preferred_element_type=jnp.float32
    )


def swapped_rows(count, part):
    return (count * part // 16) // 16 * 16


def fused_kernel(
    sizes,
    x_hbm, gain_hbm, rope_hbm, taps_hbm, cgain_hbm, cshift_hbm,
    lgain_hbm, mgain_hbm, qgain_hbm, kgain_hbm, cos_hbm, sin_hbm,
    qd, md, ku, vu, qu, cv, cg, ho, co,
    mine_ref, other_ref,
    gain_ref, rope_ref, taps_ref, cgain_ref, cshift_ref,
    lgain_ref, mgain_ref, qgain_ref, kgain_ref, cos_ref, sin_ref,
    qd_all, md_all, ku_all, vu_all, qu_all, cv_all, cg_all, ho_all, co_all,
    x_all, normed, lq_all, lm_all, mem_all, rr_all, qn_t, q_t, k_t, v_t,
    turned, ropesq, qcol, kcol, bias, scores,
    att_t, att_out, att_all, conv_s, acc_v, acc_out, gate_out, gate_in, ext, rim_out, rim, sums, stats, stats_all,
    send_d, recv_d, send_r, recv_r, send_z, recv_z, local_sem, small_sem, rim_sem, x_sem,
    part_sem, sp_send, sp_recv, fw_send, fw_recv, tp_send, tp_recv, out_send, out_recv, known,
):
    n_fs, n_sp, n_tp = sizes
    f = lax.axis_index("fs")
    s = lax.axis_index("sp")
    t = lax.axis_index("tp")
    parity = lax.rem(s, 2)
    couple = lax.div(s, 2)
    couples = n_sp // 2
    partner = {"sp": s + 1 - 2 * parity}
    twin = {"tp": 1 - t}
    even, odd = parity == 0, parity == 1

    near_x = f + 1 - 2 * lax.rem(f, 2)
    near_y = lax.rem(f + 2, 4)
    far = lax.rem(near_x + 2, 4)
    sources = [near_x, near_y]
    has_below, has_above = s > 0, s < n_sp - 1

    barrier = pltpu.get_barrier_semaphore()

    def greet(device):
        pl.semaphore_signal(barrier, inc=1, device_id=device, device_id_type=MESH_ID)

    for device in (twin, {"fs": near_x}, {"fs": near_y}):
        greet(device)
    pl.when(has_below)(lambda: greet({"sp": s - 1}))
    pl.when(has_above)(lambda: greet({"sp": s + 1}))

    slots = 3
    rows = x_hbm.shape[0]
    x_own = pltpu.make_async_copy(x_hbm, x_all.at[parity], x_sem.at[0])
    x_own.start()
    small = [
        pltpu.make_async_copy(source, landing, small_sem.at[i % slots])
        for i, (source, landing) in enumerate((
            (gain_hbm, gain_ref), (rope_hbm, rope_ref), (taps_hbm, taps_ref),
            (cgain_hbm, cgain_ref), (cshift_hbm, cshift_ref), (lgain_hbm, lgain_ref),
            (mgain_hbm, mgain_ref), (qgain_hbm, qgain_ref), (kgain_hbm, kgain_ref),
            (cos_hbm, cos_ref), (sin_hbm, sin_ref),
        ))
    ]
    for copy in small[:slots]:
        copy.start()

    def remote(source, landing, send, recv, device):
        return pltpu.make_async_remote_copy(
            src_ref=source, dst_ref=landing, send_sem=send, recv_sem=recv,
            device_id=device, device_id_type=MESH_ID,
        )

    share = rows // n_tp
    slab = pl.ds(pl.multiple_of(t * share, 16), share)
    x_send = remote(
        x_hbm.at[slab, :], x_all.at[parity, slab, :], x_sem.at[1], x_sem.at[2], partner
    )
    theirs = x_all.at[1 - parity, slab, :]
    x_forward = remote(theirs, theirs, x_sem.at[3], x_sem.at[4], twin)

    def job(a, shard, whole, swap=None, dim=0, first=0, count=None):
        depth, cols = shard.shape
        count = depth if count is None else count
        lane, mine, lacking, giving = swap or (0, 0, 0, 0)
        lack, give = swapped_rows(count, lacking), swapped_rows(count, giving)
        kept = count - lack

        def place(owner, start, size):
            if dim == 0:
                return whole.at[pl.ds(pl.multiple_of(owner * depth + start, 16), size), :]
            return whole.at[
                pl.ds(pl.multiple_of(start, 16), size),
                pl.ds(pl.multiple_of(owner * cols, 128), cols),
            ]

        start = first + mine * lack
        direct = [
            remote(
                shard.at[pl.ds(start, kept), :], place(f, start, kept),
                send_d.at[a % slots, k], recv_d.at[a, k], {"fs": target},
            )
            for k, target in enumerate(sources)
        ]
        half = (kept // 2 + 15) // 16 * 16
        relays = []
        for k, (owner, target, begin, size) in enumerate((
            (near_y, near_x, start, half), (near_x, near_y, start + half, kept - half)
        )):
            piece = place(owner, begin, size)
            relays.append(remote(
                piece, piece, send_r.at[a % slots, k], recv_r.at[a, k], {"fs": target}
            ))
        gives, lacks = [], []
        if swap:
            for k, owner in enumerate(sources + [far]):
                sems = (send_z.at[lane, k], recv_z.at[lane, k], partner)
                if give:
                    piece = place(owner, first + mine * (count - give), give)
                    gives.append(remote(piece, piece, *sems))
                if lack:
                    piece = place(owner, first + (1 - mine) * kept, lack)
                    lacks.append(remote(piece, piece, *sems))
        own = pltpu.make_async_copy(
            shard.at[pl.ds(first, count), :], place(f, first, count), local_sem.at[a % slots]
        )
        return direct, relays, gives, own, lacks

    def half_columns(shard):
        width = shard.shape[1] // 2
        return shard.at[:, pl.ds(pl.multiple_of(parity * width, 128), width)]

    wide = cv.shape[1] // 2
    side = pl.ds(pl.multiple_of(parity * wide, 128), wide)
    half_rows = ho.shape[0] // 2
    last_rows = half_rows // 4
    first_rows = half_rows * 14 // 8

    def swapping(lane, even_lacks, odd_lacks, *rest):
        shard, whole, *rest = rest
        return [
            (even, shard, whole, (lane, 0, even_lacks, odd_lacks), *rest),
            (odd, shard, whole, (lane, 1, odd_lacks, even_lacks), *rest),
        ]

    plan = [
        [(even, qd, qd_all), (odd, md, md_all)],
        [(None, half_columns(ku), ku_all)], [(None, half_columns(vu), vu_all)],
        swapping(0, 8, 8, ho, ho_all, 1, 0, first_rows),
        [(None, half_columns(qu), qu_all)],
        [(None, half_columns(cv), cv_all)], [(None, half_columns(cg), cg_all)],
        swapping(1, 8, 4, ho, ho_all, 1, first_rows, 2 * half_rows - first_rows),
        swapping(2, 8, 2, co, co_all, 1, 0, half_rows),
        [(None, co, co_all, None, 1, half_rows, half_rows - last_rows)],
        [(None, co, co_all, None, 1, 2 * half_rows - last_rows, last_rows)],
    ]
    jobs = [[(who[0], job(a, *who[1:])) for who in group] for a, group in enumerate(plan)]
    last = len(jobs) - 1
    lanes = [a for a, group in enumerate(plan) if len(group[0]) > 3 and group[0][3]]

    def each(a, action):
        for condition, parts in jobs[a]:
            if condition is None:
                action(parts)
            else:
                pl.when(condition)(functools.partial(action, parts))

    def sent(a, kind):
        def go(parts):
            for copy in parts[kind]:
                copy.wait_send()

        if a >= 0:
            each(a, go)

    def begin_array(a):
        def start(parts):
            for copy in parts[0]:
                copy.start()
            parts[3].start()

        if a <= last:
            sent(a - slots, 0)
            each(a, start)

    def finish_far(a):
        def go(parts):
            with jax.named_scope(f"far_{a}"):
                for copy in parts[1]:
                    copy.wait_recv()
            for copy in parts[2][len(sources):]:
                copy.start()

        each(a, go)

    def swap_near(a):
        def swap(parts):
            for copy in parts[2][: len(sources)]:
                copy.start()

        if a in lanes:
            each(a, swap)

    begins = {0: [3], 1: [4], 2: [5], 3: [6], 5: [7], 6: [8], 7: [9], 8: [10]}

    def tick(a):
        def go(parts):
            with jax.named_scope(f"direct_{a}"):
                for copy in parts[0]:
                    copy.wait_recv()
                parts[3].wait()
            for copy in parts[1]:
                copy.start()

        sent(a - slots, 1)
        each(a, go)
        for later in begins.get(a, ()):
            begin_array(later)
        swap_near(a)

    def complete(a, which=slice(None)):
        def go(parts):
            with jax.named_scope(f"across_{a}"):
                for copy in parts[4][which]:
                    copy.wait_recv()

        each(a, go)

    with jax.named_scope("entry"):
        pl.semaphore_wait(
            barrier, 3 + has_below.astype(jnp.int32) + has_above.astype(jnp.int32)
        )
    x_send.start()
    for a in range(slots):
        begin_array(a)

    @pl.when(jnp.logical_and(has_below, has_above))
    def _():
        pl.semaphore_signal(
            known.at[0], inc=1, device_id={"sp": s - 1}, device_id_type=MESH_ID
        )

    with jax.named_scope("small_wait"):
        for r in range(0, len(small), slots):
            if r:
                for copy in small[r : r + slots]:
                    copy.start()
            for copy in small[r : r + slots]:
                copy.wait()
        x_own.wait()

    part = 32

    def norm_block(b):
        @pl.loop(0, rows // part)
        def _(i):
            at = pl.ds(pl.multiple_of(i * part, part), part)
            x = x_all[b, at, :].astype(jnp.float32)
            scale = lax.rsqrt(jnp.mean(x * x, axis=-1, keepdims=True) + epsilon)
            normed[b, at, :] = (x * scale * gain_ref[...]).astype(jnp.bfloat16)

        rr_all[2 * couple + b] = lax.dot_general(
            rope_ref[...], normed[b], (((1,), (1,)), ((), ())), preferred_element_type=jnp.float32
        ).astype(jnp.bfloat16)

    norm_block(parity)
    half_rope = QK_ROPE // 2

    def column(row_ref, col_ref):
        shape = (QK_DIM, QK_DIM)
        here = lax.broadcasted_iota(jnp.int32, shape, 0) == lax.broadcasted_iota(jnp.int32, shape, 1)
        spread_row = jnp.broadcast_to(row_ref[...], shape)
        picked = jnp.sum(jnp.where(here, spread_row, 0.0), axis=1, keepdims=True)
        col_ref[...] = jnp.broadcast_to(picked, col_ref.shape)

    column(qgain_ref, qcol)
    column(kgain_ref, kcol)

    @pl.loop(2 * couple + 2, n_sp)
    def _(j):
        mem_all[j] = jnp.zeros(mem_all.shape[1:], jnp.bfloat16)
        rr_all[j] = jnp.zeros(rr_all.shape[1:], jnp.bfloat16)

    @pl.loop(0, n_sp)
    def _(j):
        shape = (rows, 2 * rows)
        key_at = j * rows + lax.broadcasted_iota(jnp.int32, shape, 0)
        query_at = 2 * couple * rows + lax.broadcasted_iota(jnp.int32, shape, 1)
        bias[j] = jnp.where(
            lax.div(key_at, SEG) <= lax.div(query_at, SEG), 0.0, masked_score
        )

    tick(0)
    with jax.named_scope("x_wait"):
        x_send.wait_recv()
    x_forward.start()
    tick(1)
    with jax.named_scope("x_forward"):
        x_forward.wait_recv()
    norm_block(1 - parity)
    tick(2)
    finish_far(0)

    @pl.when(s < n_sp - 2)
    def _():
        pl.semaphore_wait(known.at[0], 1)


    def project(weight, b):
        return jnp.dot(normed[b], weight[...], preferred_element_type=jnp.float32)

    lat = md.shape[1]
    lat_q = qd.shape[1]
    held = pl.ds(pl.multiple_of(t * lat, lat), lat)
    query_across = remote(lq_all.at[t], lq_all.at[t], part_sem.at[0], part_sem.at[1], partner)
    query_copy = remote(lq_all.at[t], lq_all.at[t], tp_send.at[0], tp_recv.at[0], twin)
    memory_copy = remote(lm_all.at[t], lm_all.at[t], tp_send.at[1], tp_recv.at[1], twin)
    stat_copy = remote(stats, stats_all, tp_send.at[2], tp_recv.at[2], twin)
    gate_across = remote(gate_out, gate_in, part_sem.at[2], part_sem.at[3], partner)

    complete(0)

    @pl.when(even)
    def _():
        for b in range(2):
            lq_all[t, b] = project(qd_all, b).astype(jnp.bfloat16)
        query_across.start()
        query_copy.start()

    @pl.when(odd)
    def _():
        for b in range(2):
            lm_all[t, b] = project(md_all, b).astype(jnp.bfloat16)
        memory_copy.start()

    tick(3)

    def normed_columns(parts, width, gain_at, put):
        @pl.loop(0, rows // 128)
        def _(i):
            at = pl.ds(pl.multiple_of(i * 128, 128), 128)
            pieces = [parts(g, at).astype(jnp.float32) for g in range(n_tp)]
            total = sum(jnp.sum(p * p, axis=-1, keepdims=True) for p in pieces)
            scale = lax.rsqrt(total / (width * n_tp) + epsilon)
            for g in range(n_tp):
                shaped = (pieces[g] * scale * gain_at(g * width, width)).astype(jnp.bfloat16)
                put(g * width, width, at, shaped.astype(jnp.float32).T.astype(jnp.bfloat16))

    pair = pl.ds(2 * couple, 2)
    both = mem_all.at[pair, held, :]
    back = remote(both, both, part_sem.at[4], part_sem.at[5], partner)
    back_forward = remote(both, both, fw_send.at[couples - 1], fw_recv.at[couples - 1], twin)
    onward, forwards = [], []
    for d in range(1, couples):
        group = []
        later = lax.rem(couple + d, couples)
        for e in range(2):
            target = {"sp": 2 * later + e}
            group.append((
                remote(
                    mem_all.at[pair, held, :], mem_all.at[pair, held, :],
                    sp_send.at[d - 1, e, 0], sp_recv.at[d - 1, 0], target,
                ),
                remote(
                    rr_all.at[pair], rr_all.at[pair],
                    sp_send.at[d - 1, e, 1], sp_recv.at[d - 1, 1], target,
                ),
            ))
        onward.append(group)
        earlier = mem_all.at[pl.ds(2 * lax.rem(couple + couples - d, couples), 2), held, :]
        forwards.append(remote(earlier, earlier, fw_send.at[d - 1], fw_recv.at[d - 1], twin))

    @pl.when(odd)
    def _():
        with jax.named_scope("memory_wait"):
            memory_copy.wait_recv()
        for b in (1, 0):
            def put_memory(begin, width, at, piece, b=b):
                mem_all[2 * couple + b, begin : begin + width, at] = piece

            normed_columns(
                lambda g, at, b=b: lm_all[g, b, at, :], lat,
                lambda begin, width: mgain_ref[:, begin : begin + width], put_memory,
            )
        for d in range(1, couples):
            @pl.when(couple + d < couples)
            def _(d=d):
                for e in range(2):
                    for copy in onward[d - 1][e]:
                        copy.start()
        back.start()

    finish_far(1)
    tick(4)
    finish_far(2)

    @pl.when(even)
    def _():
        with jax.named_scope("back_wait"):
            back.wait_recv()
        back_forward.start()

    tick(5)
    finish_far(3)

    @pl.when(odd)
    def _():
        with jax.named_scope("query_across"):
            query_across.wait_recv()
        query_copy.start()


    @pl.when(even)
    def _():
        with jax.named_scope("back_forward"):
            back_forward.wait_recv()

    def expand(j):
        k_t[j] = dot_heads(ku_all[...], mem_all[j])
        v_t[j] = dot_heads(vu_all[...], mem_all[j]).astype(jnp.bfloat16)
        shared = rr_all[j].astype(jnp.float32)
        ropesq[j] = jnp.sum(shared * shared, axis=0, keepdims=True)
        shared = shared * kcol[QK_NOPE:, :]
        front, back_half = shared[:half_rope], shared[half_rope:]
        at = pl.ds(pl.multiple_of(j * rows, rows), rows)
        cosine, sine = cos_ref[:, at], sin_ref[:, at]
        turned[j] = jnp.concatenate(
            [front * cosine - back_half * sine, front * sine + back_half * cosine], axis=0
        )

    pl.loop(2 * couple, n_sp)(expand)
    for d in range(1, couples):
        @pl.when(couple >= d)
        def _(d=d):
            with jax.named_scope(f"behind_{d}"):
                for copy in onward[d - 1][0]:
                    copy.wait_recv()
            forwards[d - 1].start()
    with jax.named_scope("query_wait"):
        query_copy.wait_recv()
    for b in range(2):
        def put_query(begin, width, at, piece, b=b):
            at = pl.ds(pl.multiple_of(b * rows + at.start, 128), at.size)
            qn_t[begin : begin + width, at] = piece

        normed_columns(
            lambda g, at, b=b: lq_all[g, b, at, :], lat_q,
            lambda begin, width: jnp.concatenate(
                [lgain_ref[r : r + 1, :] for r in range(begin // 128, (begin + width) // 128)],
                axis=1,
            ),
            put_query,
        )
    for d in range(1, couples):
        @pl.when(couple >= d)
        def _(d=d):
            with jax.named_scope(f"forward_{d}"):
                forwards[d - 1].wait_recv()
    pl.loop(0, 2 * couple)(expand)
    tick(6)
    finish_far(4)
    q_t[...] = dot_heads(qu_all[...], qn_t[...])
    heads = qu.shape[1] // 2 // QK_DIM
    here = pl.ds(pl.multiple_of(2 * couple * rows, rows), 2 * rows)
    score_scale = QK_DIM ** (-0.5)

    def head(h):
        q = q_t[pl.ds(pl.multiple_of(h * QK_DIM, QK_DIM), QK_DIM), :]
        q = q * lax.rsqrt(jnp.mean(q * q, axis=0, keepdims=True) + epsilon) * qcol[...]
        front, back_half = q[QK_NOPE : QK_NOPE + half_rope], q[QK_NOPE + half_rope :]
        cosine, sine = cos_ref[:, here], sin_ref[:, here]
        q = jnp.concatenate(
            [
                q[:QK_NOPE],
                front * cosine - back_half * sine,
                front * sine + back_half * cosine,
            ],
            axis=0,
        ).astype(jnp.bfloat16)
        krow = pl.ds(pl.multiple_of(h * QK_NOPE, QK_NOPE), QK_NOPE)
        vrow = pl.ds(pl.multiple_of(h * V_DIM, V_DIM), V_DIM)
        top = jnp.full((1, 2 * rows), masked_score, jnp.float32)
        for j in range(n_sp):
            nope = k_t[j, krow, :]
            scale = lax.rsqrt(
                (jnp.sum(nope * nope, axis=0, keepdims=True) + ropesq[j]) / QK_DIM + epsilon
            )
            key = jnp.concatenate(
                [nope * scale * kcol[:QK_NOPE, :], turned[j] * scale], axis=0
            ).astype(jnp.bfloat16)
            block = dot_heads(key, q) + bias[j]
            scores[j] = block
            top = jnp.maximum(top, jnp.max(block, axis=0, keepdims=True))
        total = jnp.zeros((1, 2 * rows), jnp.float32)
        summed = jnp.zeros((V_DIM, 2 * rows), jnp.float32)
        for j in range(n_sp):
            weight = jnp.exp((scores[j] - top) * score_scale)
            total = total + jnp.sum(weight, axis=0, keepdims=True)
            summed = summed + jnp.dot(
                v_t[j, vrow, :], weight.astype(jnp.bfloat16),
                preferred_element_type=jnp.float32,
            )
        att_t[vrow, :] = summed / total

    pl.loop(0, heads // 2)(head)
    finish_far(5)
    for b in range(2):
        acc_v[b] = project(cv_all, b)
    tick(7)
    pl.loop(heads // 2, heads)(head)
    value_rows = heads * V_DIM
    own_rows = pl.ds(pl.multiple_of(parity * value_rows, value_rows), value_rows)
    their_lanes = pl.ds(pl.multiple_of((1 - parity) * rows, rows), rows)
    own_lanes = pl.ds(pl.multiple_of(parity * rows, rows), rows)
    att_across = remote(
        att_out, att_all.at[own_rows, :], part_sem.at[6], part_sem.at[7], partner
    )
    att_out[...] = att_t[:, their_lanes].astype(jnp.bfloat16)
    att_across.start()
    att_all[own_rows, :] = att_t[:, own_lanes].astype(jnp.bfloat16)
    finish_far(6)
    opposite = pl.ds(pl.multiple_of((1 - parity) * wide, 128), wide)
    body_rows, halo = pl.ds(RIM, rows), pl.ds(0, RIM)

    def gate(b):
        gates = project(cg_all, b)
        return (acc_v[b] * jax.nn.sigmoid(gates)).astype(jnp.bfloat16)

    end = slice(rows - RIM, rows)
    later_rim = remote(
        rim_out, rim.at[parity], rim_sem.at[0], rim_sem.at[1 + parity],
        {"sp": 2 * lax.rem(couple + 1, couples)},
    )
    has_later, has_earlier = couple < couples - 1, jnp.logical_and(even, couple > 0)
    lower = gate(0)

    @pl.when(even)
    def _():
        ext[body_rows, side] = lower.astype(jnp.float32)
        ext[halo, :] = jnp.zeros((RIM, ext.shape[1]), jnp.float32)
        gate_out[halo, :] = lower[end]

    @pl.when(odd)
    def _():
        gate_out[halo, :] = jnp.zeros((RIM, wide), jnp.bfloat16)
        gate_out[body_rows, :] = lower
        gate_across.start()
        ext[halo, side] = lower[end].astype(jnp.float32)

    upper = gate(1)
    rim_out[...] = upper[end]

    @pl.when(has_later)
    def _():
        later_rim.start()

    @pl.when(even)
    def _():
        gate_out[body_rows, :] = upper
        gate_across.start()

    @pl.when(odd)
    def _():
        ext[body_rows, side] = upper.astype(jnp.float32)

    tick(8)

    @pl.when(has_earlier)
    def _():
        with jax.named_scope("rim_wait"):
            for g in range(2):
                remote(
                    rim_out, rim.at[g], rim_sem.at[0], rim_sem.at[1 + g], partner
                ).wait_recv()
        for g in range(2):
            ext[halo, g * wide : (g + 1) * wide] = rim[g].astype(jnp.float32)

    tap_count = taps_ref.shape[0]
    block = 64

    lead = RIM - (tap_count - 1)

    def convolve(c):
        cols = pl.ds(pl.multiple_of(c * 128, 128), 128)
        taps = taps_ref[:, cols].astype(jnp.float32)
        for r in range(0, rows, block):
            total = jnp.zeros((block, 128), jnp.float32)
            for shift in range(8):
                height = block + (8 if shift else 0)
                partial = jnp.zeros((height, 128), jnp.float32)
                for offset in range(shift, RIM + 1, 8):
                    if offset >= lead:
                        tap = taps[offset - lead : offset - lead + 1, :]
                        partial = partial + ext[pl.ds(r + offset - shift, height), cols] * tap
                total = total + partial[shift : shift + block]
            sums[pl.ds(r, block), cols] = total

    tiles = wide // 128
    pl.loop(parity * tiles, (parity + 1) * tiles)(convolve)
    pl.when(odd)(lambda: tick(9))
    with jax.named_scope("gate_wait"):
        gate_across.wait_recv()
    ext[body_rows, opposite] = gate_in[body_rows, :].astype(jnp.float32)

    @pl.when(odd)
    def _():
        ext[halo, opposite] = gate_in[halo, :].astype(jnp.float32)

    pl.loop((1 - parity) * tiles, (2 - parity) * tiles)(convolve)
    finish_far(7)

    @pl.loop(0, rows // part)
    def _(i):
        begin = pl.multiple_of(i * part, part)
        values = sums[pl.ds(begin, part), :]
        stats[pl.ds(begin, part), :] = jnp.broadcast_to(
            jnp.sum(values, axis=1, keepdims=True), (part, 128)
        )
        stats[pl.ds(pl.multiple_of(rows + begin, part), part), :] = jnp.broadcast_to(
            jnp.sum(values * values, axis=1, keepdims=True), (part, 128)
        )

    stat_copy.start()
    pl.when(even)(lambda: tick(9))
    with jax.named_scope("att_wait"):
        att_across.wait_recv()
    att = att_all[...].astype(jnp.float32).T.astype(jnp.bfloat16)
    span = ho.shape[1]

    complete(3)

    @pl.loop(0, n_fs)
    def _(i):
        cols = pl.ds(pl.multiple_of(i * span, span), span)
        acc_out[:, cols] = jnp.dot(
            att[:, :first_rows], ho_all[:first_rows, cols], preferred_element_type=jnp.float32
        )

    finish_far(8)
    with jax.named_scope("stat_wait"):
        stat_copy.wait_recv()
    channels = ext.shape[1] * n_tp

    @pl.loop(0, rows // part)
    def _(i):
        begin = pl.multiple_of(i * part, part)
        upper = pl.ds(begin, part)
        lower = pl.ds(pl.multiple_of(rows + begin, part), part)
        total = stats[upper, :] + stats_all[upper, :]
        squares = stats[lower, :] + stats_all[lower, :]
        mean = total[:, :1] / channels
        spread = squares[:, :1] / channels - mean * mean
        shaped = (sums[upper, :] - mean) * lax.rsqrt(spread + epsilon)
        conv_s[upper, :] = jax.nn.silu(
            shaped * cgain_ref[...] + cshift_ref[...]
        ).astype(jnp.bfloat16)

    tick(10)
    outs = []
    pieces = [(owner, 0, span) for owner in (f, near_x, near_y)]
    pieces += [(far, 0, span // 2), (far, span // 2, span // 2)]
    for i, (owner, begin, width) in enumerate(pieces):
        cols = pl.ds(pl.multiple_of(owner * span + begin, 128), width)
        outs.append(remote(
            mine_ref.at[:, cols], other_ref.at[:, cols], out_send.at[i], out_recv.at[i], twin
        ))
        if i == 1:
            complete(7, slice(0, len(sources)))
            complete(8, slice(0, len(sources)))
        if i == n_fs - 1:
            finish_far(9)
            finish_far(last)
            complete(7, slice(len(sources), None))
            complete(8, slice(len(sources), None))
        mine_ref[:, cols] = (
            acc_out[:, cols]
            + jnp.dot(att[:, first_rows:], ho_all[first_rows:, cols], preferred_element_type=jnp.float32)
            + jnp.dot(conv_s[...], co_all[:, cols], preferred_element_type=jnp.float32)
        ).astype(jnp.bfloat16)
        outs[i].start()

    for a in range(last + 1 - slots, last + 1):
        sent(a, 0)
        sent(a, 1)
    for a in lanes:
        sent(a, 2)
    for copy in (x_send, x_forward, query_copy, stat_copy, gate_across, att_across):
        copy.wait_send()

    @pl.when(even)
    def _():
        query_across.wait_send()
        back_forward.wait_send()

    @pl.when(odd)
    def _():
        memory_copy.wait_send()
        back.wait_send()
        for d in range(1, couples):
            @pl.when(couple + d < couples)
            def _(d=d):
                for e in range(2):
                    for copy in onward[d - 1][e]:
                        copy.wait_send()

    for d in range(1, couples):
        @pl.when(couple >= d)
        def _(d=d):
            forwards[d - 1].wait_send()

    @pl.when(has_later)
    def _():
        later_rim.wait_send()

    with jax.named_scope("out_wait"):
        for copy in outs:
            copy.wait()


def fused_call(
    sizes, x, mix_gain, rope_weight, taps, channel_gain, channel_shift,
    latent_gain, memory_gain, query_gain, key_gain,
    qd, md, cv, cg, qu, ku, vu, ho, co,
):
    n_fs, n_sp, n_tp = sizes
    rows, model = x.shape
    bf16, f32 = jnp.bfloat16, jnp.float32
    hbm = pl.BlockSpec(memory_space=pl.ANY)
    cosine, sine = table_rows(n_sp * rows)
    small = [
        mix_gain[None, :], rope_weight.T, taps, channel_gain[None, :], channel_shift[None, :],
        latent_gain.reshape(-1, 128), memory_gain[None, :], query_gain[None, :],
        key_gain[None, :], jnp.asarray(cosine), jnp.asarray(sine),
    ]

    def whole(w, dim=0, parts=1):
        rows_w, cols_w = w.shape[0], w.shape[1] // parts
        return (rows_w * n_fs, cols_w) if dim == 0 else (rows_w, cols_w * n_fs)

    def scratch(*shape, dtype=f32):
        return pltpu.VMEM(shape, dtype)

    dma = pltpu.SemaphoreType.DMA
    channels, lat = cv.shape[1], md.shape[1] * n_tp
    rope = rope_weight.shape[1]
    couples = n_sp // 2
    spare = max(couples - 1, 1)
    count, slots = 11, 3
    return pl.pallas_call(
        functools.partial(fused_kernel, sizes),
        out_shape=[jax.ShapeDtypeStruct((rows, ho.shape[1] * n_fs), bf16)] * 2,
        in_specs=[hbm] * 21,
        out_specs=[pl.BlockSpec(memory_space=pltpu.VMEM)] * 2,
        scratch_shapes=[scratch(*a.shape, dtype=a.dtype) for a in small] + [
            scratch(*whole(qd), dtype=bf16), scratch(*whole(md), dtype=bf16),
            scratch(*whole(ku, 0, 2), dtype=bf16), scratch(*whole(vu, 0, 2), dtype=bf16),
            scratch(*whole(qu, 0, 2), dtype=bf16), scratch(*whole(cv, 0, 2), dtype=bf16),
            scratch(*whole(cg, 0, 2), dtype=bf16), scratch(*whole(ho, 1), dtype=bf16),
            scratch(*whole(co, 1), dtype=bf16),
            scratch(2, rows, model, dtype=bf16), scratch(2, rows, model, dtype=bf16),
            scratch(n_tp, 2, rows, qd.shape[1], dtype=bf16),
            scratch(n_tp, 2, rows, md.shape[1], dtype=bf16),
            scratch(n_sp, lat, rows, dtype=bf16), scratch(n_sp, rope, rows, dtype=bf16),
            scratch(qu.shape[0] * n_fs, 2 * rows, dtype=bf16), scratch(qu.shape[1] // 2, 2 * rows),
            scratch(n_sp, ku.shape[1] // 2, rows),
            scratch(n_sp, vu.shape[1] // 2, rows, dtype=bf16),
            scratch(n_sp, rope, rows), scratch(n_sp, 1, rows),
            scratch(QK_DIM, 2 * rows), scratch(QK_DIM, rows),
            scratch(n_sp, rows, 2 * rows), scratch(n_sp, rows, 2 * rows),
            scratch(vu.shape[1] // 2, 2 * rows), scratch(vu.shape[1] // 2, rows, dtype=bf16),
            scratch(vu.shape[1], rows, dtype=bf16), scratch(rows, channels, dtype=bf16),
            scratch(2, rows, channels // 2),
            scratch(rows, ho.shape[1] * n_fs),
            scratch(rows + RIM, channels // 2, dtype=bf16),
            scratch(rows + RIM, channels // 2, dtype=bf16),
            scratch(rows + RIM, channels), scratch(RIM, channels // 2, dtype=bf16),
            scratch(2, RIM, channels // 2, dtype=bf16), scratch(rows, channels),
            scratch(2 * rows, 128), scratch(2 * rows, 128),
            dma((slots, 2)), dma((count, 2)), dma((slots, 2)), dma((count, 2)),
            dma((slots, 3)), dma((slots, 3)), dma((slots,)), dma((slots,)), dma((3,)),
            dma((5,)), dma((8,)), dma((spare, 2, 2)), dma((spare, 2)),
            dma((couples,)), dma((couples,)), dma((3,)), dma((3,)), dma((n_fs + 1,)), dma((n_fs + 1,)),
            pltpu.SemaphoreType.REGULAR((1,)),
        ],
        compiler_params=pltpu.CompilerParams(
            collective_id=1, has_side_effects=True, vmem_limit_bytes=40 * 1024 * 1024
        ),
    )(*[
        pltpu.with_memory_space_constraint(a, pltpu.HBM)
        for a in (x, *small, qd, md, ku, vu, qu, cv, cg, ho, co)
    ])


def fused_local(
    tokens, mix_gain, query_down, memory_down, rope_weight, query_up, key_up, value_up,
    latent_gain, memory_gain, query_gain, key_gain, conv_value, conv_gate, conv_kernel,
    channel_gain, channel_shift, heads_out, conv_out,
):
    mine, other = fused_call(
        (lax.axis_size("fs"), lax.axis_size("sp"), lax.axis_size("tp")),
        tokens[0], mix_gain, rope_weight, conv_kernel, channel_gain, channel_shift,
        latent_gain, memory_gain, query_gain, key_gain,
        query_down, memory_down, conv_value, conv_gate,
        query_up, key_up, value_up, heads_out, conv_out,
    )
    return (mine.astype(jnp.float32) + other.astype(jnp.float32)).astype(jnp.bfloat16)[None]


def solution(mesh):
    in_specs = (
        P("fs", "sp", None),
        P(),
        P("fs", "tp"),
        P("fs", "tp"),
        P(),
        P("fs", "tp"),
        P("fs", "tp"),
        P("fs", "tp"),
        P(),
        P(),
        P(),
        P(),
        P("fs", "tp"),
        P("fs", "tp"),
        P(None, "tp"),
        P("tp"),
        P("tp"),
        P("tp", "fs"),
        P("tp", "fs"),
    )
    out_specs = P("fs", "sp", None)
    n_fs, n_sp, n_tp = (mesh.shape[axis] for axis in ("fs", "sp", "tp"))
    fits = n_fs == 4 and n_tp == 2 and n_sp in (2, 4)
    body = fused_local if fits else local
    return jax.shard_map(body, mesh=mesh, in_specs=in_specs, out_specs=out_specs, check_vma=False)
```
